128 devices in a mesh: sp: 16 (over z, y), fs: 4 (over x), tp: 2 (over core).
Axes of the slice: x: 4, y: 4, z: 4, core: 2. Of those that a mesh axis runs over, the one named last changes fastest.
Arguments:
- tokens: bfloat16 [8, 2048, 2048], P('fs', 'sp', 'tp'), may hold values from -8 to 8
- norm_gain: float32 [2048], replicated, may hold values from 0.1 to 1.9
- w_recept: bfloat16 [2048, 768], P(None, 'tp'), may hold values from -0.125 to 0.125
- w_key: bfloat16 [2048, 768], P(None, 'tp'), may hold values from -0.125 to 0.125
- w_value: bfloat16 [2048, 768], P(None, 'tp'), may hold values from -0.125 to 0.125
- w_decay: bfloat16 [2048, 768], P(None, 'tp'), may hold values from -0.125 to 0.125
- w_rate: bfloat16 [2048, 768], P(None, 'tp'), may hold values from -0.125 to 0.125
- w_gate_rec: bfloat16 [2048, 768], P(None, 'tp'), may hold values from -0.125 to 0.125
- w_pool: bfloat16 [2048, 512], P(None, 'tp'), may hold values from -0.125 to 0.125
- w_gate_pool: bfloat16 [2048, 512], P(None, 'tp'), may hold values from -0.125 to 0.125
- decay_base: float32 [768], replicated, may hold values from -12 to -2.5
- rate_base: float32 [768], replicated, may hold values from -7 to 1
- head_gain: float32 [768], replicated, may hold values from 0.1 to 1.9
- pool_mix: bfloat16 [4, 128, 128], replicated, may hold values from -0.5 to 0.5
- pool_scale: float32 [512], replicated, may hold values from 0.3 to 3
- w_out_rec: bfloat16 [768, 2048], P('tp'), may hold values from -0.15625 to 0.15625
- w_out_pool: bfloat16 [512, 2048], P('tp'), may hold values from -0.15625 to 0.15625
- init_state: float32 [8, 12, 64, 64], P('fs', 'tp'), may hold values from -240 to 240
Outputs:
- mixed: bfloat16 [8, 2048, 2048], P('fs', 'sp', 'tp')
The draws below stay inside these ranges and needn't reach their ends.
All inputs are finite; a program needn't handle non-finite values.
Results may differ from the reference program's by a relative error of at most 0.015.
Values may be sent and summed in bfloat16 or wider, within the bound.
No kernel may reach another device: no remote copies, remote signals or barrier semaphores. Data moves between devices by JAX's collectives and lax.ppermute only.
A program may use at most 128 MiB of HBM per device.

```python
import math
import jax
import jax.numpy as jnp
from jax import lax

D = 2048
HEADS = 12
HEAD_DIM = 64
GROUPS = 4
GROUP_W = 128
RW = 768
PW = 512
LENGTH = 2048
SEQS = 8
N_TP = 2


def head_kinds(key):
    base = jax.random.fold_in(key, 7)
    first, second, third = jax.random.split(base, 3)
    head_ids = jnp.arange(HEADS)
    coins = jax.random.randint(first, (HEADS,), 0, 2)
    slow_pick = jax.random.randint(second, (), 0, HEADS)
    fast_pick = (slow_pick + 1 + jax.random.randint(third, (), 0, HEADS - 1)) % HEADS
    slow = jnp.where(head_ids == slow_pick, 1, jnp.where(head_ids == fast_pick, 0, coins))
    return jnp.repeat(slow, HEAD_DIM)


def draw_decay_base(key, part):
    slow = head_kinds(key)
    slow_value = jax.random.uniform(jax.random.fold_in(key, 21), (RW,), jnp.float32, -12.0, -10.0)
    fast_value = jax.random.uniform(jax.random.fold_in(key, 22), (RW,), jnp.float32, -3.5, -2.5)
    return jnp.where(slow == 1, slow_value, fast_value).astype(jnp.float32)


def draw_rate_base(key, part):
    slow = head_kinds(key)
    slow_value = jax.random.uniform(jax.random.fold_in(key, 31), (RW,), jnp.float32, -7.0, -5.5)
    fast_value = jax.random.uniform(jax.random.fold_in(key, 32), (RW,), jnp.float32, -1.0, 1.0)
    return jnp.where(slow == 1, slow_value, fast_value).astype(jnp.float32)


def draw_tokens(key, part):
    first, second = jax.random.split(jax.random.fold_in(key, 3))
    means = jax.random.truncated_normal(second, -4.0, 4.0, (SEQS, LENGTH // 64, D), jnp.float32)
    means = jnp.repeat(means, 64, axis=1)
    noise = jax.random.truncated_normal(first, -4.0, 4.0, (SEQS, LENGTH, D), jnp.float32)
    values = noise + 0.8 * means
    return values.astype(jnp.bfloat16)


def steps_of(key, shape, shards, low, top_value):
    def one(position, parts):
        draws = jax.random.uniform(jax.random.fold_in(jax.random.fold_in(key, 6), position), (parts,), jnp.float32, low / len(shards), top_value / len(shards))
        return jnp.repeat(jnp.exp(draws), shape[position] // parts).reshape((-1,) + (1,) * (len(shape) - position - 1))

    factor_of = one(*shards[0])
    for cut in shards[1:]:
        factor_of = factor_of * one(*cut)
    return factor_of


def bell_draw(own_key, extent, scale, most, shards=(), held_as=jnp.bfloat16):
    gain = steps_of(own_key, extent, shards, -0.22, 0.18) if shards else 1.0
    values = jax.random.normal(own_key, extent, jnp.float32) * scale * gain
    return jnp.minimum(jnp.maximum(values, -most), most).astype(held_as)


def setup_inputs(seed: int = 0) -> dict:
    splits = jax.random.split(jax.random.key(seed), 19)
    return {
        "tokens": draw_tokens(jax.random.fold_in(splits[18], 71), 0),
        "norm_gain": jnp.clip(1.0 + 0.18 * jax.random.normal(splits[1], (D,), jnp.float32), 0.1, 1.9),
        "w_recept": bell_draw(splits[2], (D, RW), D ** -0.5, 0.125, ((1, 2),)),
        "w_key": bell_draw(splits[3], (D, RW), D ** -0.5, 0.125, ((1, 2),)),
        "w_value": bell_draw(splits[4], (D, RW), D ** -0.5, 0.125, ((1, 2),)),
        "w_decay": bell_draw(splits[5], (D, RW), D ** -0.5, 0.125, ((1, 2),)),
        "w_rate": bell_draw(splits[6], (D, RW), D ** -0.5, 0.125, ((1, 2),)),
        "w_gate_rec": bell_draw(splits[7], (D, RW), D ** -0.5, 0.125, ((1, 2),)),
        "w_pool": bell_draw(splits[8], (D, PW), D ** -0.5, 0.125, ((1, 2),)),
        "w_gate_pool": bell_draw(splits[9], (D, PW), D ** -0.5, 0.125, ((1, 2),)),
        "decay_base": draw_decay_base(jax.random.fold_in(splits[18], 71), 0),
        "rate_base": draw_rate_base(jax.random.fold_in(splits[18], 71), 0),
        "head_gain": jnp.clip(1.0 + 0.18 * jax.random.normal(splits[12], (RW,), jnp.float32), 0.1, 1.9),
        "pool_mix": bell_draw(splits[13], (GROUPS, GROUP_W, GROUP_W), GROUP_W ** -0.5, 0.5),
        "pool_scale": jnp.clip(jnp.exp(jax.random.uniform(splits[14], (PW,), jnp.float32, math.log(0.3), math.log(3.0))), 0.3, 3.0),
        "w_out_rec": bell_draw(splits[15], (RW, D), (RW + PW) ** -0.5, 0.15625, ((0, 2),)),
        "w_out_pool": bell_draw(splits[16], (PW, D), (RW + PW) ** -0.5, 0.15625, ((0, 2),)),
        "init_state": bell_draw(splits[17], (SEQS, HEADS, HEAD_DIM, HEAD_DIM), 40.0, 240.0, ((0, 4), (1, 2)), jnp.float32),
    }


HIGHEST = lax.Precision.HIGHEST

def reference(tokens, norm_gain, w_recept, w_key, w_value, w_decay, w_rate, w_gate_rec, w_pool, w_gate_pool, decay_base, rate_base, head_gain, pool_mix, pool_scale, w_out_rec, w_out_pool, init_state):
    wide = tokens.astype(jnp.float32)
    scale = lax.rsqrt(lax.optimization_barrier(jnp.mean(wide * wide, axis=-1, keepdims=True)) + 0.25)
    normed = (wide * norm_gain).astype(jnp.bfloat16)
    flat = normed.reshape(-1, D)

    def project(weight):
        product = jnp.dot(flat, weight, preferred_element_type=jnp.float32).reshape(SEQS, LENGTH, -1)
        return (product * scale).astype(jnp.bfloat16)
    receptance, key_proj, value, decay_in, rate_in, gate_rec, pool_in, gate_pool = [project(weight) for weight in (w_recept, w_key, w_value, w_decay, w_rate, w_gate_rec, w_pool, w_gate_pool)]

    def split_heads(array):
        return array.astype(jnp.float32).reshape(SEQS, LENGTH, HEADS, HEAD_DIM)
    log_decay = -jnp.exp(-jax.nn.softplus(-(decay_base + decay_in.astype(jnp.float32))) - 0.5)
    rate = jax.nn.sigmoid(rate_base + rate_in.astype(jnp.float32))
    keys = split_heads(key_proj)
    unit_key = keys * lax.rsqrt(lax.optimization_barrier(jnp.sum(keys * keys, axis=-1, keepdims=True)) + 1.0)
    removal = unit_key * split_heads(rate)
    inputs = tuple((jnp.moveaxis(array, 1, 0) for array in (split_heads(receptance), keys, split_heads(value), jnp.exp(split_heads(log_decay)), unit_key, removal)))

    def advance(state, item):
        read, write_key, write_value, decay, unit, remove = item
        removed = jnp.einsum('bhvk,bhk->bhv', state, unit, precision=HIGHEST)
        state = state * decay[:, :, None, :] - removed[..., None] * remove[:, :, None, :] + write_value[..., None] * write_key[:, :, None, :]
        return (state, jnp.einsum('bhvk,bhk->bhv', state, read, precision=HIGHEST))
    _, outputs = lax.scan(advance, init_state, inputs)
    recurrent = jnp.moveaxis(outputs, 0, 1)
    center = lax.optimization_barrier(jnp.mean(recurrent, axis=-1, keepdims=True))
    spread = lax.optimization_barrier(jnp.mean(jnp.square(recurrent - center), axis=-1, keepdims=True))
    normal_out = ((recurrent - center) * lax.rsqrt(spread + 1.0)).reshape(SEQS, LENGTH, RW) * head_gain
    rec_out = (normal_out * jax.nn.silu(gate_rec.astype(jnp.float32))).astype(jnp.bfloat16)
    pool_wide = pool_in.astype(jnp.float32)
    padded = jnp.pad(pool_wide, ((0, 0), (15, 0), (0, 0)))
    places = jnp.arange(1, LENGTH + 1, dtype=jnp.float32)[None, :, None]
    pieces = []
    for group in range(GROUPS):
        window = 2 ** (group + 1)
        low = group * GROUP_W
        trailing = padded[:, 15:15 + LENGTH, low:low + GROUP_W]
        for offset in range(1, window):
            trailing = trailing + padded[:, 15 - offset:15 - offset + LENGTH, low:low + GROUP_W]
        pieces.append(trailing / jnp.minimum(places, float(window)) - pool_wide[:, :, low:low + GROUP_W])
    diffs = jnp.stack(pieces, axis=2).astype(jnp.bfloat16)
    pool_mixed = jnp.einsum('bsgc,gcd->bsgd', diffs.astype(jnp.float32), pool_mix.astype(jnp.float32)).reshape(SEQS, LENGTH, PW)
    pool_out = (pool_mixed * pool_scale * jax.nn.silu(gate_pool.astype(jnp.float32))).astype(jnp.bfloat16)
    rec_block = RW // N_TP
    pool_block = PW // N_TP
    rec_flat = rec_out.reshape(-1, RW)
    pool_flat = pool_out.reshape(-1, PW)
    total = jnp.zeros((SEQS * LENGTH, D), jnp.float32)
    for index in range(N_TP):
        first = jnp.dot(rec_flat[:, index * rec_block:(index + 1) * rec_block], w_out_rec[index * rec_block:(index + 1) * rec_block], preferred_element_type=jnp.float32)
        second = jnp.dot(pool_flat[:, index * pool_block:(index + 1) * pool_block], w_out_pool[index * pool_block:(index + 1) * pool_block], preferred_element_type=jnp.float32)
        partial_sum = lax.optimization_barrier((first + second).astype(jnp.bfloat16))
        total = total + partial_sum.astype(jnp.float32)
    return total.reshape(SEQS, LENGTH, D).astype(jnp.bfloat16)
```

```python
import functools

import jax
import jax.numpy as jnp
from jax import lax
from jax.experimental import pallas as pl
from jax.experimental.pallas import tpu as pltpu
from jax.sharding import Mesh
from jax.sharding import PartitionSpec as P

D = 2048
HEAD = 64
SPAN = 128
UNITS = 6
SP = ("sp_0", "sp_1")
f32 = jnp.float32
bf16 = jnp.bfloat16
NN = ((1,), (0,))
NT = ((1,), (1,))
TN = ((0,), (0,))
MIB = 2**20


def dot(a, b, dims=NN):
    return lax.dot_general(
        a.astype(bf16), b.astype(bf16), (dims, ((), ())), preferred_element_type=f32
    )


def halves(x):
    high = x.astype(bf16)
    return high, (x - high.astype(f32)).astype(bf16)


def dot_fine_left(a, b, dims=NN):
    high, low = halves(a)
    return dot(high, b, dims) + dot(low, b, dims)


def dot_fine_right(a, b, dims=NN):
    high, low = halves(b)
    return dot(a, high, dims) + dot(a, low, dims)


def iota(rows, cols, dim):
    return lax.broadcasted_iota(jnp.int32, (rows, cols), dim)


def head_masks():
    first = (iota(1, 128, 1) < HEAD).astype(f32)
    return first, 1.0 - first


def both(x, masks):
    return jnp.concatenate([x * masks[0], x * masks[1]], axis=0)


def compose(earlier, later, masks):
    moved = dot_fine_left(earlier, both(later[:HEAD].astype(f32), masks))
    written = later[HEAD:].astype(f32)
    if earlier.shape[0] == HEAD:
        return moved + written
    return jnp.concatenate([moved[:HEAD], moved[HEAD:] + written], axis=0)


def pick(x, size, odd):
    parts = [x[s : s + size] for s in range(size * odd, SPAN, 2 * size)]
    return parts[0] if len(parts) == 1 else jnp.concatenate(parts, axis=0)


def weave(even, odd, size):
    parts = []
    for s in range(0, SPAN // 2, size):
        parts += [even[s : s + size], odd[s : s + size]]
    return jnp.concatenate(parts, axis=0)


def inverses(lowers):
    row, col = iota(SPAN, SPAN, 0), iota(SPAN, SPAN, 1)
    eye = (row == col).astype(f32)
    near = ((row >> 1) == (col >> 1)).astype(f32)
    result = [eye - lower * near for lower in lowers]
    size, level = 2, 1
    while size < SPAN:
        off = (((row >> (level + 1)) == (col >> (level + 1))) & ((row >> level) != (col >> level))).astype(f32)
        if size < 8:
            inner = [dot(lower * off, inv) for lower, inv in zip(lowers, result)]
            result = [inv - dot(inv, part) for inv, part in zip(result, inner)]
        else:
            off = pick(off, size, 1)
            inner = [dot(pick(lower, size, 1) * off, inv) for lower, inv in zip(lowers, result)]
            outer = [
                dot(pick(inv, size, 1), weave(jnp.zeros_like(part), part, size))
                for inv, part in zip(result, inner)
            ]
            result = [
                weave(pick(inv, size, 0), pick(inv, size, 1) - part, size)
                for inv, part in zip(result, outer)
            ]
        size, level = size * 2, level + 1
    return result


def local_kernel(
    own_ref, other_ref, gain_ref, db_ref, rb_ref, wk_ref, wd_ref, wa_ref, wr_ref, wv_ref,
    normed_ref, scale_ref, home_ref, first_ref, second_ref, third_ref,
    wb_ref, wkk_ref, solved_ref, v_ref, rho_ref,
    k_s, d_s, a_s, r_s, v_s, maps, w_bufs, sems,
):
    tp = lax.axis_index("tp")
    y = lax.axis_index("sp_1")
    sources = (wk_ref, wd_ref, wa_ref, wr_ref, wv_ref)
    copies = [pltpu.make_async_copy(src, w_bufs.at[i], sems.at[i]) for i, src in enumerate(sources)]
    for copy in copies:
        copy.start()
    own = own_ref[...].astype(f32)
    other = other_ref[...].astype(f32)
    gain_a, gain_b = gain_ref[:, :1024], gain_ref[:, 1024:]
    is_first = tp == 0
    own_normed = (own * jnp.where(is_first, gain_a, gain_b)).astype(bf16)
    other_normed = (other * jnp.where(is_first, gain_b, gain_a)).astype(bf16)
    squares = jnp.sum(own * own + other * other, axis=1, keepdims=True)
    scale = lax.rsqrt(squares * (1.0 / D) + 0.25)
    normed_ref[:, :1024] = own_normed
    normed_ref[:, 1024:] = other_normed
    scale_ref[...] = jnp.broadcast_to(scale, (256, 128))
    for i, dest in enumerate((k_s, d_s, a_s, r_s, v_s)):
        copies[i].wait()
        total = dot(own_normed, w_bufs[i, pl.ds(tp * 1024, 1024), :])
        total = total + dot(other_normed, w_bufs[i, pl.ds((1 - tp) * 1024, 1024), :])
        rounded = (total * scale).astype(bf16)
        for u in range(UNITS):
            s, h = u // 3, u % 3
            dest[u] = rounded[s * 128 : s * 128 + 128, h * 128 : h * 128 + 128].astype(f32)

    masks = head_masks()
    n = SPAN
    row, col = iota(n, n, 0), iota(n, n, 1)
    strict, inclusive = row > col, row >= col
    triangle = inclusive.astype(f32)
    ones = ((row >> 6) == (col >> 6)).astype(f32)
    wide = (
        jnp.concatenate([masks[0], masks[0]], axis=1),
        jnp.concatenate([masks[1], masks[1]], axis=1),
    )
    slab = iota(HEAD, 128, 0)
    eye = (slab == (iota(HEAD, 128, 1) & 63)).astype(f32)
    units = range(UNITS)
    lowers, alphas, keeps = [], [], []
    for u in units:
        h = u % 3
        lanes = slice(h * 128, h * 128 + 128)
        shifted = slice(384 + h * 128, 384 + h * 128 + 128)
        db = jnp.where(is_first, db_ref[:, lanes], db_ref[:, shifted])
        rb = jnp.where(is_first, rb_ref[:, lanes], rb_ref[:, shifted])
        k = k_s[u]
        log_decay = -0.6065306597126334 * jax.nn.sigmoid(db + d_s[u])
        rate = jax.nn.sigmoid(rb + a_s[u])
        unit_key = k * lax.rsqrt(dot_fine_left(k * k, ones) + 1.0)
        removal = unit_key * rate
        total = dot_fine_right(triangle, log_decay)
        middle, final = total[63:64], total[127:128]
        alpha = jnp.exp(total - log_decay - middle) * unit_key
        fading = jnp.exp(middle - total)
        beta, kappa = removal * fading, k * fading
        rho = r_s[u] * jnp.exp(total - middle)
        ending = jnp.exp(final - total)
        lift = jnp.exp(middle)
        rho_ref[u] = rho * lift
        left = jnp.concatenate([alpha * masks[0], alpha * masks[1], rho * masks[0], rho * masks[1]], axis=0)
        pairs = dot(left, jnp.concatenate([beta, kappa], axis=0), NT)
        lower_kappa = []
        for j in (0, 1):
            lowers.append(jnp.where(strict, pairs[j * n : j * n + n, :n], 0.0))
            lower_kappa.append(jnp.where(strict, pairs[j * n : j * n + n, n:], 0.0).astype(bf16))
            wb_ref[u, :, j * n : j * n + n] = jnp.where(
                inclusive, pairs[(2 + j) * n : (3 + j) * n, :n], 0.0
            ).astype(bf16)
            wkk_ref[u, :, j * n : j * n + n] = jnp.where(
                inclusive, pairs[(2 + j) * n : (3 + j) * n, n:], 0.0
            ).astype(bf16)
        v = v_s[u]
        v_ref[u] = v.astype(bf16)
        carried = dot(jnp.concatenate(lower_kappa, axis=1), both(v, masks))
        keeps.append((alpha * lift, carried, removal * ending, k * ending, jnp.exp(final)))
    inverse = inverses(lowers)
    for u in units:
        alpha, carried, beta_end, kappa_end, gain_end = keeps[u]
        right = jnp.concatenate([alpha, carried], axis=1)
        solved = dot(jnp.concatenate(inverse[2 * u : 2 * u + 2], axis=1), both(right, wide))
        solved_ref[u] = solved.astype(bf16)
        crossed = dot(solved[:, :n], beta_end, TN)
        transit = eye * gain_end - (crossed[:HEAD] * masks[0] + crossed[HEAD:] * masks[1])
        crossed = dot(
            jnp.concatenate([v_s[u], -solved[:, n:]], axis=0),
            jnp.concatenate([kappa_end, beta_end], axis=0),
            TN,
        )
        written = crossed[:HEAD] * masks[0] + crossed[HEAD:] * masks[1]
        maps[u % 3, u // 3, :HEAD] = transit.astype(bf16)
        maps[u % 3, u // 3, HEAD:] = written.astype(bf16)
    maps[3] = jnp.zeros((2, 128, 128), bf16)
    for step, dest in enumerate((home_ref, first_ref, second_ref, third_ref)):
        dest[...] = maps[(y + step) & 3]


def side_kernel(
    normed_ref, scale_ref, wb_ref, wkk_ref, solved_ref, v_ref, rho_ref, wg_ref, wp_ref, wq_ref,
    reads_ref, local_ref, gate_ref, pool_ref, pgate_ref, tail_ref,
    g_buf, p_bufs, sems,
):
    tp = lax.axis_index("tp")
    copies = [
        pltpu.make_async_copy(wp_ref, p_bufs.at[0], sems.at[0]),
        pltpu.make_async_copy(wq_ref, p_bufs.at[1], sems.at[1]),
        pltpu.make_async_copy(wg_ref, g_buf, sems.at[2]),
    ]
    for copy in copies:
        copy.start()
    masks = head_masks()
    wide = (
        jnp.concatenate([masks[0], masks[0]], axis=1),
        jnp.concatenate([masks[1], masks[1]], axis=1),
    )
    for u in range(UNITS):
        removed = dot(wb_ref[u], both(solved_ref[u].astype(f32), wide))
        reads_ref[u] = (rho_ref[u] - removed[:, :128]).astype(bf16)
        local_ref[u] = dot(wkk_ref[u], both(v_ref[u].astype(f32), masks)) - removed[:, 128:]
    scale = scale_ref[:, :1]
    own, other = normed_ref[:, :1024], normed_ref[:, 1024:]

    def project(buf):
        total = dot(own, buf[pl.ds(tp * 1024, 1024), :])
        total = total + dot(other, buf[pl.ds((1 - tp) * 1024, 1024), :])
        return (total * scale).astype(bf16)

    copies[0].wait()
    pool = project(p_bufs.at[0])
    pool_ref[...] = pool
    tail_ref[0] = pool[112:128]
    tail_ref[1] = pool[240:256]
    copies[1].wait()
    pgate_ref[...] = project(p_bufs.at[1])
    copies[2].wait()
    gate_ref[...] = project(g_buf)


def row_kernel(home_ref, first_ref, second_ref, third_ref, prefix_ref, total_ref, maps):
    y = lax.axis_index("sp_1")
    for step, src in enumerate((home_ref, first_ref, second_ref, third_ref)):
        maps[(y + 4 - step) & 3] = src[...]
    masks = head_masks()
    for s in (0, 1):
        so_far = maps[0, s].astype(f32)
        prefix_ref[0, s] = so_far
        for j in (1, 2, 3):
            so_far = compose(so_far, maps[j, s], masks)
            if j < 3:
                prefix_ref[j, s] = so_far
            else:
                total_ref[s] = so_far.astype(bf16)


def column_kernel(
    prefix_ref, first_ref, second_ref, third_ref, init_ref,
    home_ref, one_ref, two_ref, three_ref,
    starts, rows,
):
    y = lax.axis_index("sp_1")
    z = lax.axis_index("sp_0")
    for step, src in enumerate((first_ref, second_ref, third_ref)):
        rows[(z + 3 - step) & 3] = src[...]
    masks = head_masks()
    pair = jnp.minimum(y, 2) * 2
    for s in (0, 1):
        state = jnp.concatenate([init_ref[s, pair], init_ref[s, pair + 1]], axis=1)
        for j in range(3):
            state = jnp.where(j < z, compose(state, rows[j, s], masks), state)
        starts[0, s] = state.astype(bf16)
        for j in range(3):
            starts[j + 1, s] = compose(state, prefix_ref[j, s], masks).astype(bf16)
    for step, dest in enumerate((home_ref, one_ref, two_ref, three_ref)):
        dest[...] = starts[(y + step) & 3]


def pool_kernel(pool_ref, tail_ref, pgate_ref, mix_ref, pscale_ref, out_ref):
    tp = lax.axis_index("tp")
    place = lax.axis_index("sp_0") * 4 + lax.axis_index("sp_1")
    is_first = tp == 0
    factor = jnp.where(is_first, pscale_ref[:, :256], pscale_ref[:, 256:])
    for s in (0, 1):
        current = pool_ref[s * 128 : s * 128 + 128].astype(f32)
        padded = jnp.concatenate([tail_ref[s].astype(f32), current], axis=0)
        sums = {1: padded}
        for by in (1, 2, 4, 8):
            before = sums[by]
            moved = jnp.concatenate([jnp.zeros((by, 256), f32), before[: 144 - by]], axis=0)
            sums[2 * by] = before + moved
        position = (place * 128 + iota(128, 128, 0) + 1).astype(f32)
        for g in (0, 1):
            lanes = slice(g * 128, g * 128 + 128)
            small, large = 2 << g, 8 << g
            trailing = jnp.where(is_first, sums[small][16:, lanes], sums[large][16:, lanes])
            window = jnp.where(is_first, float(small), float(large))
            diffs = trailing / jnp.minimum(position, window) - current[:, lanes]
            mixed = dot(diffs.astype(bf16), mix_ref[tp * 2 + g])
            gate = pgate_ref[s * 128 : s * 128 + 128, lanes].astype(f32)
            out_ref[s * 128 : s * 128 + 128, lanes] = (
                mixed * factor[:, lanes] * (gate * jax.nn.sigmoid(gate))
            ).astype(bf16)


def final_kernel(
    home_ref, one_ref, two_ref, three_ref, reads_ref, local_ref, gate_ref, hgain_ref, pool_ref,
    wr_ref, wp_ref,
    send_ref, keep_ref,
    starts, rec, wr_buf, wp_buf, sems,
):
    tp = lax.axis_index("tp")
    y = lax.axis_index("sp_1")
    copies = [
        pltpu.make_async_copy(wr_ref, wr_buf, sems.at[0]),
        pltpu.make_async_copy(wp_ref, wp_buf, sems.at[1]),
    ]
    for copy in copies:
        copy.start()
    for step, src in enumerate((home_ref, one_ref, two_ref, three_ref)):
        starts[(y + 4 - step) & 3] = src[...]
    masks = head_masks()
    row, col = iota(128, 128, 0), iota(128, 128, 1)
    mean_of = jnp.where((row >> 6) == (col >> 6), 1.0 / HEAD, 0.0).astype(bf16)
    is_first = tp == 0
    for u in range(UNITS):
        s, h = u // 3, u % 3
        lanes = slice(h * 128, h * 128 + 128)
        shifted = slice(384 + h * 128, 384 + h * 128 + 128)
        rows = slice(s * 128, s * 128 + 128)
        out = dot(reads_ref[u], both(starts[h, s].astype(f32), masks), NT) + local_ref[u]
        out = out - dot_fine_left(out, mean_of)
        spread = dot_fine_left(out * out, mean_of)
        gain = jnp.where(is_first, hgain_ref[:, lanes], hgain_ref[:, shifted])
        gate = gate_ref[rows, lanes].astype(f32)
        rec[rows, lanes] = (
            out * lax.rsqrt(spread + 1.0) * gain * (gate * jax.nn.sigmoid(gate))
        ).astype(bf16)
    for copy in copies:
        copy.wait()
    for dest, part in ((send_ref, 1 - tp), (keep_ref, tp)):
        cols = pl.ds(pl.multiple_of(part * 1024, 1024), 1024)
        dest[...] = (dot(rec[...], wr_buf[:, cols]) + dot(pool_ref[...], wp_buf[:, cols])).astype(bf16)


def vmem(count):
    return [pl.BlockSpec(memory_space=pltpu.VMEM)] * count


def hbm(count):
    return [pl.BlockSpec(memory_space=pl.ANY)] * count


def shape(dims, kind=bf16):
    return jax.ShapeDtypeStruct(dims, kind)


def call(body, name, ins, outs, scratch, limit, flops=0):
    return pl.pallas_call(
        body,
        name=name,
        out_shape=outs,
        in_specs=ins,
        out_specs=vmem(len(outs)) if isinstance(outs, (list, tuple)) else vmem(1)[0],
        scratch_shapes=scratch,
        compiler_params=pltpu.CompilerParams(vmem_limit_bytes=limit * MIB),
        cost_estimate=pl.CostEstimate(flops=flops, transcendentals=0, bytes_accessed=0) if flops else None,
    )


def spread_rows(parts, senders, receivers):
    out = []
    for step, part in enumerate(parts, 1):
        pairs = [(i, (i + step) & 3) for i in range(4) if i in senders and ((i + step) & 3) in receivers]
        out.append(lax.ppermute(part, "sp_1", pairs))
    return out


def shards(
    tokens, norm_gain, w_recept, w_key, w_value, w_decay, w_rate, w_gate_rec, w_pool, w_gate_pool,
    decay_base, rate_base, head_gain, pool_mix, pool_scale, w_out_rec, w_out_pool, init_state,
):
    other = lax.ppermute(tokens, "tp", [(0, 1), (1, 0)])
    line = lambda x: x.reshape(1, -1)
    normed, scale, home, m1, m2, m3, wb, wkk, solved, v, rho = call(
        local_kernel,
        "local",
        vmem(5) + hbm(5),
        [
            shape((256, D)), shape((256, 128), f32),
            shape((2, 128, 128)), shape((2, 128, 128)), shape((2, 128, 128)), shape((2, 128, 128)),
            shape((6, 128, 256)), shape((6, 128, 256)), shape((6, 128, 256)),
            shape((6, 128, 128)), shape((6, 128, 128), f32),
        ],
        [pltpu.VMEM((6, 128, 128), f32)] * 5
        + [pltpu.VMEM((4, 2, 128, 128), bf16), pltpu.VMEM((5, D, 384), bf16), pltpu.SemaphoreType.DMA((5,))],
        40,
        4_000_000_000,
    )(
        tokens.reshape(256, 1024), other.reshape(256, 1024), line(norm_gain), line(decay_base), line(rate_base),
        w_key, w_decay, w_rate, w_recept, w_value,
    )
    r1, r2, r3 = spread_rows((m1, m2, m3), (0, 1, 2, 3), (0, 1, 2))
    reads, local, gate, pool, pgate, tail = call(
        side_kernel,
        "side",
        vmem(7) + hbm(3),
        [
            shape((6, 128, 128)), shape((6, 128, 128), f32), shape((256, 384)), shape((256, 256)),
            shape((256, 256)), shape((2, 16, 256)),
        ],
        [pltpu.VMEM((D, 384), bf16), pltpu.VMEM((2, D, 256), bf16), pltpu.SemaphoreType.DMA((3,))],
        24,
        2_000_000_000,
    )(normed, scale, wb, wkk, solved, v, rho, w_gate_rec, w_pool, w_gate_pool)
    halo = lax.ppermute(tail, SP, [(i, i + 1) for i in range(15)])
    prefix, total = call(
        row_kernel,
        "row",
        vmem(4),
        [shape((3, 2, 128, 128), f32), shape((2, 128, 128))],
        [pltpu.VMEM((4, 2, 128, 128), bf16)],
        8,
        100_000_000,
    )(home, r1, r2, r3)
    columns = [
        lax.ppermute(total, "sp_0", [(i, i + step) for i in range(4) if i + step < 4]) for step in (1, 2, 3)
    ]
    s0, s1, s2, s3 = call(
        column_kernel,
        "column",
        vmem(5),
        [shape((2, 64, 128))] * 4,
        [pltpu.VMEM((4, 2, 64, 128), bf16), pltpu.VMEM((4, 2, 128, 128), bf16)],
        8,
        100_000_000,
    )(prefix, *columns, init_state)
    t1, t2, t3 = spread_rows((s1, s2, s3), (0, 1, 2), (0, 1, 2, 3))
    pool_out = call(pool_kernel, "pool", vmem(5), shape((256, 256)), [], 8, 100_000_000)(
        pool, halo, pgate, pool_mix, line(pool_scale)
    )
    send, keep = call(
        final_kernel,
        "final",
        vmem(9) + hbm(2),
        [shape((256, 1024)), shape((256, 1024))],
        [
            pltpu.VMEM((4, 2, 64, 128), bf16), pltpu.VMEM((256, 384), bf16), pltpu.VMEM((384, D), bf16),
            pltpu.VMEM((256, D), bf16), pltpu.SemaphoreType.DMA((2,)),
        ],
        20,
        1_000_000_000,
    )(s0, t1, t2, t3, reads, local, gate, line(head_gain), pool_out, w_out_rec, w_out_pool)
    arrived = lax.ppermute(send, "tp", [(0, 1), (1, 0)])
    mixed = keep.astype(f32) + arrived.astype(f32)
    return mixed.astype(bf16).reshape(2, 128, 1024)


def solution(mesh):
    split = Mesh(
        mesh.devices.reshape(4, 4, mesh.shape["fs"], mesh.shape["tp"]), ("sp_0", "sp_1", "fs", "tp")
    )
    column = P(None, "tp")
    placed = (
        (P("fs", SP, "tp"), P()) + (column,) * 8 + (P(),) * 5
        + (P("tp", None), P("tp", None), P("fs", "tp", None, None))
    )
    return jax.shard_map(
        shards, mesh=split, in_specs=placed, out_specs=P("fs", SP, "tp"), check_vma=False
    )
```

```python
import functools

import jax
import jax.numpy as jnp
from jax import lax
from jax.experimental import pallas as pl
from jax.experimental.pallas import tpu as pltpu
from jax.sharding import Mesh
from jax.sharding import PartitionSpec as P

D = 2048
HEAD = 64
SPAN = 128
UNITS = 6
SP = ("sp_0", "sp_1")
f32 = jnp.float32
bf16 = jnp.bfloat16
NN = ((1,), (0,))
NT = ((1,), (1,))
TN = ((0,), (0,))
MIB = 2**20


def dot(a, b, dims=NN):
    return lax.dot_general(
        a.astype(bf16), b.astype(bf16), (dims, ((), ())), preferred_element_type=f32
    )


def halves(x):
    high = x.astype(bf16)
    return high, (x - high.astype(f32)).astype(bf16)


def dot_fine_left(a, b, dims=NN):
    high, low = halves(a)
    return dot(high, b, dims) + dot(low, b, dims)


def dot_fine_right(a, b, dims=NN):
    high, low = halves(b)
    return dot(a, high, dims) + dot(a, low, dims)


def iota(rows, cols, dim):
    return lax.broadcasted_iota(jnp.int32, (rows, cols), dim)


def line_of(ref, lanes):
    if len(ref.shape) == 1:
        return ref[lanes].reshape(1, 128)
    return ref[:, lanes]


def head_masks():
    first = (iota(1, 128, 1) < HEAD).astype(f32)
    return first, 1.0 - first


def both(x, masks):
    return jnp.concatenate([x * masks[0], x * masks[1]], axis=0)


def compose(earlier, later, masks):
    moved = dot_fine_left(earlier, both(later[:HEAD].astype(f32), masks))
    written = later[HEAD:].astype(f32)
    if earlier.shape[0] == HEAD:
        return moved + written
    return jnp.concatenate([moved[:HEAD], moved[HEAD:] + written], axis=0)


def pick(x, size, odd):
    parts = [x[s : s + size] for s in range(size * odd, SPAN, 2 * size)]
    return parts[0] if len(parts) == 1 else jnp.concatenate(parts, axis=0)


def weave(even, odd, size):
    parts = []
    for s in range(0, SPAN // 2, size):
        parts += [even[s : s + size], odd[s : s + size]]
    return jnp.concatenate(parts, axis=0)


def inverses(lowers):
    row, col = iota(SPAN, SPAN, 0), iota(SPAN, SPAN, 1)
    eye = (row == col).astype(f32)
    near = ((row >> 1) == (col >> 1)).astype(f32)
    result = [eye - lower * near for lower in lowers]
    size, level = 2, 1
    while size < SPAN:
        off = (((row >> (level + 1)) == (col >> (level + 1))) & ((row >> level) != (col >> level))).astype(f32)
        if size < 8:
            inner = [dot(lower * off, inv) for lower, inv in zip(lowers, result)]
            result = [inv - dot(inv, part) for inv, part in zip(result, inner)]
        else:
            off = pick(off, size, 1)
            inner = [dot(pick(lower, size, 1) * off, inv) for lower, inv in zip(lowers, result)]
            outer = [
                dot(pick(inv, size, 1), weave(jnp.zeros_like(part), part, size))
                for inv, part in zip(result, inner)
            ]
            result = [
                weave(pick(inv, size, 0), pick(inv, size, 1) - part, size)
                for inv, part in zip(result, outer)
            ]
        size, level = size * 2, level + 1
    return result


WIDTHS = (384, 384, 384, 384, 384, 256)


def fetch(sources, bufs, first_row, sems):
    copies = [
        pltpu.make_async_copy(src.at[pl.ds(pl.multiple_of(first_row, 1024), 1024), :], buf, sems.at[i])
        for i, (src, buf) in enumerate(zip(sources, bufs))
    ]
    for copy in copies:
        copy.start()
    return copies


def own_kernel(*refs):
    own_ref, gain_ref = refs[:2]
    sources, normed_ref, squares_ref, partials = refs[2:8], refs[8], refs[9], refs[10:16]
    bufs, sems = refs[16:22], refs[22]
    tp = lax.axis_index("tp")
    copies = fetch(sources, bufs, tp * 1024, sems)
    own = own_ref[...].astype(f32)
    normed = (own * jnp.where(tp == 0, gain_ref[:, :1024], gain_ref[:, 1024:])).astype(bf16)
    normed_ref[...] = normed
    squares_ref[...] = jnp.broadcast_to(jnp.sum(own * own, axis=1, keepdims=True), (256, 128))
    for copy, buf, partial in zip(copies, bufs, partials):
        copy.wait()
        partial[...] = dot(normed, buf[...])


def local_kernel(*refs):
    other_ref, gain_ref, squares_ref, db_ref, rb_ref = refs[:5]
    partials, sources = refs[5:11], refs[11:17]
    (
        normed_ref, scale_ref, pool_ref, home_ref, first_ref, second_ref, third_ref,
        wb_ref, wkk_ref, solved_ref, v_ref, rho_ref,
    ) = refs[17:29]
    k_s, d_s, a_s, r_s, v_s, maps = refs[29:35]
    bufs, sems = refs[35:41], refs[41]
    tp = lax.axis_index("tp")
    y = lax.axis_index("sp_1")
    copies = fetch(sources, bufs, (1 - tp) * 1024, sems)
    is_first = tp == 0
    other = other_ref[...].astype(f32)
    normed = (other * jnp.where(is_first, gain_ref[:, 1024:], gain_ref[:, :1024])).astype(bf16)
    normed_ref[...] = normed
    squares = squares_ref[:, :1] + jnp.sum(other * other, axis=1, keepdims=True)
    scale = lax.rsqrt(squares * (1.0 / D) + 0.25)
    scale_ref[...] = jnp.broadcast_to(scale, (256, 128))
    for i in range(6):
        copies[i].wait()
        rounded = ((partials[i][...] + dot(normed, bufs[i][...])) * scale).astype(bf16)
        if i == 5:
            pool_ref[...] = rounded
            for s in (0, 1):
                for half in (0, 1):
                    at = 256 + (2 * s + half) * 16
                    first_ref[at : at + 16] = rounded[
                        s * 128 + 112 : s * 128 + 128, half * 128 : half * 128 + 128
                    ]
            continue
        dest = (k_s, d_s, a_s, r_s, v_s)[i]
        for u in range(UNITS):
            s, h = u // 3, u % 3
            dest[u] = rounded[s * 128 : s * 128 + 128, h * 128 : h * 128 + 128].astype(f32)

    masks = head_masks()
    n = SPAN
    row, col = iota(n, n, 0), iota(n, n, 1)
    strict, inclusive = row > col, row >= col
    triangle = inclusive.astype(f32)
    ones = ((row >> 6) == (col >> 6)).astype(f32)
    wide = (
        jnp.concatenate([masks[0], masks[0]], axis=1),
        jnp.concatenate([masks[1], masks[1]], axis=1),
    )
    slab = iota(HEAD, 128, 0)
    eye = (slab == (iota(HEAD, 128, 1) & 63)).astype(f32)
    units = range(UNITS)
    lowers, alphas, keeps = [], [], []
    for u in units:
        h = u % 3
        lanes = slice(h * 128, h * 128 + 128)
        shifted = slice(384 + h * 128, 384 + h * 128 + 128)
        db = jnp.where(is_first, line_of(db_ref, lanes), line_of(db_ref, shifted))
        rb = jnp.where(is_first, line_of(rb_ref, lanes), line_of(rb_ref, shifted))
        k = k_s[u]
        log_decay = -0.6065306597126334 * jax.nn.sigmoid(db + d_s[u])
        rate = jax.nn.sigmoid(rb + a_s[u])
        unit_key = k * lax.rsqrt(dot_fine_left(k * k, ones) + 1.0)
        removal = unit_key * rate
        total = dot_fine_right(triangle, log_decay)
        middle, final = total[63:64], total[127:128]
        alpha = jnp.exp(total - log_decay - middle) * unit_key
        fading = jnp.exp(middle - total)
        beta, kappa = removal * fading, k * fading
        rho = r_s[u] * jnp.exp(total - middle)
        ending = jnp.exp(final - total)
        lift = jnp.exp(middle)
        rho_ref[u] = rho * lift
        left = jnp.concatenate([alpha * masks[0], alpha * masks[1], rho * masks[0], rho * masks[1]], axis=0)
        pairs = dot(left, jnp.concatenate([beta, kappa], axis=0), NT)
        lower_kappa = []
        for j in (0, 1):
            lowers.append(jnp.where(strict, pairs[j * n : j * n + n, :n], 0.0))
            lower_kappa.append(jnp.where(strict, pairs[j * n : j * n + n, n:], 0.0).astype(bf16))
            wb_ref[u, :, j * n : j * n + n] = jnp.where(
                inclusive, pairs[(2 + j) * n : (3 + j) * n, :n], 0.0
            ).astype(bf16)
            wkk_ref[u, :, j * n : j * n + n] = jnp.where(
                inclusive, pairs[(2 + j) * n : (3 + j) * n, n:], 0.0
            ).astype(bf16)
        v = v_s[u]
        v_ref[u] = v.astype(bf16)
        carried = dot(jnp.concatenate(lower_kappa, axis=1), both(v, masks))
        keeps.append((alpha * lift, carried, removal * ending, k * ending, jnp.exp(final)))
    inverse = inverses(lowers)
    for u in units:
        alpha, carried, beta_end, kappa_end, gain_end = keeps[u]
        right = jnp.concatenate([alpha, carried], axis=1)
        solved = dot(jnp.concatenate(inverse[2 * u : 2 * u + 2], axis=1), both(right, wide))
        solved_ref[u] = solved.astype(bf16)
        crossed = dot(solved[:, :n], beta_end, TN)
        transit = eye * gain_end - (crossed[:HEAD] * masks[0] + crossed[HEAD:] * masks[1])
        crossed = dot(
            jnp.concatenate([v_s[u], -solved[:, n:]], axis=0),
            jnp.concatenate([kappa_end, beta_end], axis=0),
            TN,
        )
        written = crossed[:HEAD] * masks[0] + crossed[HEAD:] * masks[1]
        at = (u // 3) * 128
        maps[u % 3, at : at + HEAD] = transit.astype(bf16)
        maps[u % 3, at + HEAD : at + 128] = written.astype(bf16)
    maps[3] = jnp.zeros((256, 128), bf16)
    for step, dest in enumerate((home_ref, first_ref, second_ref, third_ref)):
        dest[:256] = maps[(y + step) & 3]


def side_kernel(
    own_ref, other_ref, scale_ref, wb_ref, wkk_ref, solved_ref, v_ref, rho_ref, wg_ref, wq_ref,
    reads_ref, local_ref, gate_ref, pgate_ref,
):
    tp = lax.axis_index("tp")
    masks = head_masks()
    wide = (
        jnp.concatenate([masks[0], masks[0]], axis=1),
        jnp.concatenate([masks[1], masks[1]], axis=1),
    )
    for u in range(UNITS):
        removed = dot(wb_ref[u], both(solved_ref[u].astype(f32), wide))
        reads_ref[u] = (rho_ref[u] - removed[:, :128]).astype(bf16)
        local_ref[u] = dot(wkk_ref[u], both(v_ref[u].astype(f32), masks)) - removed[:, 128:]
    scale = scale_ref[:, :1]
    mine, theirs = pl.multiple_of(tp * 1024, 1024), pl.multiple_of((1 - tp) * 1024, 1024)
    for weight, dest in ((wg_ref, gate_ref), (wq_ref, pgate_ref)):
        total = dot(own_ref[...], weight[pl.ds(mine, 1024), :])
        total = total + dot(other_ref[...], weight[pl.ds(theirs, 1024), :])
        dest[...] = (total * scale).astype(bf16)


def row_kernel(home_ref, first_ref, second_ref, third_ref, after_ref, prefix_ref, next_ref, total_ref, maps):
    y = lax.axis_index("sp_1")
    for step, src in enumerate((home_ref, first_ref, second_ref, third_ref)):
        maps[(y + 4 - step) & 3] = src[:256]
    next_ref[256:] = first_ref[256:]
    masks = head_masks()
    for s in (0, 1):
        rows = slice(s * 128, s * 128 + 128)
        so_far = maps[0, rows].astype(f32)
        prefix_ref[0, s] = so_far
        for j in (1, 2, 3):
            so_far = compose(so_far, maps[j, rows], masks)
            if j < 3:
                prefix_ref[j, s] = so_far
            else:
                next_ref[rows] = so_far.astype(bf16)
                total_ref[rows] = so_far.astype(bf16)


def column_kernel(
    prefix_ref, first_ref, second_ref, third_ref, init_ref,
    home_ref, one_ref, two_ref, three_ref,
    starts, rows,
):
    y = lax.axis_index("sp_1")
    z = lax.axis_index("sp_0")
    for step, src in enumerate((first_ref, second_ref, third_ref)):
        rows[(z + 3 - step) & 3] = src[:256]
    masks = head_masks()
    pair = jnp.minimum(y, 2) * 2
    for s in (0, 1):
        state = jnp.concatenate([init_ref[s, pair], init_ref[s, pair + 1]], axis=1)
        for j in range(3):
            state = jnp.where(j < z, compose(state, rows[j, s * 128 : s * 128 + 128], masks), state)
        starts[0, s] = state.astype(bf16)
        for j in range(3):
            starts[j + 1, s] = compose(state, prefix_ref[j, s], masks).astype(bf16)
    for step, dest in enumerate((home_ref, one_ref, two_ref, three_ref)):
        dest[...] = starts[(y + step) & 3]


def pool_kernel(pool_ref, beside_ref, above_ref, pgate_ref, mix_ref, pscale_ref, out_ref):
    tp = lax.axis_index("tp")
    y = lax.axis_index("sp_1")
    place = lax.axis_index("sp_0") * 4 + y
    is_first = tp == 0
    factor = jnp.where(is_first, pscale_ref[:, :256], pscale_ref[:, 256:])
    for s in (0, 1):
        current = pool_ref[s * 128 : s * 128 + 128].astype(f32)
        tails = []
        for half in (0, 1):
            rows = slice(256 + (2 * s + half) * 16, 272 + (2 * s + half) * 16)
            tails.append(
                jnp.where(
                    place == 0,
                    0.0,
                    jnp.where(y > 0, beside_ref[rows].astype(f32), above_ref[rows].astype(f32)),
                )
            )
        padded = jnp.concatenate([jnp.concatenate(tails, axis=1), current], axis=0)
        sums = {1: padded}
        for by in (1, 2, 4, 8):
            before = sums[by]
            moved = jnp.concatenate([jnp.zeros((by, 256), f32), before[: 144 - by]], axis=0)
            sums[2 * by] = before + moved
        position = (place * 128 + iota(128, 128, 0) + 1).astype(f32)
        for g in (0, 1):
            lanes = slice(g * 128, g * 128 + 128)
            small, large = 2 << g, 8 << g
            trailing = jnp.where(is_first, sums[small][16:, lanes], sums[large][16:, lanes])
            window = jnp.where(is_first, float(small), float(large))
            diffs = trailing / jnp.minimum(position, window) - current[:, lanes]
            mixed = dot(diffs.astype(bf16), mix_ref[tp * 2 + g])
            gate = pgate_ref[s * 128 : s * 128 + 128, lanes].astype(f32)
            out_ref[s * 128 : s * 128 + 128, lanes] = (
                mixed * factor[:, lanes] * (gate * jax.nn.sigmoid(gate))
            ).astype(bf16)


def final_kernel(
    home_ref, one_ref, two_ref, three_ref, reads_ref, local_ref, gate_ref, hgain_ref, pool_ref,
    wr_ref, wp_ref,
    send_ref, keep_ref,
    starts, rec,
):
    tp = lax.axis_index("tp")
    y = lax.axis_index("sp_1")
    for step, src in enumerate((home_ref, one_ref, two_ref, three_ref)):
        starts[(y + 4 - step) & 3] = src[...]
    masks = head_masks()
    row, col = iota(128, 128, 0), iota(128, 128, 1)
    mean_of = jnp.where((row >> 6) == (col >> 6), 1.0 / HEAD, 0.0).astype(bf16)
    is_first = tp == 0
    for u in range(UNITS):
        s, h = u // 3, u % 3
        lanes = slice(h * 128, h * 128 + 128)
        shifted = slice(384 + h * 128, 384 + h * 128 + 128)
        rows = slice(s * 128, s * 128 + 128)
        out = dot(reads_ref[u], both(starts[h, s].astype(f32), masks), NT) + local_ref[u]
        out = out - dot_fine_left(out, mean_of)
        spread = dot_fine_left(out * out, mean_of)
        gain = jnp.where(is_first, line_of(hgain_ref, lanes), line_of(hgain_ref, shifted))
        gate = gate_ref[rows, lanes].astype(f32)
        rec[rows, lanes] = (
            out * lax.rsqrt(spread + 1.0) * gain * (gate * jax.nn.sigmoid(gate))
        ).astype(bf16)
    for dest, part in ((send_ref, 1 - tp), (keep_ref, tp)):
        cols = pl.ds(pl.multiple_of(part * 1024, 1024), 1024)
        dest[...] = (dot(rec[...], wr_ref[:, cols]) + dot(pool_ref[...], wp_ref[:, cols])).astype(bf16)


def vmem(count):
    return [pl.BlockSpec(memory_space=pltpu.VMEM)] * count


def hbm(count):
    return [pl.BlockSpec(memory_space=pltpu.HBM)] * count


def shape(dims, kind=bf16):
    return jax.ShapeDtypeStruct(dims, kind)


def call(body, name, ins, outs, scratch, limit, flops=0):
    return pl.pallas_call(
        body,
        name=name,
        out_shape=outs,
        in_specs=ins,
        out_specs=vmem(len(outs)) if isinstance(outs, (list, tuple)) else vmem(1)[0],
        scratch_shapes=scratch,
        compiler_params=pltpu.CompilerParams(vmem_limit_bytes=limit * MIB),
        cost_estimate=pl.CostEstimate(flops=flops, transcendentals=0, bytes_accessed=0) if flops else None,
    )


def around(parts, axis):
    return [
        lax.ppermute(part, axis, [(i, (i + step) & 3) for i in range(4)]) for step, part in enumerate(parts, 1)
    ]


def shards(
    tokens, norm_gain, w_recept, w_key, w_value, w_decay, w_rate, w_gate_rec, w_pool, w_gate_pool,
    decay_base, rate_base, head_gain, pool_mix, pool_scale, w_out_rec, w_out_pool, init_state,
):
    other = lax.ppermute(tokens, "tp", [(0, 1), (1, 0)])
    line = lambda x: x.reshape(1, -1)
    weights = (w_key, w_decay, w_rate, w_recept, w_value, w_pool)
    bufs = [pltpu.VMEM((1024, width), bf16) for width in WIDTHS] + [pltpu.SemaphoreType.DMA((6,))]
    own_normed, squares, *partials = call(
        own_kernel,
        "own",
        vmem(2) + hbm(6),
        [shape((256, 1024)), shape((256, 128), f32)] + [shape((256, width), f32) for width in WIDTHS],
        bufs,
        20,
        1_000_000_000,
    )(tokens.reshape(256, 1024), line(norm_gain), *weights)
    normed, scale, pool, home, m1, m2, m3, wb, wkk, solved, v, rho = call(
        local_kernel,
        "local",
        vmem(11) + hbm(6),
        [
            shape((256, 1024)), shape((256, 128), f32), shape((256, 256)),
            shape((256, 128)), shape((320, 128)), shape((256, 128)), shape((256, 128)),
            shape((6, 128, 256)), shape((6, 128, 256)), shape((6, 128, 256)),
            shape((6, 128, 128)), shape((6, 128, 128), f32),
        ],
        [pltpu.VMEM((6, 128, 128), f32)] * 5 + [pltpu.VMEM((4, 256, 128), bf16)] + bufs,
        30,
        3_000_000_000,
    )(other.reshape(256, 1024), line(norm_gain), squares, decay_base, rate_base, *partials, *weights)
    r1, r2, r3 = around((m1, m2, m3), "sp_1")
    reads, local, gate, pgate = call(
        side_kernel,
        "side",
        vmem(10),
        [shape((6, 128, 128)), shape((6, 128, 128), f32), shape((256, 384)), shape((256, 256))],
        [],
        16,
        1_000_000_000,
    )(own_normed, normed, scale, wb, wkk, solved, v, rho, w_gate_rec, w_gate_pool)
    prefix, onward, total = call(
        row_kernel,
        "row",
        vmem(4) + [pl.BlockSpec(memory_space=pl.ANY)],
        [shape((3, 2, 128, 128), f32), shape((320, 128)), shape((256, 128))],
        [pltpu.VMEM((4, 256, 128), bf16)],
        8,
        100_000_000,
    )(home, r1, r2, r3, pgate)
    columns = around((onward, total, total), "sp_0")
    s0, s1, s2, s3 = call(
        column_kernel,
        "column",
        vmem(5),
        [shape((2, 64, 128))] * 4,
        [pltpu.VMEM((4, 2, 64, 128), bf16), pltpu.VMEM((4, 256, 128), bf16)],
        8,
        100_000_000,
    )(prefix, *columns, init_state)
    t1, t2, t3 = around((s1, s2, s3), "sp_1")
    pool_out = call(pool_kernel, "pool", vmem(6), shape((256, 256)), [], 8, 100_000_000)(
        pool, r1, columns[0], pgate, pool_mix, line(pool_scale)
    )
    send, keep = call(
        final_kernel,
        "final",
        vmem(11),
        [shape((256, 1024)), shape((256, 1024))],
        [pltpu.VMEM((4, 2, 64, 128), bf16), pltpu.VMEM((256, 384), bf16)],
        20,
        1_000_000_000,
    )(s0, t1, t2, t3, reads, local, gate, head_gain, pool_out, w_out_rec, w_out_pool)
    arrived = lax.ppermute(send, "tp", [(0, 1), (1, 0)])
    mixed = keep.astype(f32) + arrived.astype(f32)
    return mixed.astype(bf16).reshape(2, 128, 1024)


def solution(mesh):
    split = Mesh(
        mesh.devices.reshape(4, 4, mesh.shape["fs"], mesh.shape["tp"]), ("sp_0", "sp_1", "fs", "tp")
    )
    column = P(None, "tp")
    placed = (
        (P("fs", SP, "tp"), P()) + (column,) * 8 + (P(),) * 5
        + (P("tp", None), P("tp", None), P("fs", "tp", None, None))
    )
    return jax.shard_map(
        shards, mesh=split, in_specs=placed, out_specs=P("fs", SP, "tp"), check_vma=False
    )
```

```python
import functools

import jax
import jax.numpy as jnp
from jax import lax
from jax.experimental import pallas as pl
from jax.experimental.pallas import tpu as pltpu
from jax.sharding import Mesh
from jax.sharding import PartitionSpec as P

D = 2048
HEAD = 64
SPAN = 128
UNITS = 6
SP = ("sp_0", "sp_1")
f32 = jnp.float32
bf16 = jnp.bfloat16
NN = ((1,), (0,))
NT = ((1,), (1,))
TN = ((0,), (0,))
MIB = 2**20


def dot(a, b, dims=NN):
    return lax.dot_general(
        a.astype(bf16), b.astype(bf16), (dims, ((), ())), preferred_element_type=f32
    )


def halves(x):
    high = x.astype(bf16)
    return high, (x - high.astype(f32)).astype(bf16)


def dot_fine_left(a, b, dims=NN):
    high, low = halves(a)
    return dot(high, b, dims) + dot(low, b, dims)


def dot_fine_right(a, b, dims=NN):
    high, low = halves(b)
    return dot(a, high, dims) + dot(a, low, dims)


def iota(rows, cols, dim):
    return lax.broadcasted_iota(jnp.int32, (rows, cols), dim)


def line_of(ref, lanes):
    if len(ref.shape) == 1:
        return ref[lanes].reshape(1, 128)
    return ref[:, lanes]


def head_masks():
    first = (iota(1, 128, 1) < HEAD).astype(f32)
    return first, 1.0 - first


def both(x, masks):
    return jnp.concatenate([x * masks[0], x * masks[1]], axis=0)


def compose(earlier, later, masks):
    moved = dot_fine_left(earlier, both(later[:HEAD].astype(f32), masks))
    written = later[HEAD:].astype(f32)
    if earlier.shape[0] == HEAD:
        return moved + written
    return jnp.concatenate([moved[:HEAD], moved[HEAD:] + written], axis=0)


def pick(x, size, odd):
    parts = [x[s : s + size] for s in range(size * odd, SPAN, 2 * size)]
    return parts[0] if len(parts) == 1 else jnp.concatenate(parts, axis=0)


def weave(even, odd, size):
    parts = []
    for s in range(0, SPAN // 2, size):
        parts += [even[s : s + size], odd[s : s + size]]
    return jnp.concatenate(parts, axis=0)


def inverses(lowers):
    row, col = iota(SPAN, SPAN, 0), iota(SPAN, SPAN, 1)
    eye = (row == col).astype(f32)
    near = ((row >> 1) == (col >> 1)).astype(f32)
    result = [eye - lower * near for lower in lowers]
    size, level = 2, 1
    while size < SPAN:
        off = (((row >> (level + 1)) == (col >> (level + 1))) & ((row >> level) != (col >> level))).astype(f32)
        if size < 8:
            inner = [dot(lower * off, inv) for lower, inv in zip(lowers, result)]
            result = [inv - dot(inv, part) for inv, part in zip(result, inner)]
        else:
            off = pick(off, size, 1)
            inner = [dot(pick(lower, size, 1) * off, inv) for lower, inv in zip(lowers, result)]
            outer = [
                dot(pick(inv, size, 1), weave(jnp.zeros_like(part), part, size))
                for inv, part in zip(result, inner)
            ]
            result = [
                weave(pick(inv, size, 0), pick(inv, size, 1) - part, size)
                for inv, part in zip(result, outer)
            ]
        size, level = size * 2, level + 1
    return result


WIDTHS = (384, 384, 384, 384, 384, 256)


def fetch(sources, bufs, first_row, sems):
    copies = [
        pltpu.make_async_copy(src.at[pl.ds(pl.multiple_of(first_row, 1024), 1024), :], buf, sems.at[i])
        for i, (src, buf) in enumerate(zip(sources, bufs))
    ]
    for copy in copies:
        copy.start()
    return copies


def own_kernel(*refs):
    token_ref, norm_ref = refs[:2]
    sources, normed_ref, squares_ref, partials = refs[2:8], refs[8], refs[9], refs[10:16]
    bufs, sems, own_ref, gain_ref, first_sems = refs[16:22], refs[22], refs[23], refs[24], refs[25]
    tp = lax.axis_index("tp")
    early = [
        pltpu.make_async_copy(token_ref, own_ref, first_sems.at[0]),
        pltpu.make_async_copy(norm_ref, gain_ref, first_sems.at[1]),
    ]
    for copy in early:
        copy.start()
    copies = fetch(sources, bufs, tp * 1024, sems)
    for copy in early:
        copy.wait()
    own = own_ref[...].astype(f32)
    normed = (own * jnp.where(tp == 0, gain_ref[:, :1024], gain_ref[:, 1024:])).astype(bf16)
    normed_ref[...] = normed
    squares_ref[...] = jnp.broadcast_to(jnp.sum(own * own, axis=1, keepdims=True), (256, 128))
    for copy, buf, partial in zip(copies, bufs, partials):
        copy.wait()
        partial[...] = dot(normed, buf[...])


def local_kernel(*refs):
    other_ref, gain_ref, squares_ref, db_ref, rb_ref = refs[:5]
    partials, sources = refs[5:11], refs[11:17]
    (
        normed_ref, scale_ref, pool_ref, home_ref, first_ref, second_ref, third_ref,
        wb_ref, wkk_ref, solved_ref, v_ref, rho_ref,
    ) = refs[17:29]
    k_s, d_s, a_s, r_s, v_s, maps = refs[29:35]
    bufs, sems = refs[35:41], refs[41]
    tp = lax.axis_index("tp")
    y = lax.axis_index("sp_1")
    copies = fetch(sources, bufs, (1 - tp) * 1024, sems)
    is_first = tp == 0
    other = other_ref[...].astype(f32)
    normed = (other * jnp.where(is_first, gain_ref[:, 1024:], gain_ref[:, :1024])).astype(bf16)
    normed_ref[...] = normed
    squares = squares_ref[:, :1] + jnp.sum(other * other, axis=1, keepdims=True)
    scale = lax.rsqrt(squares * (1.0 / D) + 0.25)
    scale_ref[...] = jnp.broadcast_to(scale, (256, 128))
    for i in range(6):
        copies[i].wait()
        rounded = ((partials[i][...] + dot(normed, bufs[i][...])) * scale).astype(bf16)
        if i == 5:
            pool_ref[...] = rounded
            for s in (0, 1):
                for half in (0, 1):
                    at = 256 + (2 * s + half) * 16
                    first_ref[at : at + 16] = rounded[
                        s * 128 + 112 : s * 128 + 128, half * 128 : half * 128 + 128
                    ]
            continue
        dest = (k_s, d_s, a_s, r_s, v_s)[i]
        for u in range(UNITS):
            s, h = u // 3, u % 3
            dest[u] = rounded[s * 128 : s * 128 + 128, h * 128 : h * 128 + 128].astype(f32)

    masks = head_masks()
    n = SPAN
    row, col = iota(n, n, 0), iota(n, n, 1)
    strict, inclusive = row > col, row >= col
    triangle = inclusive.astype(f32)
    ones = ((row >> 6) == (col >> 6)).astype(f32)
    wide = (
        jnp.concatenate([masks[0], masks[0]], axis=1),
        jnp.concatenate([masks[1], masks[1]], axis=1),
    )
    slab = iota(HEAD, 128, 0)
    eye = (slab == (iota(HEAD, 128, 1) & 63)).astype(f32)
    units = range(UNITS)
    lowers, alphas, keeps = [], [], []
    for u in units:
        h = u % 3
        lanes = slice(h * 128, h * 128 + 128)
        shifted = slice(384 + h * 128, 384 + h * 128 + 128)
        db = jnp.where(is_first, line_of(db_ref, lanes), line_of(db_ref, shifted))
        rb = jnp.where(is_first, line_of(rb_ref, lanes), line_of(rb_ref, shifted))
        k = k_s[u]
        log_decay = -0.6065306597126334 * jax.nn.sigmoid(db + d_s[u])
        rate = jax.nn.sigmoid(rb + a_s[u])
        unit_key = k * lax.rsqrt(dot_fine_left(k * k, ones) + 1.0)
        removal = unit_key * rate
        total = dot_fine_right(triangle, log_decay)
        middle, final = total[63:64], total[127:128]
        alpha = jnp.exp(total - log_decay - middle) * unit_key
        fading = jnp.exp(middle - total)
        beta, kappa = removal * fading, k * fading
        rho = r_s[u] * jnp.exp(total - middle)
        ending = jnp.exp(final - total)
        lift = jnp.exp(middle)
        rho_ref[u] = rho * lift
        left = jnp.concatenate([alpha * masks[0], alpha * masks[1], rho * masks[0], rho * masks[1]], axis=0)
        pairs = dot(left, jnp.concatenate([beta, kappa], axis=0), NT)
        lower_kappa = []
        for j in (0, 1):
            lowers.append(jnp.where(strict, pairs[j * n : j * n + n, :n], 0.0))
            lower_kappa.append(jnp.where(strict, pairs[j * n : j * n + n, n:], 0.0).astype(bf16))
            wb_ref[u, :, j * n : j * n + n] = jnp.where(
                inclusive, pairs[(2 + j) * n : (3 + j) * n, :n], 0.0
            ).astype(bf16)
            wkk_ref[u, :, j * n : j * n + n] = jnp.where(
                inclusive, pairs[(2 + j) * n : (3 + j) * n, n:], 0.0
            ).astype(bf16)
        v = v_s[u]
        v_ref[u] = v.astype(bf16)
        carried = dot(jnp.concatenate(lower_kappa, axis=1), both(v, masks))
        keeps.append((alpha * lift, carried, removal * ending, k * ending, jnp.exp(final)))
    inverse = inverses(lowers)
    for u in units:
        alpha, carried, beta_end, kappa_end, gain_end = keeps[u]
        right = jnp.concatenate([alpha, carried], axis=1)
        solved = dot(jnp.concatenate(inverse[2 * u : 2 * u + 2], axis=1), both(right, wide))
        solved_ref[u] = solved.astype(bf16)
        crossed = dot(solved[:, :n], beta_end, TN)
        transit = eye * gain_end - (crossed[:HEAD] * masks[0] + crossed[HEAD:] * masks[1])
        crossed = dot(
            jnp.concatenate([v_s[u], -solved[:, n:]], axis=0),
            jnp.concatenate([kappa_end, beta_end], axis=0),
            TN,
        )
        written = crossed[:HEAD] * masks[0] + crossed[HEAD:] * masks[1]
        at = (u // 3) * 128
        maps[u % 3, at : at + HEAD] = transit.astype(bf16)
        maps[u % 3, at + HEAD : at + 128] = written.astype(bf16)
    maps[3] = jnp.zeros((256, 128), bf16)
    for step, dest in enumerate((home_ref, first_ref, second_ref, third_ref)):
        dest[:256] = maps[(y + step) & 3]


def side_kernel(
    own_ref, other_ref, scale_ref, wb_ref, wkk_ref, solved_ref, v_ref, rho_ref, wg_ref, wq_ref,
    reads_ref, local_ref, gate_ref, pgate_ref,
):
    tp = lax.axis_index("tp")
    masks = head_masks()
    wide = (
        jnp.concatenate([masks[0], masks[0]], axis=1),
        jnp.concatenate([masks[1], masks[1]], axis=1),
    )
    for u in range(UNITS):
        removed = dot(wb_ref[u], both(solved_ref[u].astype(f32), wide))
        reads_ref[u] = (rho_ref[u] - removed[:, :128]).astype(bf16)
        local_ref[u] = dot(wkk_ref[u], both(v_ref[u].astype(f32), masks)) - removed[:, 128:]
    scale = scale_ref[:, :1]
    mine, theirs = pl.multiple_of(tp * 1024, 1024), pl.multiple_of((1 - tp) * 1024, 1024)
    for weight, dest in ((wg_ref, gate_ref), (wq_ref, pgate_ref)):
        total = dot(own_ref[...], weight[pl.ds(mine, 1024), :])
        total = total + dot(other_ref[...], weight[pl.ds(theirs, 1024), :])
        dest[...] = (total * scale).astype(bf16)


def row_kernel(home_ref, first_ref, second_ref, third_ref, after_ref, prefix_ref, next_ref, total_ref, maps):
    y = lax.axis_index("sp_1")
    for step, src in enumerate((home_ref, first_ref, second_ref, third_ref)):
        maps[(y + 4 - step) & 3] = src[:256]
    next_ref[256:] = first_ref[256:]
    masks = head_masks()
    for s in (0, 1):
        rows = slice(s * 128, s * 128 + 128)
        so_far = maps[0, rows].astype(f32)
        prefix_ref[0, s] = so_far
        for j in (1, 2, 3):
            so_far = compose(so_far, maps[j, rows], masks)
            if j < 3:
                prefix_ref[j, s] = so_far
            else:
                next_ref[rows] = so_far.astype(bf16)
                total_ref[rows] = so_far.astype(bf16)


def column_kernel(
    prefix_ref, first_ref, second_ref, third_ref, init_ref,
    home_ref, one_ref, two_ref, three_ref,
    starts, rows,
):
    y = lax.axis_index("sp_1")
    z = lax.axis_index("sp_0")
    for step, src in enumerate((first_ref, second_ref, third_ref)):
        rows[(z + 3 - step) & 3] = src[:256]
    masks = head_masks()
    pair = jnp.minimum(y, 2) * 2
    for s in (0, 1):
        state = jnp.concatenate([init_ref[s, pair], init_ref[s, pair + 1]], axis=1)
        for j in range(3):
            state = jnp.where(j < z, compose(state, rows[j, s * 128 : s * 128 + 128], masks), state)
        starts[0, s] = state.astype(bf16)
        for j in range(3):
            starts[j + 1, s] = compose(state, prefix_ref[j, s], masks).astype(bf16)
    for step, dest in enumerate((home_ref, one_ref, two_ref, three_ref)):
        dest[...] = starts[(y + step) & 3]


def pool_kernel(pool_ref, beside_ref, above_ref, pgate_ref, mix_ref, pscale_ref, out_ref):
    tp = lax.axis_index("tp")
    y = lax.axis_index("sp_1")
    place = lax.axis_index("sp_0") * 4 + y
    is_first = tp == 0
    factor = jnp.where(is_first, pscale_ref[:, :256], pscale_ref[:, 256:])
    for s in (0, 1):
        current = pool_ref[s * 128 : s * 128 + 128].astype(f32)
        tails = []
        for half in (0, 1):
            rows = slice(256 + (2 * s + half) * 16, 272 + (2 * s + half) * 16)
            tails.append(
                jnp.where(
                    place == 0,
                    0.0,
                    jnp.where(y > 0, beside_ref[rows].astype(f32), above_ref[rows].astype(f32)),
                )
            )
        padded = jnp.concatenate([jnp.concatenate(tails, axis=1), current], axis=0)
        sums = {1: padded}
        for by in (1, 2, 4, 8):
            before = sums[by]
            moved = jnp.concatenate([jnp.zeros((by, 256), f32), before[: 144 - by]], axis=0)
            sums[2 * by] = before + moved
        position = (place * 128 + iota(128, 128, 0) + 1).astype(f32)
        for g in (0, 1):
            lanes = slice(g * 128, g * 128 + 128)
            small, large = 2 << g, 8 << g
            trailing = jnp.where(is_first, sums[small][16:, lanes], sums[large][16:, lanes])
            window = jnp.where(is_first, float(small), float(large))
            diffs = trailing / jnp.minimum(position, window) - current[:, lanes]
            mixed = dot(diffs.astype(bf16), mix_ref[tp * 2 + g])
            gate = pgate_ref[s * 128 : s * 128 + 128, lanes].astype(f32)
            out_ref[s * 128 : s * 128 + 128, lanes] = (
                mixed * factor[:, lanes] * (gate * jax.nn.sigmoid(gate))
            ).astype(bf16)


def final_kernel(
    home_ref, one_ref, two_ref, three_ref, reads_ref, local_ref, gate_ref, hgain_ref, pool_ref,
    wr_ref, wp_ref,
    send_ref, keep_ref,
    starts, rec,
):
    tp = lax.axis_index("tp")
    y = lax.axis_index("sp_1")
    for step, src in enumerate((home_ref, one_ref, two_ref, three_ref)):
        starts[(y + 4 - step) & 3] = src[...]
    masks = head_masks()
    row, col = iota(128, 128, 0), iota(128, 128, 1)
    mean_of = jnp.where((row >> 6) == (col >> 6), 1.0 / HEAD, 0.0).astype(bf16)
    is_first = tp == 0
    for u in range(UNITS):
        s, h = u // 3, u % 3
        lanes = slice(h * 128, h * 128 + 128)
        shifted = slice(384 + h * 128, 384 + h * 128 + 128)
        rows = slice(s * 128, s * 128 + 128)
        out = dot(reads_ref[u], both(starts[h, s].astype(f32), masks), NT) + local_ref[u]
        out = out - dot_fine_left(out, mean_of)
        spread = dot_fine_left(out * out, mean_of)
        gain = jnp.where(is_first, line_of(hgain_ref, lanes), line_of(hgain_ref, shifted))
        gate = gate_ref[rows, lanes].astype(f32)
        rec[rows, lanes] = (
            out * lax.rsqrt(spread + 1.0) * gain * (gate * jax.nn.sigmoid(gate))
        ).astype(bf16)
    for dest, part in ((send_ref, 1 - tp), (keep_ref, tp)):
        cols = pl.ds(pl.multiple_of(part * 1024, 1024), 1024)
        dest[...] = (dot(rec[...], wr_ref[:, cols]) + dot(pool_ref[...], wp_ref[:, cols])).astype(bf16)


def vmem(count):
    return [pl.BlockSpec(memory_space=pltpu.VMEM)] * count


def hbm(count):
    return [pl.BlockSpec(memory_space=pltpu.HBM)] * count


def shape(dims, kind=bf16):
    return jax.ShapeDtypeStruct(dims, kind)


def call(body, name, ins, outs, scratch, limit, flops=0):
    return pl.pallas_call(
        body,
        name=name,
        out_shape=outs,
        in_specs=ins,
        out_specs=vmem(len(outs)) if isinstance(outs, (list, tuple)) else vmem(1)[0],
        scratch_shapes=scratch,
        compiler_params=pltpu.CompilerParams(vmem_limit_bytes=limit * MIB),
        cost_estimate=pl.CostEstimate(flops=flops, transcendentals=0, bytes_accessed=0) if flops else None,
    )


def around(parts, axis):
    return [
        lax.ppermute(part, axis, [(i, (i + step) & 3) for i in range(4)]) for step, part in enumerate(parts, 1)
    ]


def shards(
    tokens, norm_gain, w_recept, w_key, w_value, w_decay, w_rate, w_gate_rec, w_pool, w_gate_pool,
    decay_base, rate_base, head_gain, pool_mix, pool_scale, w_out_rec, w_out_pool, init_state,
):
    other = lax.ppermute(tokens, "tp", [(0, 1), (1, 0)])
    line = lambda x: x.reshape(1, -1)
    pinned = lambda x: pltpu.with_memory_space_constraint(x, pltpu.HBM)
    weights = [pinned(w) for w in (w_key, w_decay, w_rate, w_recept, w_value, w_pool)]
    bufs = [pltpu.VMEM((1024, width), bf16) for width in WIDTHS] + [pltpu.SemaphoreType.DMA((6,))]
    own_normed, squares, *partials = call(
        own_kernel,
        "own",
        hbm(8),
        [shape((256, 1024)), shape((256, 128), f32)] + [shape((256, width), f32) for width in WIDTHS],
        bufs + [pltpu.VMEM((256, 1024), bf16), pltpu.VMEM((1, D), f32), pltpu.SemaphoreType.DMA((2,))],
        20,
        1_000_000_000,
    )(pinned(tokens.reshape(256, 1024)), pinned(line(norm_gain)), *weights)
    normed, scale, pool, home, m1, m2, m3, wb, wkk, solved, v, rho = call(
        local_kernel,
        "local",
        vmem(11) + hbm(6),
        [
            shape((256, 1024)), shape((256, 128), f32), shape((256, 256)),
            shape((256, 128)), shape((320, 128)), shape((256, 128)), shape((256, 128)),
            shape((6, 128, 256)), shape((6, 128, 256)), shape((6, 128, 256)),
            shape((6, 128, 128)), shape((6, 128, 128), f32),
        ],
        [pltpu.VMEM((6, 128, 128), f32)] * 5 + [pltpu.VMEM((4, 256, 128), bf16)] + bufs,
        30,
        3_000_000_000,
    )(other.reshape(256, 1024), line(norm_gain), squares, decay_base, rate_base, *partials, *weights)
    r1, r2, r3 = around((m1, m2, m3), "sp_1")
    reads, local, gate, pgate = call(
        side_kernel,
        "side",
        vmem(10),
        [shape((6, 128, 128)), shape((6, 128, 128), f32), shape((256, 384)), shape((256, 256))],
        [],
        16,
        1_000_000_000,
    )(own_normed, normed, scale, wb, wkk, solved, v, rho, w_gate_rec, w_gate_pool)
    prefix, onward, total = call(
        row_kernel,
        "row",
        vmem(4) + [pl.BlockSpec(memory_space=pl.ANY)],
        [shape((3, 2, 128, 128), f32), shape((320, 128)), shape((256, 128))],
        [pltpu.VMEM((4, 256, 128), bf16)],
        8,
        100_000_000,
    )(home, r1, r2, r3, pgate)
    columns = around((onward, total, total), "sp_0")
    s0, s1, s2, s3 = call(
        column_kernel,
        "column",
        vmem(5),
        [shape((2, 64, 128))] * 4,
        [pltpu.VMEM((4, 2, 64, 128), bf16), pltpu.VMEM((4, 256, 128), bf16)],
        8,
        100_000_000,
    )(prefix, *columns, init_state)
    t1, t2, t3 = around((s1, s2, s3), "sp_1")
    pool_out = call(pool_kernel, "pool", vmem(6), shape((256, 256)), [], 8, 100_000_000)(
        pool, r1, columns[0], pgate, pool_mix, line(pool_scale)
    )
    send, keep = call(
        final_kernel,
        "final",
        vmem(11),
        [shape((256, 1024)), shape((256, 1024))],
        [pltpu.VMEM((4, 2, 64, 128), bf16), pltpu.VMEM((256, 384), bf16)],
        20,
        1_000_000_000,
    )(s0, t1, t2, t3, reads, local, gate, head_gain, pool_out, w_out_rec, w_out_pool)
    arrived = lax.ppermute(send, "tp", [(0, 1), (1, 0)])
    mixed = keep.astype(f32) + arrived.astype(f32)
    return mixed.astype(bf16).reshape(2, 128, 1024)


def solution(mesh):
    split = Mesh(
        mesh.devices.reshape(4, 4, mesh.shape["fs"], mesh.shape["tp"]), ("sp_0", "sp_1", "fs", "tp")
    )
    column = P(None, "tp")
    placed = (
        (P("fs", SP, "tp"), P()) + (column,) * 8 + (P(),) * 5
        + (P("tp", None), P("tp", None), P("fs", "tp", None, None))
    )
    return jax.shard_map(
        shards, mesh=split, in_specs=placed, out_specs=P("fs", SP, "tp"), check_vma=False
    )
```

```python
import functools

import jax
import jax.numpy as jnp
from jax import lax
from jax.experimental import pallas as pl
from jax.experimental.pallas import tpu as pltpu
from jax.sharding import Mesh
from jax.sharding import PartitionSpec as P

D = 2048
HEAD = 64
SPAN = 128
UNITS = 6
SP = ("sp_0", "sp_1")
f32 = jnp.float32
bf16 = jnp.bfloat16
NN = ((1,), (0,))
NT = ((1,), (1,))
TN = ((0,), (0,))
MIB = 2**20


def dot(a, b, dims=NN):
    return lax.dot_general(
        a.astype(bf16), b.astype(bf16), (dims, ((), ())), preferred_element_type=f32
    )


def halves(x):
    high = x.astype(bf16)
    return high, (x - high.astype(f32)).astype(bf16)


def dot_fine_left(a, b, dims=NN):
    high, low = halves(a)
    return dot(high, b, dims) + dot(low, b, dims)


def dot_fine_right(a, b, dims=NN):
    high, low = halves(b)
    return dot(a, high, dims) + dot(a, low, dims)


def iota(rows, cols, dim):
    return lax.broadcasted_iota(jnp.int32, (rows, cols), dim)


def line_of(ref, lanes):
    if len(ref.shape) == 1:
        return ref[lanes].reshape(1, 128)
    return ref[:, lanes]


def head_masks():
    first = (iota(1, 128, 1) < HEAD).astype(f32)
    return first.astype(bf16), (1.0 - first).astype(bf16)


def both(x, masks):
    x = x.astype(bf16)
    return jnp.concatenate([x * masks[0], x * masks[1]], axis=0)


def joined(x):
    return jnp.where(iota(HEAD, 128, 1) < HEAD, x[:HEAD], x[HEAD:])


def compose(earlier, later, masks):
    moved = dot_fine_left(earlier, both(later[:HEAD], masks))
    written = later[HEAD:].astype(f32)
    if earlier.shape[0] == HEAD:
        return moved + written
    return jnp.concatenate([moved[:HEAD], moved[HEAD:] + written], axis=0)


def pick(x, size, odd):
    parts = [x[s : s + size] for s in range(size * odd, SPAN, 2 * size)]
    return parts[0] if len(parts) == 1 else jnp.concatenate(parts, axis=0)


def weave(even, odd, size):
    parts = []
    for s in range(0, SPAN // 2, size):
        parts += [even[s : s + size], odd[s : s + size]]
    return jnp.concatenate(parts, axis=0)


def woven(part, size):
    if size >= 16:
        part = part.astype(bf16)
    return weave(jnp.zeros_like(part), part, size)


def inverses(lowers):
    row, col = iota(SPAN, SPAN, 0), iota(SPAN, SPAN, 1)
    eye = (row == col).astype(f32)
    near = ((row >> 1) == (col >> 1)).astype(bf16)
    result = [eye - (lower * near).astype(f32) for lower in lowers]
    size, level = 2, 1
    while size < SPAN:
        off = (((row >> (level + 1)) == (col >> (level + 1))) & ((row >> level) != (col >> level))).astype(bf16)
        if size < 8:
            inner = [dot(lower * off, inv) for lower, inv in zip(lowers, result)]
            result = [inv - dot(inv, part) for inv, part in zip(result, inner)]
        else:
            if size < 16:
                off = pick(off.astype(f32), size, 1).astype(bf16)
                odd = [pick(lower.astype(f32), size, 1).astype(bf16) for lower in lowers]
            else:
                off = pick(off, size, 1)
                odd = [pick(lower, size, 1) for lower in lowers]
            inner = [dot(lower * off, inv) for lower, inv in zip(odd, result)]
            outer = [
                dot(pick(inv, size, 1), woven(part, size))
                for inv, part in zip(result, inner)
            ]
            result = [
                weave(pick(inv, size, 0), pick(inv, size, 1) - part, size)
                for inv, part in zip(result, outer)
            ]
        size, level = size * 2, level + 1
    return result


WIDTHS = (384, 384, 384, 384, 384, 256)


def fetch(sources, bufs, first_row, sems, base):
    copies = [
        pltpu.make_async_copy(src.at[pl.ds(pl.multiple_of(first_row, 1024), 1024), :], buf, sems.at[base + i])
        for i, (src, buf) in enumerate(zip(sources, bufs))
    ]
    for copy in copies:
        copy.start()
    return copies


def own_kernel(*refs):
    token_ref, norm_ref = refs[:2]
    sources, normed_ref, squares_ref, partials, rest = refs[2:8], refs[8], refs[9], refs[10:16], refs[16:22]
    bufs, sems, own_ref, gain_ref, first_sems = refs[22:28], refs[28], refs[29], refs[30], refs[31]
    tp = lax.axis_index("tp")
    early = [
        pltpu.make_async_copy(token_ref, own_ref, first_sems.at[0]),
        pltpu.make_async_copy(norm_ref, gain_ref, first_sems.at[1]),
    ]
    for copy in early:
        copy.start()
    copies = fetch(sources, bufs, tp * 1024, sems, 0)
    later = fetch(sources, rest, (1 - tp) * 1024, sems, 6)
    for copy in early:
        copy.wait()
    own = own_ref[...].astype(f32)
    normed = (own * jnp.where(tp == 0, gain_ref[:, :1024], gain_ref[:, 1024:])).astype(bf16)
    normed_ref[...] = normed
    squares_ref[...] = jnp.broadcast_to(jnp.sum(own * own, axis=1, keepdims=True), (256, 128))
    for copy, buf, partial in zip(copies, bufs, partials):
        copy.wait()
        partial[...] = dot(normed, buf[...])
    for copy in later:
        copy.wait()


def local_kernel(*refs):
    other_ref, gain_ref, squares_ref, db_ref, rb_ref = refs[:5]
    partials, rest = refs[5:11], refs[11:17]
    (
        normed_ref, scale_ref, pool_ref, home_ref, first_ref, second_ref, third_ref,
        right_ref, solved_ref, v_ref, rho_ref, lift_ref,
    ) = refs[17:29]
    k_s, d_s, a_s, r_s, v_s, maps = refs[29:35]
    tp = lax.axis_index("tp")
    y = lax.axis_index("sp_1")
    is_first = tp == 0
    other = other_ref[...].astype(f32)
    normed = (other * jnp.where(is_first, gain_ref[:, 1024:], gain_ref[:, :1024])).astype(bf16)
    normed_ref[...] = normed
    squares = squares_ref[:, :1] + jnp.sum(other * other, axis=1, keepdims=True)
    scale = lax.rsqrt(squares * (1.0 / D) + 0.25)
    scale_ref[...] = jnp.broadcast_to(scale, (256, 128))
    for i in range(6):
        rounded = ((partials[i][...] + dot(normed, rest[i][...])) * scale).astype(bf16)
        if i == 5:
            pool_ref[...] = rounded
            for s in (0, 1):
                for half in (0, 1):
                    at = 256 + (2 * s + half) * 16
                    first_ref[at : at + 16] = rounded[
                        s * 128 + 112 : s * 128 + 128, half * 128 : half * 128 + 128
                    ]
            continue
        dest = (k_s, d_s, a_s, r_s, v_s)[i]
        for u in range(UNITS):
            s, h = u // 3, u % 3
            dest[u] = rounded[s * 128 : s * 128 + 128, h * 128 : h * 128 + 128].astype(f32)

    masks = head_masks()
    n = SPAN
    row, col = iota(n, n, 0), iota(n, n, 1)
    strict, inclusive = row > col, row >= col
    triangle = inclusive.astype(f32)
    ones = ((row >> 6) == (col >> 6)).astype(f32)
    wide = (
        jnp.concatenate([masks[0], masks[0]], axis=1),
        jnp.concatenate([masks[1], masks[1]], axis=1),
    )
    slab = iota(HEAD, 128, 0)
    eye = (slab == (iota(HEAD, 128, 1) & 63)).astype(f32)
    units = range(UNITS)
    lowers, alphas, keeps = [], [], []
    for u in units:
        h = u % 3
        lanes = slice(h * 128, h * 128 + 128)
        shifted = slice(384 + h * 128, 384 + h * 128 + 128)
        db = jnp.where(is_first, line_of(db_ref, lanes), line_of(db_ref, shifted))
        rb = jnp.where(is_first, line_of(rb_ref, lanes), line_of(rb_ref, shifted))
        k = k_s[u]
        log_decay = -0.6065306597126334 * jax.nn.sigmoid(db + d_s[u])
        rate = jax.nn.sigmoid(rb + a_s[u])
        unit_key = k * lax.rsqrt(dot_fine_left(k * k, ones) + 1.0)
        removal = unit_key * rate
        total = dot_fine_right(triangle, log_decay)
        middle, final = total[63:64], total[127:128]
        alpha = jnp.exp(total - log_decay - middle) * unit_key
        fading = jnp.exp(middle - total)
        beta, kappa = removal * fading, k * fading
        rho = r_s[u] * jnp.exp(total - middle)
        ending = jnp.exp(final - total)
        lift = jnp.exp(middle)
        rho_ref[u] = rho
        lift_ref[u : u + 1] = lift
        right = jnp.concatenate([beta.astype(bf16), kappa.astype(bf16)], axis=0)
        right_ref[u] = right
        pairs = dot(both(alpha, masks), right, NT)
        lower_kappa = []
        for j in (0, 1):
            lowers.append(jnp.where(strict, pairs[j * n : j * n + n, :n], 0.0).astype(bf16))
            lower_kappa.append(jnp.where(strict, pairs[j * n : j * n + n, n:], 0.0).astype(bf16))
        v = v_s[u]
        v_ref[u] = v.astype(bf16)
        carried = dot(jnp.concatenate(lower_kappa, axis=1), both(v, masks))
        keeps.append((alpha * lift, carried, removal * ending, k * ending, jnp.exp(final)))
    inverse = inverses(lowers)
    for u in units:
        alpha, carried, beta_end, kappa_end, gain_end = keeps[u]
        right = jnp.concatenate([alpha, carried], axis=1)
        solved = dot(jnp.concatenate(inverse[2 * u : 2 * u + 2], axis=1), both(right, wide))
        solved_ref[u] = solved.astype(bf16)
        crossed = dot(solved[:, :n], beta_end, TN)
        transit = eye * gain_end - joined(crossed)
        crossed = dot(
            jnp.concatenate([v_s[u], -solved[:, n:]], axis=0),
            jnp.concatenate([kappa_end, beta_end], axis=0),
            TN,
        )
        written = joined(crossed)
        at = (u // 3) * 128
        maps[u % 3, at : at + HEAD] = transit.astype(bf16)
        maps[u % 3, at + HEAD : at + 128] = written.astype(bf16)
    maps[3] = jnp.zeros((256, 128), bf16)
    for step, dest in enumerate((home_ref, first_ref, second_ref, third_ref)):
        dest[:256] = maps[(y + step) & 3]


def side_kernel(
    own_ref, other_ref, scale_ref, right_ref, solved_ref, v_ref, rho_ref, lift_ref, wg_ref, wq_ref,
    reads_ref, local_ref, gate_ref, pgate_ref,
):
    tp = lax.axis_index("tp")
    masks = head_masks()
    wide = (
        jnp.concatenate([masks[0], masks[0]], axis=1),
        jnp.concatenate([masks[1], masks[1]], axis=1),
    )
    inclusive = iota(128, 128, 0) >= iota(128, 128, 1)
    inside = []
    for u in range(UNITS):
        pairs = dot(both(rho_ref[u], masks), right_ref[u], NT)
        block = lambda j, c: jnp.where(
            inclusive, pairs[j * 128 : j * 128 + 128, c * 128 : c * 128 + 128], 0.0
        ).astype(bf16)
        inside.append([jnp.concatenate([block(0, c), block(1, c)], axis=1) for c in (0, 1)])
    for u in range(UNITS):
        removed = dot(inside[u][0], both(solved_ref[u], wide))
        reads_ref[u] = (rho_ref[u] * lift_ref[u : u + 1] - removed[:, :128]).astype(bf16)
        local_ref[u] = dot(inside[u][1], both(v_ref[u], masks)) - removed[:, 128:]
    scale = scale_ref[:, :1]
    mine, theirs = pl.multiple_of(tp * 1024, 1024), pl.multiple_of((1 - tp) * 1024, 1024)
    for weight, dest in ((wg_ref, gate_ref), (wq_ref, pgate_ref)):
        total = dot(own_ref[...], weight[pl.ds(mine, 1024), :])
        total = total + dot(other_ref[...], weight[pl.ds(theirs, 1024), :])
        dest[...] = (total * scale).astype(bf16)


def row_kernel(home_ref, first_ref, second_ref, third_ref, after_ref, prefix_ref, next_ref, total_ref, maps):
    y = lax.axis_index("sp_1")
    for step, src in enumerate((home_ref, first_ref, second_ref, third_ref)):
        maps[(y + 4 - step) & 3] = src[:256]
    next_ref[256:] = first_ref[256:]
    masks = head_masks()
    for s in (0, 1):
        rows = slice(s * 128, s * 128 + 128)
        so_far = maps[0, rows].astype(f32)
        prefix_ref[0, s] = so_far
        for j in (1, 2, 3):
            so_far = compose(so_far, maps[j, rows], masks)
            if j < 3:
                prefix_ref[j, s] = so_far
            else:
                next_ref[rows] = so_far.astype(bf16)
                total_ref[rows] = so_far.astype(bf16)


def column_kernel(
    prefix_ref, first_ref, second_ref, third_ref, init_ref,
    home_ref, one_ref, two_ref, three_ref,
    starts, rows,
):
    y = lax.axis_index("sp_1")
    z = lax.axis_index("sp_0")
    for step, src in enumerate((first_ref, second_ref, third_ref)):
        rows[(z + 3 - step) & 3] = src[:256]
    masks = head_masks()
    pair = jnp.minimum(y, 2) * 2
    for s in (0, 1):
        state = jnp.concatenate([init_ref[s, pair], init_ref[s, pair + 1]], axis=1)
        for j in range(3):
            state = jnp.where(j < z, compose(state, rows[j, s * 128 : s * 128 + 128], masks), state)
        starts[0, s] = state.astype(bf16)
        for j in range(3):
            starts[j + 1, s] = compose(state, prefix_ref[j, s], masks).astype(bf16)
    for step, dest in enumerate((home_ref, one_ref, two_ref, three_ref)):
        dest[...] = starts[(y + step) & 3]


def pool_kernel(pool_ref, beside_ref, above_ref, pgate_ref, mix_ref, pscale_ref, wp_ref, part_ref, out_ref):
    tp = lax.axis_index("tp")
    y = lax.axis_index("sp_1")
    place = lax.axis_index("sp_0") * 4 + y
    is_first = tp == 0
    factor = jnp.where(is_first, pscale_ref[:, :256], pscale_ref[:, 256:])
    for s in (0, 1):
        current = pool_ref[s * 128 : s * 128 + 128].astype(f32)
        tails = []
        for half in (0, 1):
            rows = slice(256 + (2 * s + half) * 16, 272 + (2 * s + half) * 16)
            tails.append(
                jnp.where(
                    place == 0,
                    0.0,
                    jnp.where(y > 0, beside_ref[rows].astype(f32), above_ref[rows].astype(f32)),
                )
            )
        padded = jnp.concatenate([jnp.concatenate(tails, axis=1), current], axis=0)
        sums = {1: padded}
        for by in (1, 2, 4, 8):
            before = sums[by]
            moved = jnp.concatenate([jnp.zeros((by, 256), f32), before[: 144 - by]], axis=0)
            sums[2 * by] = before + moved
        position = (place * 128 + iota(128, 128, 0) + 1).astype(f32)
        for g in (0, 1):
            lanes = slice(g * 128, g * 128 + 128)
            small, large = 2 << g, 8 << g
            trailing = jnp.where(is_first, sums[small][16:, lanes], sums[large][16:, lanes])
            window = jnp.where(is_first, float(small), float(large))
            diffs = trailing / jnp.minimum(position, window) - current[:, lanes]
            mixed = dot(diffs.astype(bf16), mix_ref[tp * 2 + g])
            gate = pgate_ref[s * 128 : s * 128 + 128, lanes].astype(f32)
            out_ref[s * 128 : s * 128 + 128, lanes] = (
                mixed * factor[:, lanes] * (gate * jax.nn.sigmoid(gate))
            ).astype(bf16)
    part_ref[...] = dot(out_ref[...], wp_ref[...])


def final_kernel(
    home_ref, one_ref, two_ref, three_ref, reads_ref, local_ref, gate_ref, hgain_ref, part_ref,
    wr_ref,
    send_ref, keep_ref,
    starts, rec,
):
    tp = lax.axis_index("tp")
    y = lax.axis_index("sp_1")
    for step, src in enumerate((home_ref, one_ref, two_ref, three_ref)):
        starts[(y + 4 - step) & 3] = src[...]
    masks = head_masks()
    row, col = iota(128, 128, 0), iota(128, 128, 1)
    mean_of = jnp.where((row >> 6) == (col >> 6), 1.0 / HEAD, 0.0).astype(bf16)
    is_first = tp == 0
    for u in range(UNITS):
        s, h = u // 3, u % 3
        lanes = slice(h * 128, h * 128 + 128)
        shifted = slice(384 + h * 128, 384 + h * 128 + 128)
        rows = slice(s * 128, s * 128 + 128)
        out = dot(reads_ref[u], both(starts[h, s], masks), NT) + local_ref[u]
        out = out - dot_fine_left(out, mean_of)
        spread = dot_fine_left(out * out, mean_of)
        gain = jnp.where(is_first, line_of(hgain_ref, lanes), line_of(hgain_ref, shifted))
        gate = gate_ref[rows, lanes].astype(f32)
        rec[rows, lanes] = (
            out * lax.rsqrt(spread + 1.0) * gain * (gate * jax.nn.sigmoid(gate))
        ).astype(bf16)
    for dest, part in ((send_ref, 1 - tp), (keep_ref, tp)):
        cols = pl.ds(pl.multiple_of(part * 1024, 1024), 1024)
        dest[...] = (dot(rec[...], wr_ref[:, cols]) + part_ref[:, cols]).astype(bf16)


def vmem(count):
    return [pl.BlockSpec(memory_space=pltpu.VMEM)] * count


def hbm(count):
    return [pl.BlockSpec(memory_space=pltpu.HBM)] * count


def shape(dims, kind=bf16):
    return jax.ShapeDtypeStruct(dims, kind)


def call(body, name, ins, outs, scratch, limit, flops=0):
    return pl.pallas_call(
        body,
        name=name,
        out_shape=outs,
        in_specs=ins,
        out_specs=vmem(len(outs)) if isinstance(outs, (list, tuple)) else vmem(1)[0],
        scratch_shapes=scratch,
        compiler_params=pltpu.CompilerParams(vmem_limit_bytes=limit * MIB),
        cost_estimate=pl.CostEstimate(flops=flops, transcendentals=0, bytes_accessed=0) if flops else None,
    )


def around(parts, axis):
    return [
        lax.ppermute(part, axis, [(i, (i + step) & 3) for i in range(4)]) for step, part in enumerate(parts, 1)
    ]


def shards(
    tokens, norm_gain, w_recept, w_key, w_value, w_decay, w_rate, w_gate_rec, w_pool, w_gate_pool,
    decay_base, rate_base, head_gain, pool_mix, pool_scale, w_out_rec, w_out_pool, init_state,
):
    other = lax.ppermute(tokens, "tp", [(0, 1), (1, 0)])
    line = lambda x: x.reshape(1, -1)
    pinned = lambda x: pltpu.with_memory_space_constraint(x, pltpu.HBM)
    weights = [pinned(w) for w in (w_key, w_decay, w_rate, w_recept, w_value, w_pool)]
    bufs = [pltpu.VMEM((1024, width), bf16) for width in WIDTHS] + [pltpu.SemaphoreType.DMA((12,))]
    own_normed, squares, *halves_of = call(
        own_kernel,
        "own",
        hbm(8),
        [shape((256, 1024)), shape((256, 128), f32)] + [shape((256, width), f32) for width in WIDTHS]
        + [shape((1024, width)) for width in WIDTHS],
        bufs + [pltpu.VMEM((256, 1024), bf16), pltpu.VMEM((1, D), f32), pltpu.SemaphoreType.DMA((2,))],
        20,
        1_000_000_000,
    )(pinned(tokens.reshape(256, 1024)), pinned(line(norm_gain)), *weights)
    normed, scale, pool, home, m1, m2, m3, right, solved, v, rho, lift = call(
        local_kernel,
        "local",
        vmem(17),
        [
            shape((256, 1024)), shape((256, 128), f32), shape((256, 256)),
            shape((256, 128)), shape((320, 128)), shape((256, 128)), shape((256, 128)),
            shape((6, 256, 128)), shape((6, 128, 256)), shape((6, 128, 128)),
            shape((6, 128, 128), f32), shape((6, 128), f32),
        ],
        [pltpu.VMEM((6, 128, 128), f32)] * 5 + [pltpu.VMEM((4, 256, 128), bf16)],
        24,
        3_000_000_000,
    )(other.reshape(256, 1024), line(norm_gain), squares, decay_base, rate_base, *halves_of)
    r1, r2, r3 = around((m1, m2, m3), "sp_1")
    reads, local, gate, pgate = call(
        side_kernel,
        "side",
        vmem(10),
        [shape((6, 128, 128)), shape((6, 128, 128), f32), shape((256, 384)), shape((256, 256))],
        [],
        16,
        1_000_000_000,
    )(own_normed, normed, scale, right, solved, v, rho, lift, w_gate_rec, w_gate_pool)
    prefix, onward, total = call(
        row_kernel,
        "row",
        vmem(4) + [pl.BlockSpec(memory_space=pl.ANY)],
        [shape((3, 2, 128, 128), f32), shape((320, 128)), shape((256, 128))],
        [pltpu.VMEM((4, 256, 128), bf16)],
        8,
        100_000_000,
    )(home, r1, r2, r3, pgate)
    columns = around((onward, total, total), "sp_0")
    s0, s1, s2, s3 = call(
        column_kernel,
        "column",
        vmem(5),
        [shape((2, 64, 128))] * 4,
        [pltpu.VMEM((4, 2, 64, 128), bf16), pltpu.VMEM((4, 256, 128), bf16)],
        8,
        100_000_000,
    )(prefix, *columns, init_state)
    t1, t2, t3 = around((s1, s2, s3), "sp_1")
    pool_part = call(
        pool_kernel, "pool", vmem(7), shape((256, D), f32), [pltpu.VMEM((256, 256), bf16)], 12, 300_000_000
    )(pool, r1, columns[0], pgate, pool_mix, line(pool_scale), w_out_pool)
    send, keep = call(
        final_kernel,
        "final",
        vmem(10),
        [shape((256, 1024)), shape((256, 1024))],
        [pltpu.VMEM((4, 2, 64, 128), bf16), pltpu.VMEM((256, 384), bf16)],
        20,
        1_000_000_000,
    )(s0, t1, t2, t3, reads, local, gate, head_gain, pool_part, w_out_rec)
    arrived = lax.ppermute(send, "tp", [(0, 1), (1, 0)])
    mixed = keep.astype(f32) + arrived.astype(f32)
    return mixed.astype(bf16).reshape(2, 128, 1024)


def solution(mesh):
    split = Mesh(
        mesh.devices.reshape(4, 4, mesh.shape["fs"], mesh.shape["tp"]), ("sp_0", "sp_1", "fs", "tp")
    )
    column = P(None, "tp")
    placed = (
        (P("fs", SP, "tp"), P()) + (column,) * 8 + (P(),) * 5
        + (P("tp", None), P("tp", None), P("fs", "tp", None, None))
    )
    return jax.shard_map(
        shards, mesh=split, in_specs=placed, out_specs=P("fs", SP, "tp"), check_vma=False
    )
```

```python
import functools

import jax
import jax.numpy as jnp
from jax import lax
from jax.experimental import pallas as pl
from jax.experimental.pallas import tpu as pltpu
from jax.sharding import Mesh
from jax.sharding import PartitionSpec as P

D = 2048
HEAD = 64
SPAN = 128
UNITS = 6
SP = ("sp_0", "sp_1")
f32 = jnp.float32
bf16 = jnp.bfloat16
NN = ((1,), (0,))
NT = ((1,), (1,))
TN = ((0,), (0,))
MIB = 2**20


def dot(a, b, dims=NN):
    return lax.dot_general(
        a.astype(bf16), b.astype(bf16), (dims, ((), ())), preferred_element_type=f32
    )


def halves(x):
    high = x.astype(bf16)
    return high, (x - high.astype(f32)).astype(bf16)


def dot_fine_left(a, b, dims=NN):
    high, low = halves(a)
    return dot(high, b, dims) + dot(low, b, dims)


def dot_fine_right(a, b, dims=NN):
    high, low = halves(b)
    return dot(a, high, dims) + dot(a, low, dims)


def iota(rows, cols, dim):
    return lax.broadcasted_iota(jnp.int32, (rows, cols), dim)


def line_of(ref, lanes):
    if len(ref.shape) == 1:
        return ref[lanes].reshape(1, 128)
    return ref[:, lanes]


def head_masks():
    first = (iota(1, 128, 1) < HEAD).astype(f32)
    return first.astype(bf16), (1.0 - first).astype(bf16)


def both(x, masks):
    x = x.astype(bf16)
    return jnp.concatenate([x * masks[0], x * masks[1]], axis=0)


def joined(x):
    return jnp.where(iota(HEAD, 128, 1) < HEAD, x[:HEAD], x[HEAD:])


def compose(earlier, later, masks):
    moved = dot_fine_left(earlier, both(later[:HEAD], masks))
    written = later[HEAD:].astype(f32)
    if earlier.shape[0] == HEAD:
        return moved + written
    return jnp.concatenate([moved[:HEAD], moved[HEAD:] + written], axis=0)


def pick(x, size, odd):
    parts = [x[s : s + size] for s in range(size * odd, SPAN, 2 * size)]
    return parts[0] if len(parts) == 1 else jnp.concatenate(parts, axis=0)


def weave(even, odd, size):
    parts = []
    for s in range(0, SPAN // 2, size):
        parts += [even[s : s + size], odd[s : s + size]]
    return jnp.concatenate(parts, axis=0)


def woven(part, size):
    if size >= 16:
        part = part.astype(bf16)
    return weave(jnp.zeros_like(part), part, size)


def blocks(x):
    x = x.astype(bf16)
    zero = jnp.zeros((SPAN, 128), bf16)
    return jnp.concatenate(
        [jnp.concatenate([x[:, :128], zero], axis=1), jnp.concatenate([zero, x[:, 128:]], axis=1)], axis=0
    )


def inverses(lowers, fill):
    row, col = iota(SPAN, 256, 0), iota(SPAN, 256, 1) & 127
    eye = (row == col).astype(f32)
    near = ((row >> 1) == (col >> 1)).astype(bf16)
    result = [eye - (lower * near).astype(f32) for lower in lowers]
    size, level = 2, 1
    while size < SPAN:
        off = (((row >> (level + 1)) == (col >> (level + 1))) & ((row >> level) != (col >> level))).astype(bf16)
        if size < 8:
            inner = [dot(lower * off, blocks(inv)) for lower, inv in zip(lowers, result)]
            fill(level)
            result = [inv - dot(inv, blocks(part)) for inv, part in zip(result, inner)]
        else:
            if size < 16:
                off = pick(off.astype(f32), size, 1).astype(bf16)
                odd = [pick(lower.astype(f32), size, 1).astype(bf16) for lower in lowers]
            else:
                off = pick(off, size, 1)
                odd = [pick(lower, size, 1) for lower in lowers]
            inner = [dot(lower * off, blocks(inv)) for lower, inv in zip(odd, result)]
            fill(level)
            outer = [
                dot(pick(inv, size, 1), blocks(woven(part, size))) for inv, part in zip(result, inner)
            ]
            result = [
                weave(pick(inv, size, 0), pick(inv, size, 1) - part, size)
                for inv, part in zip(result, outer)
            ]
        size, level = size * 2, level + 1
    return result


WIDTHS = (384, 384, 384, 384, 384, 256)


def fetch(src, buf, first_row, sem):
    return pltpu.make_async_copy(src.at[pl.ds(pl.multiple_of(first_row, 1024), 1024), :], buf, sem)


EARLY = 3


def own_kernel(*refs):
    token_ref, norm_ref = refs[:2]
    sources, normed_ref, squares_ref, partials, rest = refs[2:8], refs[8], refs[9], refs[10:16], refs[16:19]
    bufs, sems, own_ref, gain_ref, first_sems = refs[19:25], refs[25], refs[26], refs[27], refs[28]
    tp = lax.axis_index("tp")
    early = [
        pltpu.make_async_copy(norm_ref, gain_ref, first_sems.at[0]),
        pltpu.make_async_copy(token_ref, own_ref, first_sems.at[1]),
    ]
    mine = [fetch(src, buf, tp * 1024, sems.at[i]) for i, (src, buf) in enumerate(zip(sources, bufs))]
    others = [
        fetch(src, buf, (1 - tp) * 1024, sems.at[6 + i]) for i, (src, buf) in enumerate(zip(sources, rest))
    ]
    queue = mine + others
    for copy in early + queue[:2]:
        copy.start()
    for copy in early:
        copy.wait()
    for copy in queue[2:4]:
        copy.start()
    own = own_ref[...].astype(f32)
    normed = (own * jnp.where(tp == 0, gain_ref[:, :1024], gain_ref[:, 1024:])).astype(bf16)
    normed_ref[...] = normed
    squares_ref[...] = jnp.broadcast_to(jnp.sum(own * own, axis=1, keepdims=True), (256, 128))
    started = 4
    for i, (copy, buf, partial) in enumerate(zip(mine, bufs, partials)):
        copy.wait()
        for extra in queue[started : started + (1 if i else 2)]:
            extra.start()
        started += 1 if i else 2
        partial[...] = dot(normed, buf[...])
    for extra in queue[started:]:
        extra.start()
    for copy in others:
        copy.wait()


def local_kernel(*refs):
    other_ref, gain_ref, squares_ref, db_ref, rb_ref = refs[:5]
    partials, ready, sources = refs[5:11], refs[11:14], refs[14:17]
    (
        normed_ref, scale_ref, pool_ref, home_ref, first_ref, second_ref, third_ref,
        right_ref, solved_ref, v_ref, r_ref, grow_ref, lift_ref,
    ) = refs[17:30]
    k_s, d_s, a_s, maps = refs[30:34]
    bufs, sems = refs[34:37], refs[37]
    tp = lax.axis_index("tp")
    y = lax.axis_index("sp_1")
    copies = [fetch(src, buf, (1 - tp) * 1024, sems.at[i]) for i, (src, buf) in enumerate(zip(sources, bufs))]
    for copy in copies:
        copy.start()
    rest = tuple(ready) + tuple(bufs)
    is_first = tp == 0
    other = other_ref[...].astype(f32)
    normed = (other * jnp.where(is_first, gain_ref[:, 1024:], gain_ref[:, :1024])).astype(bf16)
    normed_ref[...] = normed
    squares = squares_ref[:, :1] + jnp.sum(other * other, axis=1, keepdims=True)
    scale = lax.rsqrt(squares * (1.0 / D) + 0.25)
    scale_ref[...] = jnp.broadcast_to(scale, (256, 128))
    def project(i, rows):
        total = partials[i][rows] + dot(normed_ref[rows], rest[i][...])
        return (total * scale_ref[rows, :1]).astype(bf16)

    for i, dest in enumerate((k_s, d_s, a_s)):
        rounded = project(i, slice(0, 256))
        for u in range(UNITS):
            s, h = u // 3, u % 3
            dest[u] = rounded[s * 128 : s * 128 + 128, h * 128 : h * 128 + 128].astype(f32)
    for copy in copies:
        copy.wait()

    def fill(level):
        if level > 3:
            return
        if level == 3:
            pool = project(5, slice(0, 256))
            pool_ref[...] = pool
            for s in (0, 1):
                for half in (0, 1):
                    at = 256 + (2 * s + half) * 16
                    first_ref[at : at + 16] = pool[s * 128 + 112 : s * 128 + 128, half * 128 : half * 128 + 128]
            return
        dest = (v_ref, r_ref)[level - 1]
        rounded = project(2 + level, slice(0, 256))
        for u in range(UNITS):
            s, h = u // 3, u % 3
            dest[u] = rounded[s * 128 : s * 128 + 128, h * 128 : h * 128 + 128]

    masks = head_masks()
    n = SPAN
    row, col = iota(n, n, 0), iota(n, n, 1)
    strict, inclusive = row > col, row >= col
    triangle = inclusive.astype(f32)
    ones = ((row >> 6) == (col >> 6)).astype(f32)
    wide = (
        jnp.concatenate([masks[0], masks[0]], axis=1),
        jnp.concatenate([masks[1], masks[1]], axis=1),
    )
    slab = iota(HEAD, 128, 0)
    eye = (slab == (iota(HEAD, 128, 1) & 63)).astype(f32)
    units = range(UNITS)
    first_stage = []
    for u in units:
        h = u % 3
        lanes = slice(h * 128, h * 128 + 128)
        shifted = slice(384 + h * 128, 384 + h * 128 + 128)
        db = jnp.where(is_first, line_of(db_ref, lanes), line_of(db_ref, shifted))
        rb = jnp.where(is_first, line_of(rb_ref, lanes), line_of(rb_ref, shifted))
        k = k_s[u]
        log_decay = -0.6065306597126334 * jax.nn.sigmoid(db + d_s[u])
        first_stage.append(
            (log_decay, jax.nn.sigmoid(rb + a_s[u]), dot(k * k, ones), dot_fine_right(triangle, log_decay))
        )
    second_stage = []
    for u in units:
        log_decay, rate, squared, total = first_stage[u]
        k = k_s[u]
        middle = total[63:64]
        unit_key = k * lax.rsqrt(squared + 1.0)
        centred = total - middle
        alpha = jnp.exp(centred - log_decay) * unit_key
        fading = jnp.exp(-centred)
        grow_ref[u] = jnp.exp(centred)
        lift = jnp.exp(middle)
        lift_ref[u : u + 1] = lift
        right = jnp.concatenate(
            [(unit_key * rate * fading).astype(bf16), (k * fading).astype(bf16)], axis=0
        )
        right_ref[u] = right
        ends = (jnp.exp(total[127:128]), jnp.exp(centred[127:128]))
        second_stage.append((right, alpha * lift, ends, dot(both(alpha, masks), right, NT)))
    lowers, carries = [], []
    for u in units:
        pairs = second_stage[u][3]
        block = lambda j, c: jnp.where(
            strict, pairs[j * n : j * n + n, c * n : c * n + n], 0.0
        ).astype(bf16)
        lowers.append(jnp.concatenate([block(0, 0), block(1, 0)], axis=1))
        carries.append(jnp.concatenate([block(0, 1), block(1, 1)], axis=1))
    inverse = inverses(lowers, fill)
    carries = [dot(carries[u], both(v_ref[u], masks)) for u in units]
    solutions = []
    for u in units:
        wanted = jnp.concatenate([second_stage[u][1].astype(bf16), carries[u].astype(bf16)], axis=1)
        solved = dot(inverse[u], both(wanted, wide)).astype(bf16)
        solved_ref[u] = solved
        solutions.append(solved)
    for u in units:
        right, _, ends, _ = second_stage[u]
        solved = solutions[u]
        transit = eye * ends[0] - joined(dot(solved[:, :n], right[:n], TN)) * ends[1]
        written = joined(
            dot(
                jnp.concatenate([-solved[:, n:], v_ref[u]], axis=0),
                right,
                TN,
            )
        ) * ends[1]
        at = (u // 3) * 128
        maps[u % 3, at : at + HEAD] = transit.astype(bf16)
        maps[u % 3, at + HEAD : at + 128] = written.astype(bf16)
    maps[3] = jnp.zeros((256, 128), bf16)
    for step, dest in enumerate((home_ref, first_ref, second_ref, third_ref)):
        dest[:256] = maps[(y + step) & 3]


def side_kernel(
    own_ref, other_ref, scale_ref, right_ref, solved_ref, v_ref, r_ref, grow_ref, lift_ref, wg_ref, wq_ref,
    reads_ref, local_ref, gate_ref, pgate_ref,
):
    tp = lax.axis_index("tp")
    masks = head_masks()
    wide = (
        jnp.concatenate([masks[0], masks[0]], axis=1),
        jnp.concatenate([masks[1], masks[1]], axis=1),
    )
    inclusive = iota(128, 128, 0) >= iota(128, 128, 1)
    inside, rhos = [], []
    for u in range(UNITS):
        rho = r_ref[u].astype(f32) * grow_ref[u]
        rhos.append(rho * lift_ref[u : u + 1])
        pairs = dot(both(rho, masks), right_ref[u], NT)
        block = lambda j, c: jnp.where(
            inclusive, pairs[j * 128 : j * 128 + 128, c * 128 : c * 128 + 128], 0.0
        ).astype(bf16)
        inside.append([jnp.concatenate([block(0, c), block(1, c)], axis=1) for c in (0, 1)])
    for u in range(UNITS):
        removed = dot(inside[u][0], both(solved_ref[u], wide))
        reads_ref[u] = (rhos[u] - removed[:, :128]).astype(bf16)
        local_ref[u] = dot(inside[u][1], both(v_ref[u], masks)) - removed[:, 128:]
    scale = scale_ref[:, :1]
    mine, theirs = pl.multiple_of(tp * 1024, 1024), pl.multiple_of((1 - tp) * 1024, 1024)
    for weight, dest in ((wg_ref, gate_ref), (wq_ref, pgate_ref)):
        total = dot(own_ref[...], weight[pl.ds(mine, 1024), :])
        total = total + dot(other_ref[...], weight[pl.ds(theirs, 1024), :])
        dest[...] = (total * scale).astype(bf16)


def row_kernel(home_ref, first_ref, second_ref, third_ref, after_ref, prefix_ref, next_ref, total_ref, maps):
    y = lax.axis_index("sp_1")
    for step, src in enumerate((home_ref, first_ref, second_ref, third_ref)):
        maps[(y + 4 - step) & 3] = src[:256]
    next_ref[256:] = first_ref[256:]
    masks = head_masks()
    for s in (0, 1):
        rows = slice(s * 128, s * 128 + 128)
        so_far = maps[0, rows].astype(f32)
        prefix_ref[0, s] = so_far
        for j in (1, 2, 3):
            so_far = compose(so_far, maps[j, rows], masks)
            if j < 3:
                prefix_ref[j, s] = so_far
            else:
                next_ref[rows] = so_far.astype(bf16)
                total_ref[rows] = so_far.astype(bf16)


def column_kernel(
    prefix_ref, first_ref, second_ref, third_ref, init_ref,
    home_ref, one_ref, two_ref, three_ref,
    starts, rows,
):
    y = lax.axis_index("sp_1")
    z = lax.axis_index("sp_0")
    for step, src in enumerate((first_ref, second_ref, third_ref)):
        rows[(z + 3 - step) & 3] = src[:256]
    masks = head_masks()
    pair = jnp.minimum(y, 2) * 2
    for s in (0, 1):
        state = jnp.concatenate([init_ref[s, pair], init_ref[s, pair + 1]], axis=1)
        for j in range(3):
            state = jnp.where(j < z, compose(state, rows[j, s * 128 : s * 128 + 128], masks), state)
        starts[0, s] = state.astype(bf16)
        for j in range(3):
            starts[j + 1, s] = compose(state, prefix_ref[j, s], masks).astype(bf16)
    for step, dest in enumerate((home_ref, one_ref, two_ref, three_ref)):
        dest[...] = starts[(y + step) & 3]


def pool_kernel(pool_ref, beside_ref, above_ref, pgate_ref, mix_ref, pscale_ref, wp_ref, part_ref, out_ref):
    tp = lax.axis_index("tp")
    y = lax.axis_index("sp_1")
    place = lax.axis_index("sp_0") * 4 + y
    is_first = tp == 0
    factor = jnp.where(is_first, pscale_ref[:, :256], pscale_ref[:, 256:])
    for s in (0, 1):
        current = pool_ref[s * 128 : s * 128 + 128].astype(f32)
        tails = []
        for half in (0, 1):
            rows = slice(256 + (2 * s + half) * 16, 272 + (2 * s + half) * 16)
            tails.append(
                jnp.where(
                    place == 0,
                    0.0,
                    jnp.where(y > 0, beside_ref[rows].astype(f32), above_ref[rows].astype(f32)),
                )
            )
        padded = jnp.concatenate([jnp.concatenate(tails, axis=1), current], axis=0)
        sums = {1: padded}
        for by in (1, 2, 4, 8):
            before = sums[by]
            moved = jnp.concatenate([jnp.zeros((by, 256), f32), before[: 144 - by]], axis=0)
            sums[2 * by] = before + moved
        position = (place * 128 + iota(128, 128, 0) + 1).astype(f32)
        for g in (0, 1):
            lanes = slice(g * 128, g * 128 + 128)
            small, large = 2 << g, 8 << g
            trailing = jnp.where(is_first, sums[small][16:, lanes], sums[large][16:, lanes])
            window = jnp.where(is_first, float(small), float(large))
            diffs = trailing / jnp.minimum(position, window) - current[:, lanes]
            mixed = dot(diffs.astype(bf16), mix_ref[tp * 2 + g])
            gate = pgate_ref[s * 128 : s * 128 + 128, lanes].astype(f32)
            out_ref[s * 128 : s * 128 + 128, lanes] = (
                mixed * factor[:, lanes] * (gate * jax.nn.sigmoid(gate))
            ).astype(bf16)
    part_ref[...] = dot(out_ref[...], wp_ref[...])


def final_kernel(
    home_ref, one_ref, two_ref, three_ref, reads_ref, local_ref, gate_ref, hgain_ref, part_ref,
    wr_ref,
    send_ref, keep_ref,
    starts, rec,
):
    tp = lax.axis_index("tp")
    y = lax.axis_index("sp_1")
    for step, src in enumerate((home_ref, one_ref, two_ref, three_ref)):
        starts[(y + 4 - step) & 3] = src[...]
    masks = head_masks()
    row, col = iota(128, 128, 0), iota(128, 128, 1)
    mean_of = jnp.where((row >> 6) == (col >> 6), 1.0 / HEAD, 0.0).astype(bf16)
    is_first = tp == 0
    for u in range(UNITS):
        s, h = u // 3, u % 3
        lanes = slice(h * 128, h * 128 + 128)
        shifted = slice(384 + h * 128, 384 + h * 128 + 128)
        rows = slice(s * 128, s * 128 + 128)
        out = dot(reads_ref[u], both(starts[h, s], masks), NT) + local_ref[u]
        out = out - dot_fine_left(out, mean_of)
        spread = dot_fine_left(out * out, mean_of)
        gain = jnp.where(is_first, line_of(hgain_ref, lanes), line_of(hgain_ref, shifted))
        gate = gate_ref[rows, lanes].astype(f32)
        rec[rows, lanes] = (
            out * lax.rsqrt(spread + 1.0) * gain * (gate * jax.nn.sigmoid(gate))
        ).astype(bf16)
    for dest, part in ((send_ref, 1 - tp), (keep_ref, tp)):
        cols = pl.ds(pl.multiple_of(part * 1024, 1024), 1024)
        dest[...] = (dot(rec[...], wr_ref[:, cols]) + part_ref[:, cols]).astype(bf16)


def vmem(count):
    return [pl.BlockSpec(memory_space=pltpu.VMEM)] * count


def hbm(count):
    return [pl.BlockSpec(memory_space=pltpu.HBM)] * count


def shape(dims, kind=bf16):
    return jax.ShapeDtypeStruct(dims, kind)


def call(body, name, ins, outs, scratch, limit, flops=0):
    return pl.pallas_call(
        body,
        name=name,
        out_shape=outs,
        in_specs=ins,
        out_specs=vmem(len(outs)) if isinstance(outs, (list, tuple)) else vmem(1)[0],
        scratch_shapes=scratch,
        compiler_params=pltpu.CompilerParams(vmem_limit_bytes=limit * MIB),
        cost_estimate=pl.CostEstimate(flops=flops, transcendentals=0, bytes_accessed=0) if flops else None,
    )


def around(parts, axis):
    return [
        lax.ppermute(part, axis, [(i, (i + step) & 3) for i in range(4)]) for step, part in enumerate(parts, 1)
    ]


def shards(
    tokens, norm_gain, w_recept, w_key, w_value, w_decay, w_rate, w_gate_rec, w_pool, w_gate_pool,
    decay_base, rate_base, head_gain, pool_mix, pool_scale, w_out_rec, w_out_pool, init_state,
):
    other = lax.ppermute(tokens, "tp", [(0, 1), (1, 0)])
    line = lambda x: x.reshape(1, -1)
    pinned = lambda x: pltpu.with_memory_space_constraint(x, pltpu.HBM)
    weights = [pinned(w) for w in (w_key, w_decay, w_rate, w_value, w_recept, w_pool)]
    bufs = [pltpu.VMEM((1024, width), bf16) for width in WIDTHS] + [pltpu.SemaphoreType.DMA((9,))]
    own_normed, squares, *halves_of = call(
        own_kernel,
        "own",
        hbm(8),
        [shape((256, 1024)), shape((256, 128), f32)] + [shape((256, width), f32) for width in WIDTHS]
        + [shape((1024, width)) for width in WIDTHS[:EARLY]],
        bufs + [pltpu.VMEM((256, 1024), bf16), pltpu.VMEM((1, D), f32), pltpu.SemaphoreType.DMA((2,))],
        20,
        1_000_000_000,
    )(pinned(tokens.reshape(256, 1024)), pinned(line(norm_gain)), *weights)
    normed, scale, pool, home, m1, m2, m3, right, solved, v, r, grow, lift = call(
        local_kernel,
        "local",
        vmem(14) + hbm(3),
        [
            shape((256, 1024)), shape((256, 128), f32), shape((256, 256)),
            shape((256, 128)), shape((320, 128)), shape((256, 128)), shape((256, 128)),
            shape((6, 256, 128)), shape((6, 128, 256)), shape((6, 128, 128)),
            shape((6, 128, 128)), shape((6, 128, 128), f32), shape((6, 128), f32),
        ],
        [pltpu.VMEM((6, 128, 128), f32)] * 3 + [pltpu.VMEM((4, 256, 128), bf16)]
        + [pltpu.VMEM((1024, width), bf16) for width in WIDTHS[EARLY:]]
        + [pltpu.SemaphoreType.DMA((3,))],
        24,
        3_000_000_000,
    )(other.reshape(256, 1024), line(norm_gain), squares, decay_base, rate_base, *halves_of, *weights[EARLY:])
    r1, r2, r3 = around((m1, m2, m3), "sp_1")
    reads, local, gate, pgate = call(
        side_kernel,
        "side",
        vmem(11),
        [shape((6, 128, 128)), shape((6, 128, 128), f32), shape((256, 384)), shape((256, 256))],
        [],
        16,
        1_000_000_000,
    )(own_normed, normed, scale, right, solved, v, r, grow, lift, w_gate_rec, w_gate_pool)
    prefix, onward, total = call(
        row_kernel,
        "row",
        vmem(4) + [pl.BlockSpec(memory_space=pl.ANY)],
        [shape((3, 2, 128, 128), f32), shape((320, 128)), shape((256, 128))],
        [pltpu.VMEM((4, 256, 128), bf16)],
        8,
        100_000_000,
    )(home, r1, r2, r3, pgate)
    columns = around((onward, total, total), "sp_0")
    s0, s1, s2, s3 = call(
        column_kernel,
        "column",
        vmem(5),
        [shape((2, 64, 128))] * 4,
        [pltpu.VMEM((4, 2, 64, 128), bf16), pltpu.VMEM((4, 256, 128), bf16)],
        8,
        100_000_000,
    )(prefix, *columns, init_state)
    t1, t2, t3 = around((s1, s2, s3), "sp_1")
    pool_part = call(
        pool_kernel, "pool", vmem(7), shape((256, D), f32), [pltpu.VMEM((256, 256), bf16)], 12, 300_000_000
    )(pool, r1, columns[0], pgate, pool_mix, line(pool_scale), w_out_pool)
    send, keep = call(
        final_kernel,
        "final",
        vmem(10),
        [shape((256, 1024)), shape((256, 1024))],
        [pltpu.VMEM((4, 2, 64, 128), bf16), pltpu.VMEM((256, 384), bf16)],
        20,
        1_000_000_000,
    )(s0, t1, t2, t3, reads, local, gate, head_gain, pool_part, w_out_rec)
    arrived = lax.ppermute(send, "tp", [(0, 1), (1, 0)])
    mixed = keep.astype(f32) + arrived.astype(f32)
    return mixed.astype(bf16).reshape(2, 128, 1024)


def solution(mesh):
    split = Mesh(
        mesh.devices.reshape(4, 4, mesh.shape["fs"], mesh.shape["tp"]), ("sp_0", "sp_1", "fs", "tp")
    )
    column = P(None, "tp")
    placed = (
        (P("fs", SP, "tp"), P()) + (column,) * 8 + (P(),) * 5
        + (P("tp", None), P("tp", None), P("fs", "tp", None, None))
    )
    return jax.shard_map(
        shards, mesh=split, in_specs=placed, out_specs=P("fs", SP, "tp"), check_vma=False
    )
```

```python
import functools

import jax
import jax.numpy as jnp
from jax import lax
from jax.experimental import pallas as pl
from jax.experimental.pallas import tpu as pltpu
from jax.sharding import Mesh
from jax.sharding import PartitionSpec as P

D = 2048
HEAD = 64
SPAN = 128
UNITS = 6
SP = ("sp_0", "sp_1")
f32 = jnp.float32
bf16 = jnp.bfloat16
NN = ((1,), (0,))
NT = ((1,), (1,))
TN = ((0,), (0,))
MIB = 2**20


def dot(a, b, dims=NN):
    return lax.dot_general(
        a.astype(bf16), b.astype(bf16), (dims, ((), ())), preferred_element_type=f32
    )


def halves(x):
    high = x.astype(bf16)
    return high, (x - high.astype(f32)).astype(bf16)


def dot_fine_left(a, b, dims=NN):
    high, low = halves(a)
    return dot(high, b, dims) + dot(low, b, dims)


def dot_fine_right(a, b, dims=NN):
    high, low = halves(b)
    return dot(a, high, dims) + dot(a, low, dims)


def iota(rows, cols, dim):
    return lax.broadcasted_iota(jnp.int32, (rows, cols), dim)


def line_of(ref, lanes):
    if len(ref.shape) == 1:
        return ref[lanes].reshape(1, 128)
    return ref[:, lanes]


def head_masks():
    first = (iota(1, 128, 1) < HEAD).astype(f32)
    return first.astype(bf16), (1.0 - first).astype(bf16)


def both(x, masks):
    x = x.astype(bf16)
    return jnp.concatenate([x * masks[0], x * masks[1]], axis=0)


def joined(x):
    return jnp.where(iota(HEAD, 128, 1) < HEAD, x[:HEAD], x[HEAD:])


def compose(earlier, later, masks):
    moved = dot_fine_left(earlier, both(later[:HEAD], masks))
    written = later[HEAD:].astype(f32)
    if earlier.shape[0] == HEAD:
        return moved + written
    return jnp.concatenate([moved[:HEAD], moved[HEAD:] + written], axis=0)


def pick(x, size, odd):
    parts = [x[s : s + size] for s in range(size * odd, SPAN, 2 * size)]
    return parts[0] if len(parts) == 1 else jnp.concatenate(parts, axis=0)


def weave(even, odd, size):
    parts = []
    for s in range(0, SPAN // 2, size):
        parts += [even[s : s + size], odd[s : s + size]]
    return jnp.concatenate(parts, axis=0)


def woven(part, size):
    if size >= 16:
        part = part.astype(bf16)
    return weave(jnp.zeros_like(part), part, size)


def blocks(x):
    x = x.astype(bf16)
    zero = jnp.zeros((SPAN, 128), bf16)
    return jnp.concatenate(
        [jnp.concatenate([x[:, :128], zero], axis=1), jnp.concatenate([zero, x[:, 128:]], axis=1)], axis=0
    )


def inverses(lowers, fill):
    row, col = iota(SPAN, 256, 0), iota(SPAN, 256, 1) & 127
    eye = (row == col).astype(f32)
    near = ((row >> 1) == (col >> 1)).astype(bf16)
    result = [eye - (lower * near).astype(f32) for lower in lowers]
    size, level = 2, 1
    while size < SPAN:
        off = (((row >> (level + 1)) == (col >> (level + 1))) & ((row >> level) != (col >> level))).astype(bf16)
        if size < 8:
            inner = [dot(lower * off, blocks(inv)) for lower, inv in zip(lowers, result)]
            fill(level)
            result = [inv - dot(inv, blocks(part)) for inv, part in zip(result, inner)]
        else:
            if size < 16:
                off = pick(off.astype(f32), size, 1).astype(bf16)
                odd = [pick(lower.astype(f32), size, 1).astype(bf16) for lower in lowers]
            else:
                off = pick(off, size, 1)
                odd = [pick(lower, size, 1) for lower in lowers]
            inner = [dot(lower * off, blocks(inv)) for lower, inv in zip(odd, result)]
            fill(level)
            outer = [
                dot(pick(inv, size, 1), blocks(woven(part, size))) for inv, part in zip(result, inner)
            ]
            result = [
                weave(pick(inv, size, 0), pick(inv, size, 1) - part, size)
                for inv, part in zip(result, outer)
            ]
        size, level = size * 2, level + 1
    return result


GROUPS = ((384, 384), (384, 384), (384, 256))
WIDE = tuple(sum(group) for group in GROUPS)


def fetch(sources, buf, first_row, sems, base):
    copies, at = [], 0
    for i, src in enumerate(sources):
        width = src.shape[1]
        copies.append(
            pltpu.make_async_copy(
                src.at[pl.ds(pl.multiple_of(first_row, 1024), 1024), :],
                buf.at[:, at : at + width],
                sems.at[base + i],
            )
        )
        at += width
    return copies


def begin(copies):
    for copy in copies:
        copy.start()


def finish(copies):
    for copy in copies:
        copy.wait()


def own_kernel(*refs):
    token_ref, norm_ref = refs[:2]
    sources, normed_ref, squares_ref, partials, rest = refs[2:8], refs[8], refs[9], refs[10:13], refs[13]
    bufs, sems, own_ref, gain_ref, first_sems = refs[14:17], refs[17], refs[18], refs[19], refs[20]
    tp = lax.axis_index("tp")
    early = [
        pltpu.make_async_copy(norm_ref, gain_ref, first_sems.at[0]),
        pltpu.make_async_copy(token_ref, own_ref, first_sems.at[1]),
    ]
    mine = [fetch(sources[2 * i : 2 * i + 2], bufs[i], tp * 1024, sems, 2 * i) for i in range(3)]
    others = fetch(sources[:2], rest, (1 - tp) * 1024, sems, 6)
    begin(early)
    begin(mine[0])
    finish(early)
    begin(mine[1])
    own = own_ref[...].astype(f32)
    normed = (own * jnp.where(tp == 0, gain_ref[:, :1024], gain_ref[:, 1024:])).astype(bf16)
    normed_ref[...] = normed
    squares_ref[...] = jnp.broadcast_to(jnp.sum(own * own, axis=1, keepdims=True), (256, 128))
    for i in range(3):
        finish(mine[i])
        if i == 0:
            begin(mine[2])
        if i == 1:
            begin(others)
        partials[i][...] = dot(normed, bufs[i][...])
    finish(others)


def local_kernel(*refs):
    other_ref, gain_ref, squares_ref, db_ref, rb_ref = refs[:5]
    partials, ready, sources = refs[5:8], refs[8], refs[9:13]
    (
        normed_ref, scale_ref, pool_ref, home_ref, first_ref, second_ref, third_ref,
        right_ref, solved_ref, v_ref, r_ref, grow_ref, lift_ref,
    ) = refs[13:26]
    k_s, d_s, a_s, maps = refs[26:30]
    bufs, sems = refs[30:32], refs[32]
    tp = lax.axis_index("tp")
    y = lax.axis_index("sp_1")
    copies = [
        fetch(sources[2 * i : 2 * i + 2], bufs[i], (1 - tp) * 1024, sems, 2 * i) for i in range(2)
    ]
    begin(copies[0])
    begin(copies[1])
    rest = (ready,) + tuple(bufs)
    is_first = tp == 0
    other = other_ref[...].astype(f32)
    normed = (other * jnp.where(is_first, gain_ref[:, 1024:], gain_ref[:, :1024])).astype(bf16)
    normed_ref[...] = normed
    squares = squares_ref[:, :1] + jnp.sum(other * other, axis=1, keepdims=True)
    scale = lax.rsqrt(squares * (1.0 / D) + 0.25)
    scale_ref[...] = jnp.broadcast_to(scale, (256, 128))

    def project(i):
        total = partials[i][...] + dot(normed_ref[...], rest[i][...])
        return (total * scale_ref[:, :1]).astype(bf16)

    def place(dest, rounded, at, kind):
        for u in range(UNITS):
            s, h = u // 3, u % 3
            dest[u] = rounded[s * 128 : s * 128 + 128, at + h * 128 : at + h * 128 + 128].astype(kind)

    rounded = project(0)
    place(k_s, rounded, 0, f32)
    place(d_s, rounded, 384, f32)

    def fill(level):
        if level != 1:
            return
        rounded = project(2)
        place(r_ref, rounded, 0, bf16)
        pool = rounded[:, 384:]
        pool_ref[...] = pool
        for s in (0, 1):
            for half in (0, 1):
                at = 256 + (2 * s + half) * 16
                first_ref[at : at + 16] = pool[s * 128 + 112 : s * 128 + 128, half * 128 : half * 128 + 128]

    masks = head_masks()
    n = SPAN
    row, col = iota(n, n, 0), iota(n, n, 1)
    strict, inclusive = row > col, row >= col
    triangle = inclusive.astype(f32)
    ones = ((row >> 6) == (col >> 6)).astype(f32)
    wide = (
        jnp.concatenate([masks[0], masks[0]], axis=1),
        jnp.concatenate([masks[1], masks[1]], axis=1),
    )
    slab = iota(HEAD, 128, 0)
    eye = (slab == (iota(HEAD, 128, 1) & 63)).astype(f32)
    units = range(UNITS)
    first_stage = []
    for u in units:
        h = u % 3
        lanes = slice(h * 128, h * 128 + 128)
        shifted = slice(384 + h * 128, 384 + h * 128 + 128)
        db = jnp.where(is_first, line_of(db_ref, lanes), line_of(db_ref, shifted))
        k = k_s[u]
        log_decay = -0.6065306597126334 * jax.nn.sigmoid(db + d_s[u])
        first_stage.append((log_decay, dot(k * k, ones), dot_fine_right(triangle, log_decay)))
    finish(copies[0])
    rounded = project(1)
    place(a_s, rounded, 0, f32)
    place(v_ref, rounded, 384, bf16)
    second_stage = []
    for u in units:
        h = u % 3
        lanes = slice(h * 128, h * 128 + 128)
        shifted = slice(384 + h * 128, 384 + h * 128 + 128)
        rb = jnp.where(is_first, line_of(rb_ref, lanes), line_of(rb_ref, shifted))
        rate = jax.nn.sigmoid(rb + a_s[u])
        log_decay, squared, total = first_stage[u]
        k = k_s[u]
        middle = total[63:64]
        unit_key = k * lax.rsqrt(squared + 1.0)
        centred = total - middle
        alpha = jnp.exp(centred - log_decay) * unit_key
        fading = jnp.exp(-centred)
        grow_ref[u] = jnp.exp(centred)
        lift = jnp.exp(middle)
        lift_ref[u : u + 1] = lift
        right = jnp.concatenate(
            [(unit_key * rate * fading).astype(bf16), (k * fading).astype(bf16)], axis=0
        )
        right_ref[u] = right
        ends = (jnp.exp(total[127:128]), jnp.exp(centred[127:128]))
        second_stage.append((right, alpha * lift, ends, dot(both(alpha, masks), right, NT)))
    finish(copies[1])
    lowers, carries = [], []
    for u in units:
        pairs = second_stage[u][3]
        block = lambda j, c: jnp.where(
            strict, pairs[j * n : j * n + n, c * n : c * n + n], 0.0
        ).astype(bf16)
        lowers.append(jnp.concatenate([block(0, 0), block(1, 0)], axis=1))
        carries.append(jnp.concatenate([block(0, 1), block(1, 1)], axis=1))
    inverse = inverses(lowers, fill)
    carries = [dot(carries[u], both(v_ref[u], masks)) for u in units]
    solutions = []
    for u in units:
        wanted = jnp.concatenate([second_stage[u][1].astype(bf16), carries[u].astype(bf16)], axis=1)
        solved = dot(inverse[u], both(wanted, wide)).astype(bf16)
        solved_ref[u] = solved
        solutions.append(solved)
    for u in units:
        right, _, ends, _ = second_stage[u]
        solved = solutions[u]
        transit = eye * ends[0] - joined(dot(solved[:, :n], right[:n], TN)) * ends[1]
        written = joined(
            dot(
                jnp.concatenate([-solved[:, n:], v_ref[u]], axis=0),
                right,
                TN,
            )
        ) * ends[1]
        at = (u // 3) * 128
        maps[u % 3, at : at + HEAD] = transit.astype(bf16)
        maps[u % 3, at + HEAD : at + 128] = written.astype(bf16)
    maps[3] = jnp.zeros((256, 128), bf16)
    for step, dest in enumerate((home_ref, first_ref, second_ref, third_ref)):
        dest[:256] = maps[(y + step) & 3]


def side_kernel(
    own_ref, other_ref, scale_ref, right_ref, solved_ref, v_ref, r_ref, grow_ref, lift_ref, wg_ref, wq_ref,
    reads_ref, local_ref, gate_ref, pgate_ref,
    buf, sems,
):
    tp = lax.axis_index("tp")
    copies = [
        pltpu.make_async_copy(wg_ref, buf.at[:, :384], sems.at[0]),
        pltpu.make_async_copy(wq_ref, buf.at[:, 384:], sems.at[1]),
    ]
    begin(copies)
    masks = head_masks()
    wide = (
        jnp.concatenate([masks[0], masks[0]], axis=1),
        jnp.concatenate([masks[1], masks[1]], axis=1),
    )
    inclusive = iota(128, 128, 0) >= iota(128, 128, 1)
    inside, rhos = [], []
    for u in range(UNITS):
        rho = r_ref[u].astype(f32) * grow_ref[u]
        rhos.append(rho * lift_ref[u : u + 1])
        pairs = dot(both(rho, masks), right_ref[u], NT)
        block = lambda j, c: jnp.where(
            inclusive, pairs[j * 128 : j * 128 + 128, c * 128 : c * 128 + 128], 0.0
        ).astype(bf16)
        inside.append([jnp.concatenate([block(0, c), block(1, c)], axis=1) for c in (0, 1)])
    for u in range(UNITS):
        removed = dot(inside[u][0], both(solved_ref[u], wide))
        reads_ref[u] = (rhos[u] - removed[:, :128]).astype(bf16)
        local_ref[u] = dot(inside[u][1], both(v_ref[u], masks)) - removed[:, 128:]
    scale = scale_ref[:, :1]
    mine, theirs = pl.multiple_of(tp * 1024, 1024), pl.multiple_of((1 - tp) * 1024, 1024)
    finish(copies)
    total = dot(own_ref[...], buf[pl.ds(mine, 1024), :]) + dot(other_ref[...], buf[pl.ds(theirs, 1024), :])
    rounded = (total * scale).astype(bf16)
    gate_ref[...] = rounded[:, :384]
    pgate_ref[...] = rounded[:, 384:]


def row_kernel(home_ref, first_ref, second_ref, third_ref, after_ref, prefix_ref, next_ref, total_ref, maps):
    y = lax.axis_index("sp_1")
    for step, src in enumerate((home_ref, first_ref, second_ref, third_ref)):
        maps[(y + 4 - step) & 3] = src[:256]
    next_ref[256:] = first_ref[256:]
    masks = head_masks()
    for s in (0, 1):
        rows = slice(s * 128, s * 128 + 128)
        so_far = maps[0, rows].astype(f32)
        prefix_ref[0, s] = so_far
        for j in (1, 2, 3):
            so_far = compose(so_far, maps[j, rows], masks)
            if j < 3:
                prefix_ref[j, s] = so_far
            else:
                next_ref[rows] = so_far.astype(bf16)
                total_ref[rows] = so_far.astype(bf16)


def column_kernel(
    prefix_ref, first_ref, second_ref, third_ref, init_ref,
    home_ref, one_ref, two_ref, three_ref,
    starts, rows,
):
    y = lax.axis_index("sp_1")
    z = lax.axis_index("sp_0")
    for step, src in enumerate((first_ref, second_ref, third_ref)):
        rows[(z + 3 - step) & 3] = src[:256]
    masks = head_masks()
    pair = jnp.minimum(y, 2) * 2
    for s in (0, 1):
        state = jnp.concatenate([init_ref[s, pair], init_ref[s, pair + 1]], axis=1)
        for j in range(3):
            state = jnp.where(j < z, compose(state, rows[j, s * 128 : s * 128 + 128], masks), state)
        starts[0, s] = state.astype(bf16)
        for j in range(3):
            starts[j + 1, s] = compose(state, prefix_ref[j, s], masks).astype(bf16)
    for step, dest in enumerate((home_ref, one_ref, two_ref, three_ref)):
        dest[...] = starts[(y + step) & 3]


def pool_kernel(pool_ref, beside_ref, above_ref, pgate_ref, mix_ref, pscale_ref, wp_ref, part_ref, out_ref):
    tp = lax.axis_index("tp")
    y = lax.axis_index("sp_1")
    place = lax.axis_index("sp_0") * 4 + y
    is_first = tp == 0
    factor = jnp.where(is_first, pscale_ref[:, :256], pscale_ref[:, 256:])
    for s in (0, 1):
        current = pool_ref[s * 128 : s * 128 + 128].astype(f32)
        tails = []
        for half in (0, 1):
            rows = slice(256 + (2 * s + half) * 16, 272 + (2 * s + half) * 16)
            tails.append(
                jnp.where(
                    place == 0,
                    0.0,
                    jnp.where(y > 0, beside_ref[rows].astype(f32), above_ref[rows].astype(f32)),
                )
            )
        padded = jnp.concatenate([jnp.concatenate(tails, axis=1), current], axis=0)
        sums = {1: padded}
        for by in (1, 2, 4, 8):
            before = sums[by]
            moved = jnp.concatenate([jnp.zeros((by, 256), f32), before[: 144 - by]], axis=0)
            sums[2 * by] = before + moved
        position = (place * 128 + iota(128, 128, 0) + 1).astype(f32)
        for g in (0, 1):
            lanes = slice(g * 128, g * 128 + 128)
            small, large = 2 << g, 8 << g
            trailing = jnp.where(is_first, sums[small][16:, lanes], sums[large][16:, lanes])
            window = jnp.where(is_first, float(small), float(large))
            diffs = trailing / jnp.minimum(position, window) - current[:, lanes]
            mixed = dot(diffs.astype(bf16), mix_ref[tp * 2 + g])
            gate = pgate_ref[s * 128 : s * 128 + 128, lanes].astype(f32)
            out_ref[s * 128 : s * 128 + 128, lanes] = (
                mixed * factor[:, lanes] * (gate * jax.nn.sigmoid(gate))
            ).astype(bf16)
    part_ref[...] = dot(out_ref[...], wp_ref[...])


def final_kernel(
    home_ref, one_ref, two_ref, three_ref, reads_ref, local_ref, gate_ref, hgain_ref, part_ref,
    wr_ref,
    send_ref, rec,
    starts,
):
    tp = lax.axis_index("tp")
    y = lax.axis_index("sp_1")
    for step, src in enumerate((home_ref, one_ref, two_ref, three_ref)):
        starts[(y + 4 - step) & 3] = src[...]
    masks = head_masks()
    row, col = iota(128, 128, 0), iota(128, 128, 1)
    mean_of = jnp.where((row >> 6) == (col >> 6), 1.0 / HEAD, 0.0).astype(bf16)
    is_first = tp == 0
    for u in range(UNITS):
        s, h = u // 3, u % 3
        lanes = slice(h * 128, h * 128 + 128)
        shifted = slice(384 + h * 128, 384 + h * 128 + 128)
        rows = slice(s * 128, s * 128 + 128)
        out = dot(reads_ref[u], both(starts[h, s], masks), NT) + local_ref[u]
        out = out - dot_fine_left(out, mean_of)
        spread = dot_fine_left(out * out, mean_of)
        gain = jnp.where(is_first, line_of(hgain_ref, lanes), line_of(hgain_ref, shifted))
        gate = gate_ref[rows, lanes].astype(f32)
        rec[rows, lanes] = (
            out * lax.rsqrt(spread + 1.0) * gain * (gate * jax.nn.sigmoid(gate))
        ).astype(bf16)
    cols = pl.ds(pl.multiple_of((1 - tp) * 1024, 1024), 1024)
    send_ref[...] = (dot(rec[...], wr_ref[:, cols]) + part_ref[:, cols]).astype(bf16)


def keep_kernel(rec_ref, part_ref, wr_ref, keep_ref):
    cols = pl.ds(pl.multiple_of(lax.axis_index("tp") * 1024, 1024), 1024)
    keep_ref[...] = (dot(rec_ref[...], wr_ref[:, cols]) + part_ref[:, cols]).astype(bf16)


def vmem(count):
    return [pl.BlockSpec(memory_space=pltpu.VMEM)] * count


def hbm(count):
    return [pl.BlockSpec(memory_space=pltpu.HBM)] * count


def shape(dims, kind=bf16):
    return jax.ShapeDtypeStruct(dims, kind)


def call(body, name, ins, outs, scratch, limit, flops=0):
    return pl.pallas_call(
        body,
        name=name,
        out_shape=outs,
        in_specs=ins,
        out_specs=vmem(len(outs)) if isinstance(outs, (list, tuple)) else vmem(1)[0],
        scratch_shapes=scratch,
        compiler_params=pltpu.CompilerParams(vmem_limit_bytes=limit * MIB),
        cost_estimate=pl.CostEstimate(flops=flops, transcendentals=0, bytes_accessed=0) if flops else None,
    )


def around(parts, axis):
    return [
        lax.ppermute(part, axis, [(i, (i + step) & 3) for i in range(4)]) for step, part in enumerate(parts, 1)
    ]


def shards(
    tokens, norm_gain, w_recept, w_key, w_value, w_decay, w_rate, w_gate_rec, w_pool, w_gate_pool,
    decay_base, rate_base, head_gain, pool_mix, pool_scale, w_out_rec, w_out_pool, init_state,
):
    other = lax.ppermute(tokens, "tp", [(0, 1), (1, 0)])
    line = lambda x: x.reshape(1, -1)
    pinned = lambda x: pltpu.with_memory_space_constraint(x, pltpu.HBM)
    weights = [pinned(w) for w in (w_key, w_decay, w_rate, w_value, w_recept, w_pool)]
    own_normed, squares, *prepared = call(
        own_kernel,
        "own",
        hbm(8),
        [shape((256, 1024)), shape((256, 128), f32)]
        + [shape((256, width), f32) for width in WIDE]
        + [shape((1024, WIDE[0]))],
        [pltpu.VMEM((1024, width), bf16) for width in WIDE]
        + [
            pltpu.SemaphoreType.DMA((8,)), pltpu.VMEM((256, 1024), bf16), pltpu.VMEM((1, D), f32),
            pltpu.SemaphoreType.DMA((2,)),
        ],
        20,
        1_000_000_000,
    )(pinned(tokens.reshape(256, 1024)), pinned(line(norm_gain)), *weights)
    normed, scale, pool, home, m1, m2, m3, right, solved, v, r, grow, lift = call(
        local_kernel,
        "local",
        vmem(9) + hbm(4),
        [
            shape((256, 1024)), shape((256, 128), f32), shape((256, 256)),
            shape((256, 128)), shape((320, 128)), shape((256, 128)), shape((256, 128)),
            shape((6, 256, 128)), shape((6, 128, 256)), shape((6, 128, 128)),
            shape((6, 128, 128)), shape((6, 128, 128), f32), shape((6, 128), f32),
        ],
        [pltpu.VMEM((6, 128, 128), f32)] * 3
        + [pltpu.VMEM((4, 256, 128), bf16)]
        + [pltpu.VMEM((1024, width), bf16) for width in WIDE[1:]]
        + [pltpu.SemaphoreType.DMA((4,))],
        24,
        3_000_000_000,
    )(
        other.reshape(256, 1024), line(norm_gain), squares, decay_base, rate_base, *prepared, *weights[2:]
    )
    r1, r2, r3 = around((m1, m2, m3), "sp_1")
    reads, local, gate, pgate = call(
        side_kernel,
        "side",
        vmem(9) + hbm(2),
        [shape((6, 128, 128)), shape((6, 128, 128), f32), shape((256, 384)), shape((256, 256))],
        [pltpu.VMEM((D, 640), bf16), pltpu.SemaphoreType.DMA((2,))],
        16,
        1_000_000_000,
    )(own_normed, normed, scale, right, solved, v, r, grow, lift, pinned(w_gate_rec), pinned(w_gate_pool))
    prefix, onward, total = call(
        row_kernel,
        "row",
        vmem(4) + [pl.BlockSpec(memory_space=pl.ANY)],
        [shape((3, 2, 128, 128), f32), shape((320, 128)), shape((256, 128))],
        [pltpu.VMEM((4, 256, 128), bf16)],
        8,
        100_000_000,
    )(home, r1, r2, r3, pgate)
    columns = around((onward, total, total), "sp_0")
    s0, s1, s2, s3 = call(
        column_kernel,
        "column",
        vmem(5),
        [shape((2, 64, 128))] * 4,
        [pltpu.VMEM((4, 2, 64, 128), bf16), pltpu.VMEM((4, 256, 128), bf16)],
        8,
        100_000_000,
    )(prefix, *columns, init_state)
    t1, t2, t3 = around((s1, s2, s3), "sp_1")
    pool_part = call(
        pool_kernel, "pool", vmem(7), shape((256, D), f32), [pltpu.VMEM((256, 256), bf16)], 12, 300_000_000
    )(pool, r1, columns[0], pgate, pool_mix, line(pool_scale), w_out_pool)
    send, rec = call(
        final_kernel,
        "final",
        vmem(10),
        [shape((256, 1024)), shape((256, 384))],
        [pltpu.VMEM((4, 2, 64, 128), bf16)],
        20,
        1_000_000_000,
    )(s0, t1, t2, t3, reads, local, gate, head_gain, pool_part, w_out_rec)
    arrived = lax.ppermute(send, "tp", [(0, 1), (1, 0)])
    keep = call(keep_kernel, "keep", vmem(3), shape((256, 1024)), [], 8, 300_000_000)(rec, pool_part, w_out_rec)
    mixed = keep.astype(f32) + arrived.astype(f32)
    return mixed.astype(bf16).reshape(2, 128, 1024)


def solution(mesh):
    split = Mesh(
        mesh.devices.reshape(4, 4, mesh.shape["fs"], mesh.shape["tp"]), ("sp_0", "sp_1", "fs", "tp")
    )
    column = P(None, "tp")
    placed = (
        (P("fs", SP, "tp"), P()) + (column,) * 8 + (P(),) * 5
        + (P("tp", None), P("tp", None), P("fs", "tp", None, None))
    )
    return jax.shard_map(
        shards, mesh=split, in_specs=placed, out_specs=P("fs", SP, "tp"), check_vma=False
    )
```

```python
import functools

import jax
import jax.numpy as jnp
from jax import lax
from jax.experimental import pallas as pl
from jax.experimental.pallas import tpu as pltpu
from jax.sharding import Mesh
from jax.sharding import PartitionSpec as P

D = 2048
HEAD = 64
SPAN = 128
UNITS = 6
SP = ("sp_0", "sp_1")
f32 = jnp.float32
bf16 = jnp.bfloat16
NN = ((1,), (0,))
NT = ((1,), (1,))
TN = ((0,), (0,))
MIB = 2**20


def dot(a, b, dims=NN):
    return lax.dot_general(
        a.astype(bf16), b.astype(bf16), (dims, ((), ())), preferred_element_type=f32
    )


def halves(x):
    high = x.astype(bf16)
    return high, (x - high.astype(f32)).astype(bf16)


def dot_fine_left(a, b, dims=NN):
    high, low = halves(a)
    return dot(high, b, dims) + dot(low, b, dims)


def dot_fine_right(a, b, dims=NN):
    high, low = halves(b)
    return dot(a, high, dims) + dot(a, low, dims)


def iota(rows, cols, dim):
    return lax.broadcasted_iota(jnp.int32, (rows, cols), dim)


def line_of(ref, lanes):
    if len(ref.shape) == 1:
        return ref[lanes].reshape(1, 128)
    return ref[:, lanes]


def head_masks():
    first = (iota(1, 128, 1) < HEAD).astype(f32)
    return first.astype(bf16), (1.0 - first).astype(bf16)


def both(x, masks):
    x = x.astype(bf16)
    return jnp.concatenate([x * masks[0], x * masks[1]], axis=0)


def joined(x):
    return jnp.where(iota(HEAD, 128, 1) < HEAD, x[:HEAD], x[HEAD:])


def compose(earlier, later, masks):
    moved = dot_fine_left(earlier, both(later[:HEAD], masks))
    written = later[HEAD:].astype(f32)
    if earlier.shape[0] == HEAD:
        return moved + written
    return jnp.concatenate([moved[:HEAD], moved[HEAD:] + written], axis=0)


def pick(x, size, odd):
    parts = [x[s : s + size] for s in range(size * odd, SPAN, 2 * size)]
    return parts[0] if len(parts) == 1 else jnp.concatenate(parts, axis=0)


def weave(even, odd, size):
    parts = []
    for s in range(0, SPAN // 2, size):
        parts += [even[s : s + size], odd[s : s + size]]
    return jnp.concatenate(parts, axis=0)


def woven(part, size):
    if size >= 16:
        part = part.astype(bf16)
    return weave(jnp.zeros_like(part), part, size)


def blocks(x):
    x = x.astype(bf16)
    zero = jnp.zeros((SPAN, 128), bf16)
    return jnp.concatenate(
        [jnp.concatenate([x[:, :128], zero], axis=1), jnp.concatenate([zero, x[:, 128:]], axis=1)], axis=0
    )


def inverses(lowers, fill):
    row, col = iota(SPAN, 256, 0), iota(SPAN, 256, 1) & 127
    eye = (row == col).astype(f32)
    near = ((row >> 1) == (col >> 1)).astype(bf16)
    result = [eye - (lower * near).astype(f32) for lower in lowers]
    size, level = 2, 1
    while size < SPAN:
        off = (((row >> (level + 1)) == (col >> (level + 1))) & ((row >> level) != (col >> level))).astype(bf16)
        if size < 8:
            inner = [dot(lower * off, blocks(inv)) for lower, inv in zip(lowers, result)]
            fill(level)
            result = [inv - dot(inv, blocks(part)) for inv, part in zip(result, inner)]
        else:
            if size < 16:
                off = pick(off.astype(f32), size, 1).astype(bf16)
                odd = [pick(lower.astype(f32), size, 1).astype(bf16) for lower in lowers]
            else:
                off = pick(off, size, 1)
                odd = [pick(lower, size, 1) for lower in lowers]
            inner = [dot(lower * off, blocks(inv)) for lower, inv in zip(odd, result)]
            fill(level)
            outer = [
                dot(pick(inv, size, 1), blocks(woven(part, size))) for inv, part in zip(result, inner)
            ]
            result = [
                weave(pick(inv, size, 0), pick(inv, size, 1) - part, size)
                for inv, part in zip(result, outer)
            ]
        size, level = size * 2, level + 1
    return result


def fetch(sources, buf, first_row, sems, base):
    copies, at = [], 0
    for i, src in enumerate(sources):
        width = src.shape[1]
        copies.append(
            pltpu.make_async_copy(
                src.at[pl.ds(pl.multiple_of(first_row, 1024), 1024), :],
                buf.at[:, at : at + width],
                sems.at[base + i],
            )
        )
        at += width
    return copies


def begin(copies):
    for copy in copies:
        copy.start()


def finish(copies):
    for copy in copies:
        copy.wait()


def own_kernel(*refs):
    token_ref, norm_ref = refs[:2]
    sources, normed_ref, squares_ref, partials, rest = refs[2:6], refs[6], refs[7], refs[8:10], refs[10:12]
    bufs, sems, own_ref, gain_ref, first_sems = refs[12:14], refs[14], refs[15], refs[16], refs[17]
    tp = lax.axis_index("tp")
    early = [
        pltpu.make_async_copy(norm_ref, gain_ref, first_sems.at[0]),
        pltpu.make_async_copy(token_ref, own_ref, first_sems.at[1]),
    ]
    mine = [fetch(sources[2 * i : 2 * i + 2], bufs[i], tp * 1024, sems, 2 * i) for i in range(2)]
    others = [
        fetch(sources[2 * i : 2 * i + 2], rest[i], (1 - tp) * 1024, sems, 4 + 2 * i) for i in range(2)
    ]
    begin(early)
    begin(mine[0])
    pl.delay(400)
    begin(mine[1])
    pl.delay(400)
    begin(others[0])
    finish(early)
    own = own_ref[...].astype(f32)
    normed = (own * jnp.where(tp == 0, gain_ref[:, :1024], gain_ref[:, 1024:])).astype(bf16)
    normed_ref[...] = normed
    squares_ref[...] = jnp.broadcast_to(jnp.sum(own * own, axis=1, keepdims=True), (256, 128))
    begin(others[1])
    for i in range(2):
        finish(mine[i])
        partials[i][...] = dot(normed_ref[...], bufs[i][...])
    finish(others[0])
    finish(others[1])


def local_kernel(*refs):
    other_ref, own_ref, gain_ref, squares_ref, db_ref, rb_ref = refs[:6]
    partials, rest, pool_weight = refs[6:8], refs[8:10], refs[10]
    (
        normed_ref, scale_ref, pool_ref, home_ref, first_ref, second_ref, third_ref,
        right_ref, solved_ref, v_ref, grow_ref, lift_ref,
    ) = refs[11:23]
    k_s, d_s, a_s, maps, pool_buf, sems = refs[23:29]
    tp = lax.axis_index("tp")
    y = lax.axis_index("sp_1")
    copy = pltpu.make_async_copy(pool_weight, pool_buf, sems.at[0])
    copy.start()
    is_first = tp == 0
    other = other_ref[...].astype(f32)
    normed = (other * jnp.where(is_first, gain_ref[:, 1024:], gain_ref[:, :1024])).astype(bf16)
    normed_ref[...] = normed
    squares = squares_ref[:, :1] + jnp.sum(other * other, axis=1, keepdims=True)
    scale = lax.rsqrt(squares * (1.0 / D) + 0.25)
    scale_ref[...] = jnp.broadcast_to(scale, (256, 128))

    def project(i):
        total = partials[i][...] + dot(normed_ref[...], rest[i][...])
        return (total * scale_ref[:, :1]).astype(bf16)

    def place(dest, rounded, at, kind):
        for u in range(UNITS):
            s, h = u // 3, u % 3
            dest[u] = rounded[s * 128 : s * 128 + 128, at + h * 128 : at + h * 128 + 128].astype(kind)

    rounded = project(0)
    place(k_s, rounded, 0, f32)
    place(d_s, rounded, 384, f32)
    rounded = project(1)
    place(a_s, rounded, 0, f32)
    place(v_ref, rounded, 384, bf16)

    def fill(level):
        if level != 1:
            return
        total = dot(own_ref[...], pool_buf[pl.ds(pl.multiple_of(tp * 1024, 1024), 1024), :])
        total = total + dot(normed_ref[...], pool_buf[pl.ds(pl.multiple_of((1 - tp) * 1024, 1024), 1024), :])
        pool = (total * scale_ref[:, :1]).astype(bf16)
        pool_ref[...] = pool
        for s in (0, 1):
            for half in (0, 1):
                at = 256 + (2 * s + half) * 16
                first_ref[at : at + 16] = pool[s * 128 + 112 : s * 128 + 128, half * 128 : half * 128 + 128]

    masks = head_masks()
    n = SPAN
    row, col = iota(n, n, 0), iota(n, n, 1)
    strict, inclusive = row > col, row >= col
    triangle = inclusive.astype(f32)
    ones = ((row >> 6) == (col >> 6)).astype(f32)
    wide = (
        jnp.concatenate([masks[0], masks[0]], axis=1),
        jnp.concatenate([masks[1], masks[1]], axis=1),
    )
    slab = iota(HEAD, 128, 0)
    eye = (slab == (iota(HEAD, 128, 1) & 63)).astype(f32)
    units = range(UNITS)
    first_stage = []
    for u in units:
        h = u % 3
        lanes = slice(h * 128, h * 128 + 128)
        shifted = slice(384 + h * 128, 384 + h * 128 + 128)
        db = jnp.where(is_first, line_of(db_ref, lanes), line_of(db_ref, shifted))
        k = k_s[u]
        log_decay = -0.6065306597126334 * jax.nn.sigmoid(db + d_s[u])
        first_stage.append((log_decay, dot(k * k, ones), dot_fine_right(triangle, log_decay)))
    second_stage = []
    for u in units:
        h = u % 3
        lanes = slice(h * 128, h * 128 + 128)
        shifted = slice(384 + h * 128, 384 + h * 128 + 128)
        rb = jnp.where(is_first, line_of(rb_ref, lanes), line_of(rb_ref, shifted))
        rate = jax.nn.sigmoid(rb + a_s[u])
        log_decay, squared, total = first_stage[u]
        k = k_s[u]
        middle = total[63:64]
        unit_key = k * lax.rsqrt(squared + 1.0)
        centred = total - middle
        alpha = jnp.exp(centred - log_decay) * unit_key
        fading = jnp.exp(-centred)
        grow_ref[u] = jnp.exp(centred)
        lift = jnp.exp(middle)
        lift_ref[u : u + 1] = lift
        right = jnp.concatenate(
            [(unit_key * rate * fading).astype(bf16), (k * fading).astype(bf16)], axis=0
        )
        right_ref[u] = right
        ends = (jnp.exp(total[127:128]), jnp.exp(centred[127:128]))
        second_stage.append((right, alpha * lift, ends, dot(both(alpha, masks), right, NT)))
    copy.wait()
    lowers, carries = [], []
    for u in units:
        pairs = second_stage[u][3]
        block = lambda j, c: jnp.where(
            strict, pairs[j * n : j * n + n, c * n : c * n + n], 0.0
        ).astype(bf16)
        lowers.append(jnp.concatenate([block(0, 0), block(1, 0)], axis=1))
        carries.append(jnp.concatenate([block(0, 1), block(1, 1)], axis=1))
    inverse = inverses(lowers, fill)
    carries = [dot(carries[u], both(v_ref[u], masks)) for u in units]
    solutions = []
    for u in units:
        wanted = jnp.concatenate([second_stage[u][1].astype(bf16), carries[u].astype(bf16)], axis=1)
        solved = dot(inverse[u], both(wanted, wide)).astype(bf16)
        solved_ref[u] = solved
        solutions.append(solved)
    for u in units:
        right, _, ends, _ = second_stage[u]
        solved = solutions[u]
        transit = eye * ends[0] - joined(dot(solved[:, :n], right[:n], TN)) * ends[1]
        written = joined(
            dot(
                jnp.concatenate([-solved[:, n:], v_ref[u]], axis=0),
                right,
                TN,
            )
        ) * ends[1]
        at = (u // 3) * 128
        maps[u % 3, at : at + HEAD] = transit.astype(bf16)
        maps[u % 3, at + HEAD : at + 128] = written.astype(bf16)
    maps[3] = jnp.zeros((256, 128), bf16)
    for step, dest in enumerate((home_ref, first_ref, second_ref, third_ref)):
        dest[:256] = maps[(y + step) & 3]


def side_kernel(
    own_ref, other_ref, scale_ref, right_ref, solved_ref, v_ref, grow_ref, lift_ref, wr_ref, wg_ref, wq_ref,
    reads_ref, local_ref, gate_ref, pgate_ref,
):
    tp = lax.axis_index("tp")
    scale = scale_ref[:, :1]
    mine, theirs = pl.multiple_of(tp * 1024, 1024), pl.multiple_of((1 - tp) * 1024, 1024)

    def project(weight):
        total = dot(own_ref[...], weight[pl.ds(mine, 1024), :])
        total = total + dot(other_ref[...], weight[pl.ds(theirs, 1024), :])
        return (total * scale).astype(bf16)

    receptance = project(wr_ref)
    masks = head_masks()
    wide = (
        jnp.concatenate([masks[0], masks[0]], axis=1),
        jnp.concatenate([masks[1], masks[1]], axis=1),
    )
    inclusive = iota(128, 128, 0) >= iota(128, 128, 1)
    inside, rhos = [], []
    for u in range(UNITS):
        s, h = u // 3, u % 3
        rho = receptance[s * 128 : s * 128 + 128, h * 128 : h * 128 + 128].astype(f32) * grow_ref[u]
        rhos.append(rho * lift_ref[u : u + 1])
        pairs = dot(both(rho, masks), right_ref[u], NT)
        block = lambda j, c: jnp.where(
            inclusive, pairs[j * 128 : j * 128 + 128, c * 128 : c * 128 + 128], 0.0
        ).astype(bf16)
        inside.append([jnp.concatenate([block(0, c), block(1, c)], axis=1) for c in (0, 1)])
    for u in range(UNITS):
        removed = dot(inside[u][0], both(solved_ref[u], wide))
        reads_ref[u] = (rhos[u] - removed[:, :128]).astype(bf16)
        local_ref[u] = dot(inside[u][1], both(v_ref[u], masks)) - removed[:, 128:]
    gate_ref[...] = project(wg_ref)
    pgate_ref[...] = project(wq_ref)


def row_kernel(home_ref, first_ref, second_ref, third_ref, after_ref, prefix_ref, next_ref, total_ref, maps):
    y = lax.axis_index("sp_1")
    for step, src in enumerate((home_ref, first_ref, second_ref, third_ref)):
        maps[(y + 4 - step) & 3] = src[:256]
    next_ref[256:] = first_ref[256:]
    masks = head_masks()
    for s in (0, 1):
        rows = slice(s * 128, s * 128 + 128)
        so_far = maps[0, rows].astype(f32)
        prefix_ref[0, s] = so_far
        for j in (1, 2, 3):
            so_far = compose(so_far, maps[j, rows], masks)
            if j < 3:
                prefix_ref[j, s] = so_far
            else:
                next_ref[rows] = so_far.astype(bf16)
                total_ref[rows] = so_far.astype(bf16)


def column_kernel(
    prefix_ref, first_ref, second_ref, third_ref, init_ref,
    home_ref, one_ref, two_ref, three_ref,
    starts, rows,
):
    y = lax.axis_index("sp_1")
    z = lax.axis_index("sp_0")
    for step, src in enumerate((first_ref, second_ref, third_ref)):
        rows[(z + 3 - step) & 3] = src[:256]
    masks = head_masks()
    pair = jnp.minimum(y, 2) * 2
    for s in (0, 1):
        state = jnp.concatenate([init_ref[s, pair], init_ref[s, pair + 1]], axis=1)
        for j in range(3):
            state = jnp.where(j < z, compose(state, rows[j, s * 128 : s * 128 + 128], masks), state)
        starts[0, s] = state.astype(bf16)
        for j in range(3):
            starts[j + 1, s] = compose(state, prefix_ref[j, s], masks).astype(bf16)
    for step, dest in enumerate((home_ref, one_ref, two_ref, three_ref)):
        dest[...] = starts[(y + step) & 3]


def pool_kernel(pool_ref, beside_ref, above_ref, pgate_ref, mix_ref, pscale_ref, wp_ref, part_ref, out_ref):
    tp = lax.axis_index("tp")
    y = lax.axis_index("sp_1")
    place = lax.axis_index("sp_0") * 4 + y
    is_first = tp == 0
    factor = jnp.where(is_first, pscale_ref[:, :256], pscale_ref[:, 256:])
    for s in (0, 1):
        current = pool_ref[s * 128 : s * 128 + 128].astype(f32)
        tails = []
        for half in (0, 1):
            rows = slice(256 + (2 * s + half) * 16, 272 + (2 * s + half) * 16)
            tails.append(
                jnp.where(
                    place == 0,
                    0.0,
                    jnp.where(y > 0, beside_ref[rows].astype(f32), above_ref[rows].astype(f32)),
                )
            )
        padded = jnp.concatenate([jnp.concatenate(tails, axis=1), current], axis=0)
        sums = {1: padded}
        for by in (1, 2, 4, 8):
            before = sums[by]
            moved = jnp.concatenate([jnp.zeros((by, 256), f32), before[: 144 - by]], axis=0)
            sums[2 * by] = before + moved
        position = (place * 128 + iota(128, 128, 0) + 1).astype(f32)
        for g in (0, 1):
            lanes = slice(g * 128, g * 128 + 128)
            small, large = 2 << g, 8 << g
            trailing = jnp.where(is_first, sums[small][16:, lanes], sums[large][16:, lanes])
            window = jnp.where(is_first, float(small), float(large))
            diffs = trailing / jnp.minimum(position, window) - current[:, lanes]
            mixed = dot(diffs.astype(bf16), mix_ref[tp * 2 + g])
            gate = pgate_ref[s * 128 : s * 128 + 128, lanes].astype(f32)
            out_ref[s * 128 : s * 128 + 128, lanes] = (
                mixed * factor[:, lanes] * (gate * jax.nn.sigmoid(gate))
            ).astype(bf16)
    part_ref[...] = dot(out_ref[...], wp_ref[...])


def final_kernel(
    home_ref, one_ref, two_ref, three_ref, reads_ref, local_ref, gate_ref, hgain_ref, part_ref,
    wr_ref,
    send_ref, rec,
    starts,
):
    tp = lax.axis_index("tp")
    y = lax.axis_index("sp_1")
    for step, src in enumerate((home_ref, one_ref, two_ref, three_ref)):
        starts[(y + 4 - step) & 3] = src[...]
    masks = head_masks()
    row, col = iota(128, 128, 0), iota(128, 128, 1)
    mean_of = jnp.where((row >> 6) == (col >> 6), 1.0 / HEAD, 0.0).astype(bf16)
    is_first = tp == 0
    for u in range(UNITS):
        s, h = u // 3, u % 3
        lanes = slice(h * 128, h * 128 + 128)
        shifted = slice(384 + h * 128, 384 + h * 128 + 128)
        rows = slice(s * 128, s * 128 + 128)
        out = dot(reads_ref[u], both(starts[h, s], masks), NT) + local_ref[u]
        out = out - dot_fine_left(out, mean_of)
        spread = dot_fine_left(out * out, mean_of)
        gain = jnp.where(is_first, line_of(hgain_ref, lanes), line_of(hgain_ref, shifted))
        gate = gate_ref[rows, lanes].astype(f32)
        rec[rows, lanes] = (
            out * lax.rsqrt(spread + 1.0) * gain * (gate * jax.nn.sigmoid(gate))
        ).astype(bf16)
    cols = pl.ds(pl.multiple_of((1 - tp) * 1024, 1024), 1024)
    send_ref[...] = (dot(rec[...], wr_ref[:, cols]) + part_ref[:, cols]).astype(bf16)


def keep_kernel(rec_ref, part_ref, wr_ref, keep_ref):
    cols = pl.ds(pl.multiple_of(lax.axis_index("tp") * 1024, 1024), 1024)
    keep_ref[...] = (dot(rec_ref[...], wr_ref[:, cols]) + part_ref[:, cols]).astype(bf16)


def vmem(count):
    return [pl.BlockSpec(memory_space=pltpu.VMEM)] * count


def hbm(count):
    return [pl.BlockSpec(memory_space=pltpu.HBM)] * count


def shape(dims, kind=bf16):
    return jax.ShapeDtypeStruct(dims, kind)


def call(body, name, ins, outs, scratch, limit, flops=0):
    return pl.pallas_call(
        body,
        name=name,
        out_shape=outs,
        in_specs=ins,
        out_specs=vmem(len(outs)) if isinstance(outs, (list, tuple)) else vmem(1)[0],
        scratch_shapes=scratch,
        compiler_params=pltpu.CompilerParams(vmem_limit_bytes=limit * MIB),
        cost_estimate=pl.CostEstimate(flops=flops, transcendentals=0, bytes_accessed=0) if flops else None,
    )


def around(parts, axis):
    return [
        lax.ppermute(part, axis, [(i, (i + step) & 3) for i in range(4)]) for step, part in enumerate(parts, 1)
    ]


def shards(
    tokens, norm_gain, w_recept, w_key, w_value, w_decay, w_rate, w_gate_rec, w_pool, w_gate_pool,
    decay_base, rate_base, head_gain, pool_mix, pool_scale, w_out_rec, w_out_pool, init_state,
):
    other = lax.ppermute(tokens, "tp", [(0, 1), (1, 0)])
    line = lambda x: x.reshape(1, -1)
    pinned = lambda x: pltpu.with_memory_space_constraint(x, pltpu.HBM)
    weights = [pinned(w) for w in (w_key, w_decay, w_rate, w_value)]
    own_normed, squares, *prepared = call(
        own_kernel,
        "own",
        hbm(6),
        [shape((256, 1024)), shape((256, 128), f32)]
        + [shape((256, 768), f32)] * 2
        + [shape((1024, 768))] * 2,
        [pltpu.VMEM((1024, 768), bf16)] * 2
        + [
            pltpu.SemaphoreType.DMA((8,)), pltpu.VMEM((256, 1024), bf16), pltpu.VMEM((1, D), f32),
            pltpu.SemaphoreType.DMA((2,)),
        ],
        20,
        1_000_000_000,
    )(pinned(tokens.reshape(256, 1024)), pinned(line(norm_gain)), *weights)
    normed, scale, pool, home, m1, m2, m3, right, solved, v, grow, lift = call(
        local_kernel,
        "local",
        vmem(10) + hbm(1),
        [
            shape((256, 1024)), shape((256, 128), f32), shape((256, 256)),
            shape((256, 128)), shape((320, 128)), shape((256, 128)), shape((256, 128)),
            shape((6, 256, 128)), shape((6, 128, 256)), shape((6, 128, 128)),
            shape((6, 128, 128), f32), shape((6, 128), f32),
        ],
        [pltpu.VMEM((6, 128, 128), f32)] * 3
        + [pltpu.VMEM((4, 256, 128), bf16)]
        + [pltpu.VMEM((D, 256), bf16), pltpu.SemaphoreType.DMA((1,))],
        24,
        3_000_000_000,
    )(
        other.reshape(256, 1024), own_normed, line(norm_gain), squares, decay_base, rate_base, *prepared,
        pinned(w_pool),
    )
    r1, r2, r3 = around((m1, m2, m3), "sp_1")
    reads, local, gate, pgate = call(
        side_kernel,
        "side",
        vmem(11),
        [shape((6, 128, 128)), shape((6, 128, 128), f32), shape((256, 384)), shape((256, 256))],
        [],
        16,
        1_000_000_000,
    )(own_normed, normed, scale, right, solved, v, grow, lift, w_recept, w_gate_rec, w_gate_pool)
    prefix, onward, total = call(
        row_kernel,
        "row",
        vmem(4) + [pl.BlockSpec(memory_space=pl.ANY)],
        [shape((3, 2, 128, 128), f32), shape((320, 128)), shape((256, 128))],
        [pltpu.VMEM((4, 256, 128), bf16)],
        8,
        100_000_000,
    )(home, r1, r2, r3, pgate)
    columns = around((onward, total, total), "sp_0")
    s0, s1, s2, s3 = call(
        column_kernel,
        "column",
        vmem(5),
        [shape((2, 64, 128))] * 4,
        [pltpu.VMEM((4, 2, 64, 128), bf16), pltpu.VMEM((4, 256, 128), bf16)],
        8,
        100_000_000,
    )(prefix, *columns, init_state)
    t1, t2, t3 = around((s1, s2, s3), "sp_1")
    pool_part = call(
        pool_kernel, "pool", vmem(7), shape((256, D), f32), [pltpu.VMEM((256, 256), bf16)], 12, 300_000_000
    )(pool, r1, columns[0], pgate, pool_mix, line(pool_scale), w_out_pool)
    send, rec = call(
        final_kernel,
        "final",
        vmem(10),
        [shape((256, 1024)), shape((256, 384))],
        [pltpu.VMEM((4, 2, 64, 128), bf16)],
        20,
        1_000_000_000,
    )(s0, t1, t2, t3, reads, local, gate, head_gain, pool_part, w_out_rec)
    arrived = lax.ppermute(send, "tp", [(0, 1), (1, 0)])
    keep = call(keep_kernel, "keep", vmem(3), shape((256, 1024)), [], 8, 300_000_000)(rec, pool_part, w_out_rec)
    mixed = keep.astype(f32) + arrived.astype(f32)
    return mixed.astype(bf16).reshape(2, 128, 1024)


def solution(mesh):
    split = Mesh(
        mesh.devices.reshape(4, 4, mesh.shape["fs"], mesh.shape["tp"]), ("sp_0", "sp_1", "fs", "tp")
    )
    column = P(None, "tp")
    placed = (
        (P("fs", SP, "tp"), P()) + (column,) * 8 + (P(),) * 5
        + (P("tp", None), P("tp", None), P("fs", "tp", None, None))
    )
    return jax.shard_map(
        shards, mesh=split, in_specs=placed, out_specs=P("fs", SP, "tp"), check_vma=False
    )
```

```python
import functools

import jax
import jax.numpy as jnp
from jax import lax
from jax.experimental import pallas as pl
from jax.experimental.pallas import tpu as pltpu
from jax.sharding import Mesh
from jax.sharding import PartitionSpec as P

D = 2048
HEAD = 64
SPAN = 128
UNITS = 6
SP = ("sp_0", "sp_1")
f32 = jnp.float32
bf16 = jnp.bfloat16
NN = ((1,), (0,))
NT = ((1,), (1,))
TN = ((0,), (0,))
MIB = 2**20


def dot(a, b, dims=NN):
    return lax.dot_general(
        a.astype(bf16), b.astype(bf16), (dims, ((), ())), preferred_element_type=f32
    )


def halves(x):
    high = x.astype(bf16)
    return high, (x - high.astype(f32)).astype(bf16)


def dot_fine_left(a, b, dims=NN):
    high, low = halves(a)
    return dot(high, b, dims) + dot(low, b, dims)


def dot_fine_right(a, b, dims=NN):
    high, low = halves(b)
    return dot(a, high, dims) + dot(a, low, dims)


def iota(rows, cols, dim):
    return lax.broadcasted_iota(jnp.int32, (rows, cols), dim)


def line_of(ref, lanes):
    if len(ref.shape) == 1:
        return ref[lanes].reshape(1, 128)
    return ref[:, lanes]


def head_masks():
    first = (iota(1, 128, 1) < HEAD).astype(f32)
    return first.astype(bf16), (1.0 - first).astype(bf16)


def both(x, masks):
    x = x.astype(bf16)
    return jnp.concatenate([x * masks[0], x * masks[1]], axis=0)


def joined(x):
    return jnp.where(iota(HEAD, 128, 1) < HEAD, x[:HEAD], x[HEAD:])


def compose(earlier, later, masks):
    moved = dot_fine_left(earlier, both(later[:HEAD], masks))
    written = later[HEAD:].astype(f32)
    if earlier.shape[0] == HEAD:
        return moved + written
    return jnp.concatenate([moved[:HEAD], moved[HEAD:] + written], axis=0)


def pick(x, size, odd):
    parts = [x[s : s + size] for s in range(size * odd, SPAN, 2 * size)]
    return parts[0] if len(parts) == 1 else jnp.concatenate(parts, axis=0)


def weave(even, odd, size):
    parts = []
    for s in range(0, SPAN // 2, size):
        parts += [even[s : s + size], odd[s : s + size]]
    return jnp.concatenate(parts, axis=0)


def woven(part, size):
    if size >= 16:
        part = part.astype(bf16)
    return weave(jnp.zeros_like(part), part, size)


def blocks(x):
    x = x.astype(bf16)
    zero = jnp.zeros((SPAN, 128), bf16)
    return jnp.concatenate(
        [jnp.concatenate([x[:, :128], zero], axis=1), jnp.concatenate([zero, x[:, 128:]], axis=1)], axis=0
    )


def inverses(lowers, fill):
    row, col = iota(SPAN, 256, 0), iota(SPAN, 256, 1) & 127
    eye = (row == col).astype(f32)
    near = ((row >> 1) == (col >> 1)).astype(bf16)
    result = [eye - (lower * near).astype(f32) for lower in lowers]
    size, level = 2, 1
    while size < SPAN:
        off = (((row >> (level + 1)) == (col >> (level + 1))) & ((row >> level) != (col >> level))).astype(bf16)
        if size < 8:
            inner = [dot(lower * off, blocks(inv)) for lower, inv in zip(lowers, result)]
            fill(level)
            result = [inv - dot(inv, blocks(part)) for inv, part in zip(result, inner)]
        else:
            if size < 16:
                off = pick(off.astype(f32), size, 1).astype(bf16)
                odd = [pick(lower.astype(f32), size, 1).astype(bf16) for lower in lowers]
            else:
                off = pick(off, size, 1)
                odd = [pick(lower, size, 1) for lower in lowers]
            inner = [dot(lower * off, blocks(inv)) for lower, inv in zip(odd, result)]
            fill(level)
            outer = [
                dot(pick(inv, size, 1), blocks(woven(part, size))) for inv, part in zip(result, inner)
            ]
            result = [
                weave(pick(inv, size, 0), pick(inv, size, 1) - part, size)
                for inv, part in zip(result, outer)
            ]
        size, level = size * 2, level + 1
    return result


def fetch(sources, buf, first_row, sems, base):
    copies, at = [], 0
    for i, src in enumerate(sources):
        width = src.shape[1]
        copies.append(
            pltpu.make_async_copy(
                src.at[pl.ds(pl.multiple_of(first_row, 1024), 1024), :],
                buf.at[:, at : at + width],
                sems.at[base + i],
            )
        )
        at += width
    return copies


def begin(copies):
    for copy in copies:
        copy.start()


def finish(copies):
    for copy in copies:
        copy.wait()


def own_kernel(*refs):
    token_ref, norm_ref = refs[:2]
    sources, normed_ref, squares_ref, partial_ref, rest_ref = refs[2:6], *refs[6:10]
    buf, sems, own_ref, gain_ref, first_sems = refs[10:15]
    tp = lax.axis_index("tp")
    early = [
        pltpu.make_async_copy(norm_ref, gain_ref, first_sems.at[0]),
        pltpu.make_async_copy(token_ref, own_ref, first_sems.at[1]),
    ]
    mine = fetch(sources, buf, tp * 1024, sems, 0)
    others = fetch(sources, rest_ref, (1 - tp) * 1024, sems, 4)
    mine = (mine[:2], mine[2:])
    others = (others[:2], others[2:])
    begin(early)
    begin(mine[0])
    pl.delay(400)
    begin(mine[1])
    pl.delay(400)
    begin(others[0])
    finish(early)
    own = own_ref[...].astype(f32)
    normed = (own * jnp.where(tp == 0, gain_ref[:, :1024], gain_ref[:, 1024:])).astype(bf16)
    normed_ref[...] = normed
    squares_ref[...] = jnp.broadcast_to(jnp.sum(own * own, axis=1, keepdims=True), (256, 128))
    begin(others[1])
    for i in range(2):
        finish(mine[i])
        cols = slice(768 * i, 768 * i + 768)
        partial_ref[:, cols] = dot(normed_ref[...], buf[:, cols])
    finish(others[0])
    finish(others[1])


def local_kernel(*refs):
    other_ref, own_ref, gain_ref, squares_ref, db_ref, rb_ref = refs[:6]
    partial_ref, rest_ref, pool_weight = refs[6:9]
    (
        normed_ref, scale_ref, pool_ref, home_ref, first_ref, second_ref, third_ref,
        right_ref, solved_ref, v_ref, grow_ref, lift_ref,
    ) = refs[9:21]
    k_s, d_s, a_s, maps, pool_buf, sems = refs[21:27]
    tp = lax.axis_index("tp")
    y = lax.axis_index("sp_1")
    pool_buf = pool_weight
    is_first = tp == 0
    other = other_ref[...].astype(f32)
    normed = (other * jnp.where(is_first, gain_ref[:, 1024:], gain_ref[:, :1024])).astype(bf16)
    normed_ref[...] = normed
    squares = squares_ref[:, :1] + jnp.sum(other * other, axis=1, keepdims=True)
    scale = lax.rsqrt(squares * (1.0 / D) + 0.25)
    scale_ref[...] = jnp.broadcast_to(scale, (256, 128))

    def project(rows, cols):
        total = partial_ref[rows, cols] + dot(normed_ref[rows], rest_ref[:, cols])
        return (total * scale_ref[rows, :1]).astype(bf16)

    rounded = project(slice(0, 256), slice(0, 1152))
    for u in range(UNITS):
        s, h = u // 3, u % 3
        for i, dest in enumerate((k_s, d_s, a_s)):
            at = 384 * i + h * 128
            dest[u] = rounded[s * 128 : s * 128 + 128, at : at + 128].astype(f32)

    def fill(level):
        if level > 4:
            return
        s = (level - 1) & 1
        rows = slice(s * 128, s * 128 + 128)
        if level <= 2:
            value = project(rows, slice(1152, 1536))
            for h in range(3):
                v_ref[3 * s + h] = value[:, h * 128 : h * 128 + 128]
            return
        total = dot(own_ref[rows], pool_buf[pl.ds(pl.multiple_of(tp * 1024, 1024), 1024), :])
        total = total + dot(normed_ref[rows], pool_buf[pl.ds(pl.multiple_of((1 - tp) * 1024, 1024), 1024), :])
        pool = (total * scale_ref[rows, :1]).astype(bf16)
        pool_ref[rows] = pool
        for half in (0, 1):
            at = 256 + (2 * s + half) * 16
            first_ref[at : at + 16] = pool[112:128, half * 128 : half * 128 + 128]

    masks = head_masks()
    n = SPAN
    row, col = iota(n, n, 0), iota(n, n, 1)
    strict, inclusive = row > col, row >= col
    triangle = inclusive.astype(f32)
    ones = ((row >> 6) == (col >> 6)).astype(f32)
    wide = (
        jnp.concatenate([masks[0], masks[0]], axis=1),
        jnp.concatenate([masks[1], masks[1]], axis=1),
    )
    slab = iota(HEAD, 128, 0)
    eye = (slab == (iota(HEAD, 128, 1) & 63)).astype(f32)
    units = range(UNITS)
    first_stage = []
    for u in units:
        h = u % 3
        lanes = slice(h * 128, h * 128 + 128)
        shifted = slice(384 + h * 128, 384 + h * 128 + 128)
        db = jnp.where(is_first, line_of(db_ref, lanes), line_of(db_ref, shifted))
        k = k_s[u]
        log_decay = -0.6065306597126334 * jax.nn.sigmoid(db + d_s[u])
        first_stage.append((log_decay, dot(k * k, ones), dot_fine_right(triangle, log_decay)))
    second_stage = []
    for u in units:
        h = u % 3
        lanes = slice(h * 128, h * 128 + 128)
        shifted = slice(384 + h * 128, 384 + h * 128 + 128)
        rb = jnp.where(is_first, line_of(rb_ref, lanes), line_of(rb_ref, shifted))
        rate = jax.nn.sigmoid(rb + a_s[u])
        log_decay, squared, total = first_stage[u]
        k = k_s[u]
        middle = total[63:64]
        unit_key = k * lax.rsqrt(squared + 1.0)
        centred = total - middle
        alpha = jnp.exp(centred - log_decay) * unit_key
        fading = jnp.exp(-centred)
        grow_ref[u] = jnp.exp(centred)
        lift = jnp.exp(middle)
        lift_ref[u : u + 1] = lift
        right = jnp.concatenate(
            [(unit_key * rate * fading).astype(bf16), (k * fading).astype(bf16)], axis=0
        )
        right_ref[u] = right
        ends = (jnp.exp(total[127:128]), jnp.exp(centred[127:128]))
        second_stage.append((right, alpha * lift, ends, dot(both(alpha, masks), right, NT)))
    lowers, carries = [], []
    for u in units:
        pairs = second_stage[u][3]
        block = lambda j, c: jnp.where(
            strict, pairs[j * n : j * n + n, c * n : c * n + n], 0.0
        ).astype(bf16)
        lowers.append(jnp.concatenate([block(0, 0), block(1, 0)], axis=1))
        carries.append(jnp.concatenate([block(0, 1), block(1, 1)], axis=1))
    inverse = inverses(lowers, fill)
    carries = [dot(carries[u], both(v_ref[u], masks)) for u in units]
    solutions = []
    for u in units:
        wanted = jnp.concatenate([second_stage[u][1].astype(bf16), carries[u].astype(bf16)], axis=1)
        solved = dot(inverse[u], both(wanted, wide)).astype(bf16)
        solved_ref[u] = solved
        solutions.append(solved)
    for u in units:
        right, _, ends, _ = second_stage[u]
        solved = solutions[u]
        transit = eye * ends[0] - joined(dot(solved[:, :n], right[:n], TN)) * ends[1]
        written = joined(
            dot(
                jnp.concatenate([-solved[:, n:], v_ref[u]], axis=0),
                right,
                TN,
            )
        ) * ends[1]
        at = (u // 3) * 128
        maps[u % 3, at : at + HEAD] = transit.astype(bf16)
        maps[u % 3, at + HEAD : at + 128] = written.astype(bf16)
    maps[3] = jnp.zeros((256, 128), bf16)
    for step, dest in enumerate((home_ref, first_ref, second_ref, third_ref)):
        dest[:256] = maps[(y + step) & 3]


def side_kernel(
    own_ref, other_ref, scale_ref, right_ref, solved_ref, v_ref, grow_ref, lift_ref, wr_ref, wg_ref, wq_ref,
    reads_ref, local_ref, gate_ref, pgate_ref,
):
    tp = lax.axis_index("tp")
    scale = scale_ref[:, :1]
    mine, theirs = pl.multiple_of(tp * 1024, 1024), pl.multiple_of((1 - tp) * 1024, 1024)

    def project(weight):
        total = dot(own_ref[...], weight[pl.ds(mine, 1024), :])
        total = total + dot(other_ref[...], weight[pl.ds(theirs, 1024), :])
        return (total * scale).astype(bf16)

    receptance = project(wr_ref)
    masks = head_masks()
    wide = (
        jnp.concatenate([masks[0], masks[0]], axis=1),
        jnp.concatenate([masks[1], masks[1]], axis=1),
    )
    inclusive = iota(128, 128, 0) >= iota(128, 128, 1)
    inside, rhos = [], []
    for u in range(UNITS):
        s, h = u // 3, u % 3
        rho = receptance[s * 128 : s * 128 + 128, h * 128 : h * 128 + 128].astype(f32) * grow_ref[u]
        rhos.append(rho * lift_ref[u : u + 1])
        pairs = dot(both(rho, masks), right_ref[u], NT)
        block = lambda j, c: jnp.where(
            inclusive, pairs[j * 128 : j * 128 + 128, c * 128 : c * 128 + 128], 0.0
        ).astype(bf16)
        inside.append([jnp.concatenate([block(0, c), block(1, c)], axis=1) for c in (0, 1)])
    for u in range(UNITS):
        removed = dot(inside[u][0], both(solved_ref[u], wide))
        reads_ref[u] = (rhos[u] - removed[:, :128]).astype(bf16)
        local_ref[u] = dot(inside[u][1], both(v_ref[u], masks)) - removed[:, 128:]
    gate_ref[...] = project(wg_ref)
    pgate_ref[...] = project(wq_ref)


def row_kernel(home_ref, first_ref, second_ref, third_ref, after_ref, prefix_ref, next_ref, total_ref, maps):
    y = lax.axis_index("sp_1")
    for step, src in enumerate((home_ref, first_ref, second_ref, third_ref)):
        maps[(y + 4 - step) & 3] = src[:256]
    next_ref[256:] = first_ref[256:]
    masks = head_masks()
    for s in (0, 1):
        rows = slice(s * 128, s * 128 + 128)
        so_far = maps[0, rows].astype(f32)
        prefix_ref[0, s] = so_far
        for j in (1, 2, 3):
            so_far = compose(so_far, maps[j, rows], masks)
            if j < 3:
                prefix_ref[j, s] = so_far
            else:
                next_ref[rows] = so_far.astype(bf16)
                total_ref[rows] = so_far.astype(bf16)


def column_kernel(
    prefix_ref, first_ref, second_ref, third_ref, init_ref,
    home_ref, one_ref, two_ref, three_ref,
    starts, rows,
):
    y = lax.axis_index("sp_1")
    z = lax.axis_index("sp_0")
    for step, src in enumerate((first_ref, second_ref, third_ref)):
        rows[(z + 3 - step) & 3] = src[:256]
    masks = head_masks()
    pair = jnp.minimum(y, 2) * 2
    for s in (0, 1):
        state = jnp.concatenate([init_ref[s, pair], init_ref[s, pair + 1]], axis=1)
        for j in range(3):
            state = jnp.where(j < z, compose(state, rows[j, s * 128 : s * 128 + 128], masks), state)
        starts[0, s] = state.astype(bf16)
        for j in range(3):
            starts[j + 1, s] = compose(state, prefix_ref[j, s], masks).astype(bf16)
    for step, dest in enumerate((home_ref, one_ref, two_ref, three_ref)):
        dest[...] = starts[(y + step) & 3]


def pool_kernel(pool_ref, beside_ref, above_ref, pgate_ref, mix_ref, pscale_ref, wp_ref, part_ref, out_ref):
    tp = lax.axis_index("tp")
    y = lax.axis_index("sp_1")
    place = lax.axis_index("sp_0") * 4 + y
    is_first = tp == 0
    factor = jnp.where(is_first, pscale_ref[:, :256], pscale_ref[:, 256:])
    for s in (0, 1):
        current = pool_ref[s * 128 : s * 128 + 128].astype(f32)
        tails = []
        for half in (0, 1):
            rows = slice(256 + (2 * s + half) * 16, 272 + (2 * s + half) * 16)
            tails.append(
                jnp.where(
                    place == 0,
                    0.0,
                    jnp.where(y > 0, beside_ref[rows].astype(f32), above_ref[rows].astype(f32)),
                )
            )
        padded = jnp.concatenate([jnp.concatenate(tails, axis=1), current], axis=0)
        sums = {1: padded}
        for by in (1, 2, 4, 8):
            before = sums[by]
            moved = jnp.concatenate([jnp.zeros((by, 256), f32), before[: 144 - by]], axis=0)
            sums[2 * by] = before + moved
        position = (place * 128 + iota(128, 128, 0) + 1).astype(f32)
        for g in (0, 1):
            lanes = slice(g * 128, g * 128 + 128)
            small, large = 2 << g, 8 << g
            trailing = jnp.where(is_first, sums[small][16:, lanes], sums[large][16:, lanes])
            window = jnp.where(is_first, float(small), float(large))
            diffs = trailing / jnp.minimum(position, window) - current[:, lanes]
            mixed = dot(diffs.astype(bf16), mix_ref[tp * 2 + g])
            gate = pgate_ref[s * 128 : s * 128 + 128, lanes].astype(f32)
            out_ref[s * 128 : s * 128 + 128, lanes] = (
                mixed * factor[:, lanes] * (gate * jax.nn.sigmoid(gate))
            ).astype(bf16)
    part_ref[...] = dot(out_ref[...], wp_ref[...])


def final_kernel(
    home_ref, one_ref, two_ref, three_ref, reads_ref, local_ref, gate_ref, hgain_ref, part_ref,
    wr_ref,
    send_ref, rec,
    starts,
):
    tp = lax.axis_index("tp")
    y = lax.axis_index("sp_1")
    for step, src in enumerate((home_ref, one_ref, two_ref, three_ref)):
        starts[(y + 4 - step) & 3] = src[...]
    masks = head_masks()
    row, col = iota(128, 128, 0), iota(128, 128, 1)
    mean_of = jnp.where((row >> 6) == (col >> 6), 1.0 / HEAD, 0.0).astype(bf16)
    is_first = tp == 0
    for u in range(UNITS):
        s, h = u // 3, u % 3
        lanes = slice(h * 128, h * 128 + 128)
        shifted = slice(384 + h * 128, 384 + h * 128 + 128)
        rows = slice(s * 128, s * 128 + 128)
        out = dot(reads_ref[u], both(starts[h, s], masks), NT) + local_ref[u]
        out = out - dot_fine_left(out, mean_of)
        spread = dot_fine_left(out * out, mean_of)
        gain = jnp.where(is_first, line_of(hgain_ref, lanes), line_of(hgain_ref, shifted))
        gate = gate_ref[rows, lanes].astype(f32)
        rec[rows, lanes] = (
            out * lax.rsqrt(spread + 1.0) * gain * (gate * jax.nn.sigmoid(gate))
        ).astype(bf16)
    cols = pl.ds(pl.multiple_of((1 - tp) * 1024, 1024), 1024)
    send_ref[...] = (dot(rec[...], wr_ref[:, cols]) + part_ref[:, cols]).astype(bf16)


def keep_kernel(rec_ref, part_ref, wr_ref, keep_ref):
    cols = pl.ds(pl.multiple_of(lax.axis_index("tp") * 1024, 1024), 1024)
    keep_ref[...] = (dot(rec_ref[...], wr_ref[:, cols]) + part_ref[:, cols]).astype(bf16)


def vmem(count):
    return [pl.BlockSpec(memory_space=pltpu.VMEM)] * count


def hbm(count):
    return [pl.BlockSpec(memory_space=pltpu.HBM)] * count


def shape(dims, kind=bf16):
    return jax.ShapeDtypeStruct(dims, kind)


def call(body, name, ins, outs, scratch, limit, flops=0):
    return pl.pallas_call(
        body,
        name=name,
        out_shape=outs,
        in_specs=ins,
        out_specs=vmem(len(outs)) if isinstance(outs, (list, tuple)) else vmem(1)[0],
        scratch_shapes=scratch,
        compiler_params=pltpu.CompilerParams(vmem_limit_bytes=limit * MIB),
        cost_estimate=pl.CostEstimate(flops=flops, transcendentals=0, bytes_accessed=0) if flops else None,
    )


def around(parts, axis):
    return [
        lax.ppermute(part, axis, [(i, (i + step) & 3) for i in range(4)]) for step, part in enumerate(parts, 1)
    ]


def shards(
    tokens, norm_gain, w_recept, w_key, w_value, w_decay, w_rate, w_gate_rec, w_pool, w_gate_pool,
    decay_base, rate_base, head_gain, pool_mix, pool_scale, w_out_rec, w_out_pool, init_state,
):
    other = lax.ppermute(tokens, "tp", [(0, 1), (1, 0)])
    line = lambda x: x.reshape(1, -1)
    pinned = lambda x: pltpu.with_memory_space_constraint(x, pltpu.HBM)
    weights = [pinned(w) for w in (w_key, w_decay, w_rate, w_value)]
    own_normed, squares, *prepared = call(
        own_kernel,
        "own",
        hbm(6),
        [shape((256, 1024)), shape((256, 128), f32)]
        + [shape((256, 1536), f32), shape((1024, 1536))],
        [pltpu.VMEM((1024, 1536), bf16)]
        + [
            pltpu.SemaphoreType.DMA((8,)), pltpu.VMEM((256, 1024), bf16), pltpu.VMEM((1, D), f32),
            pltpu.SemaphoreType.DMA((2,)),
        ],
        20,
        1_000_000_000,
    )(pinned(tokens.reshape(256, 1024)), pinned(line(norm_gain)), *weights)
    normed, scale, pool, home, m1, m2, m3, right, solved, v, grow, lift = call(
        local_kernel,
        "local",
        vmem(9),
        [
            shape((256, 1024)), shape((256, 128), f32), shape((256, 256)),
            shape((256, 128)), shape((320, 128)), shape((256, 128)), shape((256, 128)),
            shape((6, 256, 128)), shape((6, 128, 256)), shape((6, 128, 128)),
            shape((6, 128, 128), f32), shape((6, 128), f32),
        ],
        [pltpu.VMEM((6, 128, 128), f32)] * 3
        + [pltpu.VMEM((4, 256, 128), bf16)]
        + [pltpu.VMEM((D, 256), bf16), pltpu.SemaphoreType.DMA((1,))],
        24,
        3_000_000_000,
    )(
        other.reshape(256, 1024), own_normed, line(norm_gain), squares, decay_base, rate_base, *prepared,
        w_pool,
    )
    r1, r2, r3 = around((m1, m2, m3), "sp_1")
    reads, local, gate, pgate = call(
        side_kernel,
        "side",
        vmem(11),
        [shape((6, 128, 128)), shape((6, 128, 128), f32), shape((256, 384)), shape((256, 256))],
        [],
        16,
        1_000_000_000,
    )(own_normed, normed, scale, right, solved, v, grow, lift, w_recept, w_gate_rec, w_gate_pool)
    prefix, onward, total = call(
        row_kernel,
        "row",
        vmem(4) + [pl.BlockSpec(memory_space=pl.ANY)],
        [shape((3, 2, 128, 128), f32), shape((320, 128)), shape((256, 128))],
        [pltpu.VMEM((4, 256, 128), bf16)],
        8,
        100_000_000,
    )(home, r1, r2, r3, pgate)
    columns = around((onward, total, total), "sp_0")
    s0, s1, s2, s3 = call(
        column_kernel,
        "column",
        vmem(5),
        [shape((2, 64, 128))] * 4,
        [pltpu.VMEM((4, 2, 64, 128), bf16), pltpu.VMEM((4, 256, 128), bf16)],
        8,
        100_000_000,
    )(prefix, *columns, init_state)
    t1, t2, t3 = around((s1, s2, s3), "sp_1")
    pool_part = call(
        pool_kernel, "pool", vmem(7), shape((256, D), f32), [pltpu.VMEM((256, 256), bf16)], 12, 300_000_000
    )(pool, r1, columns[0], pgate, pool_mix, line(pool_scale), w_out_pool)
    send, rec = call(
        final_kernel,
        "final",
        vmem(10),
        [shape((256, 1024)), shape((256, 384))],
        [pltpu.VMEM((4, 2, 64, 128), bf16)],
        20,
        1_000_000_000,
    )(s0, t1, t2, t3, reads, local, gate, head_gain, pool_part, w_out_rec)
    arrived = lax.ppermute(send, "tp", [(0, 1), (1, 0)])
    keep = call(keep_kernel, "keep", vmem(3), shape((256, 1024)), [], 8, 300_000_000)(rec, pool_part, w_out_rec)
    mixed = keep.astype(f32) + arrived.astype(f32)
    return mixed.astype(bf16).reshape(2, 128, 1024)


def solution(mesh):
    split = Mesh(
        mesh.devices.reshape(4, 4, mesh.shape["fs"], mesh.shape["tp"]), ("sp_0", "sp_1", "fs", "tp")
    )
    column = P(None, "tp")
    placed = (
        (P("fs", SP, "tp"), P()) + (column,) * 8 + (P(),) * 5
        + (P("tp", None), P("tp", None), P("fs", "tp", None, None))
    )
    return jax.shard_map(
        shards, mesh=split, in_specs=placed, out_specs=P("fs", SP, "tp"), check_vma=False
    )
```

```python
import functools

import jax
import jax.numpy as jnp
from jax import lax
from jax.experimental import pallas as pl
from jax.experimental.pallas import tpu as pltpu
from jax.sharding import Mesh
from jax.sharding import PartitionSpec as P

D = 2048
HEAD = 64
SPAN = 128
UNITS = 6
SP = ("sp_0", "sp_1")
f32 = jnp.float32
bf16 = jnp.bfloat16
NN = ((1,), (0,))
NT = ((1,), (1,))
TN = ((0,), (0,))
MIB = 2**20


def dot(a, b, dims=NN):
    return lax.dot_general(
        a.astype(bf16), b.astype(bf16), (dims, ((), ())), preferred_element_type=f32
    )


def halves(x):
    high = x.astype(bf16)
    return high, (x - high.astype(f32)).astype(bf16)


def dot_fine_left(a, b, dims=NN):
    high, low = halves(a)
    return dot(high, b, dims) + dot(low, b, dims)


def dot_fine_right(a, b, dims=NN):
    high, low = halves(b)
    return dot(a, high, dims) + dot(a, low, dims)


def iota(rows, cols, dim):
    return lax.broadcasted_iota(jnp.int32, (rows, cols), dim)


def line_of(ref, lanes):
    if len(ref.shape) == 1:
        return ref[lanes].reshape(1, 128)
    return ref[:, lanes]


def head_masks():
    first = (iota(1, 128, 1) < HEAD).astype(f32)
    return first.astype(bf16), (1.0 - first).astype(bf16)


def both(x, masks):
    x = x.astype(bf16)
    return jnp.concatenate([x * masks[0], x * masks[1]], axis=0)


def joined(x):
    return jnp.where(iota(HEAD, 128, 1) < HEAD, x[:HEAD], x[HEAD:])


def compose(earlier, later, masks):
    high, low = halves(earlier) if earlier.dtype == f32 else (earlier, None)
    upper, lower = halves(later[:HEAD]) if later.dtype == f32 else (later[:HEAD], None)
    left, right = [high], [both(upper, masks)]
    if low is not None:
        left.append(low)
        right.append(right[0])
    if lower is not None:
        left.append(high)
        right.append(both(lower, masks))
    moved = dot(jnp.concatenate(left, axis=1), jnp.concatenate(right, axis=0))
    written = later[HEAD:].astype(f32)
    if earlier.shape[0] == HEAD:
        return moved + written
    return jnp.concatenate([moved[:HEAD], moved[HEAD:] + written], axis=0)


def pick(x, size, odd):
    parts = [x[s : s + size] for s in range(size * odd, SPAN, 2 * size)]
    return parts[0] if len(parts) == 1 else jnp.concatenate(parts, axis=0)


def weave(even, odd, size):
    parts = []
    for s in range(0, SPAN // 2, size):
        parts += [even[s : s + size], odd[s : s + size]]
    return jnp.concatenate(parts, axis=0)


def woven(part, size):
    if size >= 16:
        part = part.astype(bf16)
    return weave(jnp.zeros_like(part), part, size)


def blocks(x):
    x = x.astype(bf16)
    zero = jnp.zeros((SPAN, 128), bf16)
    return jnp.concatenate(
        [jnp.concatenate([x[:, :128], zero], axis=1), jnp.concatenate([zero, x[:, 128:]], axis=1)], axis=0
    )


def inverses(lowers, fill):
    row, col = iota(SPAN, 256, 0), iota(SPAN, 256, 1) & 127
    eye = (row == col).astype(f32)
    near = ((row >> 1) == (col >> 1)).astype(bf16)
    result = [eye - (lower * near).astype(f32) for lower in lowers]
    size, level = 2, 1
    while size < SPAN:
        off = (((row >> (level + 1)) == (col >> (level + 1))) & ((row >> level) != (col >> level))).astype(bf16)
        if size < 8:
            inner = [dot(lower * off, blocks(inv)) for lower, inv in zip(lowers, result)]
            fill(level)
            result = [inv - dot(inv, blocks(part)) for inv, part in zip(result, inner)]
        else:
            if size < 16:
                off = pick(off.astype(f32), size, 1).astype(bf16)
                odd = [pick(lower.astype(f32), size, 1).astype(bf16) for lower in lowers]
            else:
                off = pick(off, size, 1)
                odd = [pick(lower, size, 1) for lower in lowers]
            inner = [dot(lower * off, blocks(inv)) for lower, inv in zip(odd, result)]
            fill(level)
            outer = [
                dot(pick(inv, size, 1), blocks(woven(part, size))) for inv, part in zip(result, inner)
            ]
            result = [
                weave(pick(inv, size, 0), pick(inv, size, 1) - part, size)
                for inv, part in zip(result, outer)
            ]
        size, level = size * 2, level + 1
    return result


def fetch(sources, buf, first_row, sems, base):
    copies, at = [], 0
    for i, src in enumerate(sources):
        width = src.shape[1]
        copies.append(
            pltpu.make_async_copy(
                src.at[pl.ds(pl.multiple_of(first_row, 1024), 1024), :],
                buf.at[:, at : at + width],
                sems.at[base + i],
            )
        )
        at += width
    return copies


def begin(copies):
    for copy in copies:
        copy.start()


def finish(copies):
    for copy in copies:
        copy.wait()


def own_kernel(*refs):
    token_ref, norm_ref = refs[:2]
    sources, normed_ref, squares_ref, partial_ref, rest_ref = refs[2:6], *refs[6:10]
    buf, sems, own_ref, gain_ref, first_sems = refs[10:15]
    tp = lax.axis_index("tp")
    early = [
        pltpu.make_async_copy(norm_ref, gain_ref, first_sems.at[0]),
        pltpu.make_async_copy(token_ref, own_ref, first_sems.at[1]),
    ]
    mine = fetch(sources, buf, tp * 1024, sems, 0)
    others = fetch(sources, rest_ref, (1 - tp) * 1024, sems, 4)
    mine = (mine[:2], mine[2:])
    others = (others[:2], others[2:])
    begin(early)
    begin(mine[0])
    pl.delay(400)
    begin(mine[1])
    pl.delay(400)
    begin(others[0])
    finish(early)
    own = own_ref[...].astype(f32)
    normed = (own * jnp.where(tp == 0, gain_ref[:, :1024], gain_ref[:, 1024:])).astype(bf16)
    normed_ref[...] = normed
    squares_ref[...] = jnp.broadcast_to(jnp.sum(own * own, axis=1, keepdims=True), (256, 128))
    begin(others[1])
    for i in range(2):
        finish(mine[i])
        cols = slice(768 * i, 768 * i + 768)
        partial_ref[:, cols] = dot(normed_ref[...], buf[:, cols])
    finish(others[0])
    finish(others[1])


def local_kernel(*refs):
    other_ref, own_ref, gain_ref, squares_ref, db_ref, rb_ref = refs[:6]
    partial_ref, rest_ref, pool_weight = refs[6:9]
    (
        normed_ref, scale_ref, pool_ref, home_ref, first_ref, second_ref, third_ref,
        right_ref, solved_ref, v_ref, grow_ref, lift_ref,
    ) = refs[9:21]
    k_s, d_s, a_s, maps, pool_buf, sems = refs[21:27]
    tp = lax.axis_index("tp")
    y = lax.axis_index("sp_1")
    pool_buf = pool_weight
    is_first = tp == 0
    other = other_ref[...].astype(f32)
    normed = (other * jnp.where(is_first, gain_ref[:, 1024:], gain_ref[:, :1024])).astype(bf16)
    normed_ref[...] = normed
    squares = squares_ref[:, :1] + jnp.sum(other * other, axis=1, keepdims=True)
    scale = lax.rsqrt(squares * (1.0 / D) + 0.25)
    scale_ref[...] = jnp.broadcast_to(scale, (256, 128))

    def project(rows, cols):
        total = partial_ref[rows, cols] + dot(normed_ref[rows], rest_ref[:, cols])
        return (total * scale_ref[rows, :1]).astype(bf16)

    rounded = project(slice(0, 256), slice(0, 1152))
    for u in range(UNITS):
        s, h = u // 3, u % 3
        for i, dest in enumerate((k_s, d_s, a_s)):
            at = 384 * i + h * 128
            dest[u] = rounded[s * 128 : s * 128 + 128, at : at + 128].astype(f32)

    def fill(level):
        if level > 4:
            return
        s = (level - 1) & 1
        rows = slice(s * 128, s * 128 + 128)
        if level <= 2:
            value = project(rows, slice(1152, 1536))
            for h in range(3):
                v_ref[3 * s + h] = value[:, h * 128 : h * 128 + 128]
            return
        total = dot(own_ref[rows], pool_buf[pl.ds(pl.multiple_of(tp * 1024, 1024), 1024), :])
        total = total + dot(normed_ref[rows], pool_buf[pl.ds(pl.multiple_of((1 - tp) * 1024, 1024), 1024), :])
        pool = (total * scale_ref[rows, :1]).astype(bf16)
        pool_ref[rows] = pool
        for half in (0, 1):
            at = 256 + (2 * s + half) * 16
            first_ref[at : at + 16] = pool[112:128, half * 128 : half * 128 + 128]

    masks = head_masks()
    n = SPAN
    row, col = iota(n, n, 0), iota(n, n, 1)
    strict, inclusive = row > col, row >= col
    triangle = inclusive.astype(f32)
    ones = ((row >> 6) == (col >> 6)).astype(f32)
    wide = (
        jnp.concatenate([masks[0], masks[0]], axis=1),
        jnp.concatenate([masks[1], masks[1]], axis=1),
    )
    slab = iota(HEAD, 128, 0)
    eye = (slab == (iota(HEAD, 128, 1) & 63)).astype(f32)
    units = range(UNITS)
    first_stage = []
    for u in units:
        h = u % 3
        lanes = slice(h * 128, h * 128 + 128)
        shifted = slice(384 + h * 128, 384 + h * 128 + 128)
        db = jnp.where(is_first, line_of(db_ref, lanes), line_of(db_ref, shifted))
        k = k_s[u]
        log_decay = -0.6065306597126334 * jax.nn.sigmoid(db + d_s[u])
        first_stage.append((log_decay, dot(k * k, ones), dot_fine_right(triangle, log_decay)))
    second_stage = []
    for u in units:
        h = u % 3
        lanes = slice(h * 128, h * 128 + 128)
        shifted = slice(384 + h * 128, 384 + h * 128 + 128)
        rb = jnp.where(is_first, line_of(rb_ref, lanes), line_of(rb_ref, shifted))
        rate = jax.nn.sigmoid(rb + a_s[u])
        log_decay, squared, total = first_stage[u]
        k = k_s[u]
        middle = total[63:64]
        unit_key = k * lax.rsqrt(squared + 1.0)
        centred = total - middle
        alpha = jnp.exp(centred - log_decay) * unit_key
        fading = jnp.exp(-centred)
        grow_ref[u] = jnp.exp(centred)
        lift = jnp.exp(middle)
        lift_ref[u : u + 1] = lift
        right = jnp.concatenate(
            [(unit_key * rate * fading).astype(bf16), (k * fading).astype(bf16)], axis=0
        )
        right_ref[u] = right
        ends = (jnp.exp(total[127:128]), jnp.exp(centred[127:128]))
        second_stage.append((right, alpha * lift, ends, dot(both(alpha, masks), right, NT)))
    lowers, carries = [], []
    for u in units:
        pairs = second_stage[u][3]
        block = lambda j, c: jnp.where(
            strict, pairs[j * n : j * n + n, c * n : c * n + n], 0.0
        ).astype(bf16)
        lowers.append(jnp.concatenate([block(0, 0), block(1, 0)], axis=1))
        carries.append(jnp.concatenate([block(0, 1), block(1, 1)], axis=1))
    inverse = inverses(lowers, fill)
    carries = [dot(carries[u], both(v_ref[u], masks)) for u in units]
    solutions = []
    for u in units:
        wanted = jnp.concatenate([second_stage[u][1].astype(bf16), carries[u].astype(bf16)], axis=1)
        solved = dot(inverse[u], both(wanted, wide)).astype(bf16)
        solved_ref[u] = solved
        solutions.append(solved)
    for u in units:
        right, _, ends, _ = second_stage[u]
        solved = solutions[u]
        transit = eye * ends[0] - joined(dot(solved[:, :n], right[:n], TN)) * ends[1]
        written = joined(
            dot(
                jnp.concatenate([-solved[:, n:], v_ref[u]], axis=0),
                right,
                TN,
            )
        ) * ends[1]
        at = (u // 3) * 128
        maps[u % 3, at : at + HEAD] = transit.astype(bf16)
        maps[u % 3, at + HEAD : at + 128] = written.astype(bf16)
    maps[3] = jnp.zeros((256, 128), bf16)
    for step, dest in enumerate((home_ref, first_ref, second_ref, third_ref)):
        dest[:256] = maps[(y + step) & 3]


def side_kernel(
    own_ref, other_ref, scale_ref, right_ref, solved_ref, v_ref, grow_ref, lift_ref, wr_ref, wg_ref, wq_ref,
    reads_ref, local_ref, gate_ref, pgate_ref,
):
    tp = lax.axis_index("tp")
    scale = scale_ref[:, :1]
    mine, theirs = pl.multiple_of(tp * 1024, 1024), pl.multiple_of((1 - tp) * 1024, 1024)

    def project(weight):
        total = dot(own_ref[...], weight[pl.ds(mine, 1024), :])
        total = total + dot(other_ref[...], weight[pl.ds(theirs, 1024), :])
        return (total * scale).astype(bf16)

    receptance = project(wr_ref)
    masks = head_masks()
    wide = (
        jnp.concatenate([masks[0], masks[0]], axis=1),
        jnp.concatenate([masks[1], masks[1]], axis=1),
    )
    inclusive = iota(128, 128, 0) >= iota(128, 128, 1)
    inside, rhos = [], []
    for u in range(UNITS):
        s, h = u // 3, u % 3
        rho = receptance[s * 128 : s * 128 + 128, h * 128 : h * 128 + 128].astype(f32) * grow_ref[u]
        rhos.append(rho * lift_ref[u : u + 1])
        pairs = dot(both(rho, masks), right_ref[u], NT)
        block = lambda j, c: jnp.where(
            inclusive, pairs[j * 128 : j * 128 + 128, c * 128 : c * 128 + 128], 0.0
        ).astype(bf16)
        inside.append([jnp.concatenate([block(0, c), block(1, c)], axis=1) for c in (0, 1)])
    for u in range(UNITS):
        removed = dot(inside[u][0], both(solved_ref[u], wide))
        reads_ref[u] = (rhos[u] - removed[:, :128]).astype(bf16)
        local_ref[u] = dot(inside[u][1], both(v_ref[u], masks)) - removed[:, 128:]
    gate_ref[...] = project(wg_ref)
    pgate_ref[...] = project(wq_ref)


def row_kernel(home_ref, first_ref, second_ref, third_ref, after_ref, prefix_ref, next_ref, total_ref, maps):
    y = lax.axis_index("sp_1")
    for step, src in enumerate((home_ref, first_ref, second_ref, third_ref)):
        maps[(y + 4 - step) & 3] = src[:256]
    next_ref[256:] = first_ref[256:]
    masks = head_masks()
    for s in (0, 1):
        rows = slice(s * 128, s * 128 + 128)
        own = [maps[j, rows] for j in range(4)]
        front = compose(own[0], own[1], masks)
        back = compose(own[2], own[3], masks)
        whole = compose(front, back, masks).astype(bf16)
        next_ref[rows] = whole
        total_ref[rows] = whole
        prefix_ref[0, s] = own[0].astype(f32)
        prefix_ref[1, s] = front
        prefix_ref[2, s] = compose(front, own[2], masks)


def column_kernel(
    prefix_ref, first_ref, second_ref, third_ref, init_ref,
    home_ref, one_ref, two_ref, three_ref,
    starts, rows,
):
    y = lax.axis_index("sp_1")
    z = lax.axis_index("sp_0")
    for step, src in enumerate((first_ref, second_ref, third_ref)):
        rows[(z + 3 - step) & 3] = src[:256]
    masks = head_masks()
    pair = jnp.minimum(y, 2) * 2
    for s in (0, 1):
        state = jnp.concatenate([init_ref[s, pair], init_ref[s, pair + 1]], axis=1)
        later = [rows[j, s * 128 : s * 128 + 128] for j in range(3)]
        first = compose(state, later[0], masks)
        second = compose(first, later[1], masks)
        third = compose(first, compose(later[1], later[2], masks), masks)
        state = jnp.where(z == 0, state, jnp.where(z == 1, first, jnp.where(z == 2, second, third)))
        starts[0, s] = state.astype(bf16)
        for j in range(3):
            starts[j + 1, s] = compose(state, prefix_ref[j, s], masks).astype(bf16)
    for step, dest in enumerate((home_ref, one_ref, two_ref, three_ref)):
        dest[...] = starts[(y + step) & 3]


def pool_kernel(pool_ref, beside_ref, above_ref, pgate_ref, mix_ref, pscale_ref, wp_ref, part_ref, out_ref):
    tp = lax.axis_index("tp")
    y = lax.axis_index("sp_1")
    place = lax.axis_index("sp_0") * 4 + y
    is_first = tp == 0
    factor = jnp.where(is_first, pscale_ref[:, :256], pscale_ref[:, 256:])
    for s in (0, 1):
        current = pool_ref[s * 128 : s * 128 + 128].astype(f32)
        tails = []
        for half in (0, 1):
            rows = slice(256 + (2 * s + half) * 16, 272 + (2 * s + half) * 16)
            tails.append(
                jnp.where(
                    place == 0,
                    0.0,
                    jnp.where(y > 0, beside_ref[rows].astype(f32), above_ref[rows].astype(f32)),
                )
            )
        padded = jnp.concatenate([jnp.concatenate(tails, axis=1), current], axis=0)
        sums = {1: padded}
        for by in (1, 2, 4, 8):
            before = sums[by]
            moved = jnp.concatenate([jnp.zeros((by, 256), f32), before[: 144 - by]], axis=0)
            sums[2 * by] = before + moved
        position = (place * 128 + iota(128, 128, 0) + 1).astype(f32)
        for g in (0, 1):
            lanes = slice(g * 128, g * 128 + 128)
            small, large = 2 << g, 8 << g
            trailing = jnp.where(is_first, sums[small][16:, lanes], sums[large][16:, lanes])
            window = jnp.where(is_first, float(small), float(large))
            diffs = trailing / jnp.minimum(position, window) - current[:, lanes]
            mixed = dot(diffs.astype(bf16), mix_ref[tp * 2 + g])
            gate = pgate_ref[s * 128 : s * 128 + 128, lanes].astype(f32)
            out_ref[s * 128 : s * 128 + 128, lanes] = (
                mixed * factor[:, lanes] * (gate * jax.nn.sigmoid(gate))
            ).astype(bf16)
    part_ref[...] = dot(out_ref[...], wp_ref[...])


def final_kernel(
    home_ref, one_ref, two_ref, three_ref, reads_ref, local_ref, gate_ref, hgain_ref, part_ref,
    wr_ref,
    send_ref, rec,
    starts,
):
    tp = lax.axis_index("tp")
    y = lax.axis_index("sp_1")
    for step, src in enumerate((home_ref, one_ref, two_ref, three_ref)):
        starts[(y + 4 - step) & 3] = src[...]
    masks = head_masks()
    row, col = iota(128, 128, 0), iota(128, 128, 1)
    mean_of = jnp.where((row >> 6) == (col >> 6), 1.0 / HEAD, 0.0).astype(bf16)
    is_first = tp == 0
    for u in range(UNITS):
        s, h = u // 3, u % 3
        lanes = slice(h * 128, h * 128 + 128)
        shifted = slice(384 + h * 128, 384 + h * 128 + 128)
        rows = slice(s * 128, s * 128 + 128)
        out = dot(reads_ref[u], both(starts[h, s], masks), NT) + local_ref[u]
        out = out - dot_fine_left(out, mean_of)
        spread = dot(out * out, mean_of)
        gain = jnp.where(is_first, line_of(hgain_ref, lanes), line_of(hgain_ref, shifted))
        gate = gate_ref[rows, lanes].astype(f32)
        rec[rows, lanes] = (
            out * lax.rsqrt(spread + 1.0) * gain * (gate * jax.nn.sigmoid(gate))
        ).astype(bf16)
    cols = pl.ds(pl.multiple_of((1 - tp) * 1024, 1024), 1024)
    send_ref[...] = (dot(rec[...], wr_ref[:, cols]) + part_ref[:, cols]).astype(bf16)


def keep_kernel(rec_ref, part_ref, wr_ref, keep_ref):
    cols = pl.ds(pl.multiple_of(lax.axis_index("tp") * 1024, 1024), 1024)
    keep_ref[...] = (dot(rec_ref[...], wr_ref[:, cols]) + part_ref[:, cols]).astype(bf16)


def sum_kernel(keep_ref, arrived_ref, out_ref, buf, sems):
    copies = []
    for i in range(4):
        rows = slice(i * 64, i * 64 + 64)
        buf[rows] = (keep_ref[rows].astype(f32) + arrived_ref[rows].astype(f32)).astype(bf16)
        copies.append(pltpu.make_async_copy(buf.at[rows], out_ref.at[rows], sems.at[i]))
        copies[-1].start()
    finish(copies)


def vmem(count):
    return [pl.BlockSpec(memory_space=pltpu.VMEM)] * count


def hbm(count):
    return [pl.BlockSpec(memory_space=pltpu.HBM)] * count


def shape(dims, kind=bf16):
    return jax.ShapeDtypeStruct(dims, kind)


def call(body, name, ins, outs, scratch, limit, flops=0):
    return pl.pallas_call(
        body,
        name=name,
        out_shape=outs,
        in_specs=ins,
        out_specs=vmem(len(outs)) if isinstance(outs, (list, tuple)) else vmem(1)[0],
        scratch_shapes=scratch,
        compiler_params=pltpu.CompilerParams(vmem_limit_bytes=limit * MIB),
        cost_estimate=pl.CostEstimate(flops=flops, transcendentals=0, bytes_accessed=0) if flops else None,
    )


def around(parts, axis):
    return [
        lax.ppermute(part, axis, [(i, (i + step) & 3) for i in range(4)]) for step, part in enumerate(parts, 1)
    ]


def shards(
    tokens, norm_gain, w_recept, w_key, w_value, w_decay, w_rate, w_gate_rec, w_pool, w_gate_pool,
    decay_base, rate_base, head_gain, pool_mix, pool_scale, w_out_rec, w_out_pool, init_state,
):
    other = lax.ppermute(tokens, "tp", [(0, 1), (1, 0)])
    line = lambda x: x.reshape(1, -1)
    pinned = lambda x: pltpu.with_memory_space_constraint(x, pltpu.HBM)
    weights = [pinned(w) for w in (w_key, w_decay, w_rate, w_value)]
    own_normed, squares, *prepared = call(
        own_kernel,
        "own",
        hbm(6),
        [shape((256, 1024)), shape((256, 128), f32)]
        + [shape((256, 1536), f32), shape((1024, 1536))],
        [pltpu.VMEM((1024, 1536), bf16)]
        + [
            pltpu.SemaphoreType.DMA((8,)), pltpu.VMEM((256, 1024), bf16), pltpu.VMEM((1, D), f32),
            pltpu.SemaphoreType.DMA((2,)),
        ],
        20,
        1_000_000_000,
    )(pinned(tokens.reshape(256, 1024)), pinned(line(norm_gain)), *weights)
    normed, scale, pool, home, m1, m2, m3, right, solved, v, grow, lift = call(
        local_kernel,
        "local",
        vmem(9),
        [
            shape((256, 1024)), shape((256, 128), f32), shape((256, 256)),
            shape((256, 128)), shape((320, 128)), shape((256, 128)), shape((256, 128)),
            shape((6, 256, 128)), shape((6, 128, 256)), shape((6, 128, 128)),
            shape((6, 128, 128), f32), shape((6, 128), f32),
        ],
        [pltpu.VMEM((6, 128, 128), f32)] * 3
        + [pltpu.VMEM((4, 256, 128), bf16)]
        + [pltpu.VMEM((D, 256), bf16), pltpu.SemaphoreType.DMA((1,))],
        24,
        3_000_000_000,
    )(
        other.reshape(256, 1024), own_normed, line(norm_gain), squares, decay_base, rate_base, *prepared,
        w_pool,
    )
    r1, r2, r3 = around((m1, m2, m3), "sp_1")
    reads, local, gate, pgate = call(
        side_kernel,
        "side",
        vmem(11),
        [shape((6, 128, 128)), shape((6, 128, 128), f32), shape((256, 384)), shape((256, 256))],
        [],
        16,
        1_000_000_000,
    )(own_normed, normed, scale, right, solved, v, grow, lift, w_recept, w_gate_rec, w_gate_pool)
    prefix, onward, total = call(
        row_kernel,
        "row",
        vmem(4) + [pl.BlockSpec(memory_space=pl.ANY)],
        [shape((3, 2, 128, 128), f32), shape((320, 128)), shape((256, 128))],
        [pltpu.VMEM((4, 256, 128), bf16)],
        8,
        100_000_000,
    )(home, r1, r2, r3, pgate)
    columns = around((onward, total, total), "sp_0")
    s0, s1, s2, s3 = call(
        column_kernel,
        "column",
        vmem(5),
        [shape((2, 64, 128))] * 4,
        [pltpu.VMEM((4, 2, 64, 128), bf16), pltpu.VMEM((4, 256, 128), bf16)],
        8,
        100_000_000,
    )(prefix, *columns, init_state)
    t1, t2, t3 = around((s1, s2, s3), "sp_1")
    pool_part = call(
        pool_kernel, "pool", vmem(7), shape((256, D), f32), [pltpu.VMEM((256, 256), bf16)], 12, 300_000_000
    )(pool, r1, columns[0], pgate, pool_mix, line(pool_scale), w_out_pool)
    send, rec = call(
        final_kernel,
        "final",
        vmem(10),
        [shape((256, 1024)), shape((256, 384))],
        [pltpu.VMEM((4, 2, 64, 128), bf16)],
        20,
        1_000_000_000,
    )(s0, t1, t2, t3, reads, local, gate, head_gain, pool_part, w_out_rec)
    arrived = lax.ppermute(send, "tp", [(0, 1), (1, 0)])
    keep = call(keep_kernel, "keep", vmem(3), shape((256, 1024)), [], 8, 300_000_000)(rec, pool_part, w_out_rec)
    mixed = pl.pallas_call(
        sum_kernel,
        name="sum",
        out_shape=shape((256, 1024)),
        in_specs=vmem(2),
        out_specs=hbm(1)[0],
        scratch_shapes=[pltpu.VMEM((256, 1024), bf16), pltpu.SemaphoreType.DMA((4,))],
        compiler_params=pltpu.CompilerParams(vmem_limit_bytes=4 * MIB),
    )(keep, arrived)
    return mixed.reshape(2, 128, 1024)


def solution(mesh):
    split = Mesh(
        mesh.devices.reshape(4, 4, mesh.shape["fs"], mesh.shape["tp"]), ("sp_0", "sp_1", "fs", "tp")
    )
    column = P(None, "tp")
    placed = (
        (P("fs", SP, "tp"), P()) + (column,) * 8 + (P(),) * 5
        + (P("tp", None), P("tp", None), P("fs", "tp", None, None))
    )
    return jax.shard_map(
        shards, mesh=split, in_specs=placed, out_specs=P("fs", SP, "tp"), check_vma=False
    )
```

```python
import functools

import jax
import jax.numpy as jnp
from jax import lax
from jax.experimental import pallas as pl
from jax.experimental.pallas import tpu as pltpu
from jax.sharding import Mesh
from jax.sharding import PartitionSpec as P

D = 2048
HEAD = 64
SPAN = 128
UNITS = 6
SP = ("sp_0", "sp_1")
f32 = jnp.float32
bf16 = jnp.bfloat16
NN = ((1,), (0,))
NT = ((1,), (1,))
TN = ((0,), (0,))
MIB = 2**20


def dot(a, b, dims=NN):
    return lax.dot_general(
        a.astype(bf16), b.astype(bf16), (dims, ((), ())), preferred_element_type=f32
    )


def halves(x):
    high = x.astype(bf16)
    return high, (x - high.astype(f32)).astype(bf16)


def dot_fine_left(a, b, dims=NN):
    b = b.astype(bf16)
    return dot(jnp.concatenate(halves(a), axis=1), jnp.concatenate([b, b], axis=0), dims)


def dot_fine_right(a, b, dims=NN):
    a = a.astype(bf16)
    return dot(jnp.concatenate([a, a], axis=1), jnp.concatenate(halves(b), axis=0), dims)


def iota(rows, cols, dim):
    return lax.broadcasted_iota(jnp.int32, (rows, cols), dim)


def line_of(ref, lanes):
    if len(ref.shape) == 1:
        return ref[lanes].reshape(1, 128)
    return ref[:, lanes]


def head_masks():
    first = (iota(1, 128, 1) < HEAD).astype(f32)
    return first.astype(bf16), (1.0 - first).astype(bf16)


def both(x, masks):
    x = x.astype(bf16)
    return jnp.concatenate([x * masks[0], x * masks[1]], axis=0)


def joined(x):
    return jnp.where(iota(HEAD, 128, 1) < HEAD, x[:HEAD], x[HEAD:])


def compose(earlier, later, masks):
    high, low = halves(earlier) if earlier.dtype == f32 else (earlier, None)
    upper, lower = halves(later[:HEAD]) if later.dtype == f32 else (later[:HEAD], None)
    left, right = [high], [both(upper, masks)]
    if low is not None:
        left.append(low)
        right.append(right[0])
    if lower is not None:
        left.append(high)
        right.append(both(lower, masks))
    moved = dot(jnp.concatenate(left, axis=1), jnp.concatenate(right, axis=0))
    written = later[HEAD:].astype(f32)
    if earlier.shape[0] == HEAD:
        return moved + written
    return jnp.concatenate([moved[:HEAD], moved[HEAD:] + written], axis=0)


def pick(x, size, odd):
    parts = [x[s : s + size] for s in range(size * odd, SPAN, 2 * size)]
    return parts[0] if len(parts) == 1 else jnp.concatenate(parts, axis=0)


def weave(even, odd, size):
    parts = []
    for s in range(0, SPAN // 2, size):
        parts += [even[s : s + size], odd[s : s + size]]
    return jnp.concatenate(parts, axis=0)


def woven(part, size):
    if size >= 16:
        part = part.astype(bf16)
    return weave(jnp.zeros_like(part), part, size)


def blocks(x):
    x = x.astype(bf16)
    zero = jnp.zeros((SPAN, 128), bf16)
    return jnp.concatenate(
        [jnp.concatenate([x[:, :128], zero], axis=1), jnp.concatenate([zero, x[:, 128:]], axis=1)], axis=0
    )


def inverses(lowers, fill):
    row, col = iota(SPAN, 256, 0), iota(SPAN, 256, 1) & 127
    eye = (row == col).astype(f32)
    near = ((row >> 1) == (col >> 1)).astype(bf16)
    result = [eye - (lower * near).astype(f32) for lower in lowers]
    size, level = 2, 1
    while size < SPAN:
        off = (((row >> (level + 1)) == (col >> (level + 1))) & ((row >> level) != (col >> level))).astype(bf16)
        if size < 8:
            inner = [dot(lower * off, blocks(inv)) for lower, inv in zip(lowers, result)]
            fill(level)
            result = [inv - dot(inv, blocks(part)) for inv, part in zip(result, inner)]
        else:
            if size < 16:
                off = pick(off.astype(f32), size, 1).astype(bf16)
                odd = [pick(lower.astype(f32), size, 1).astype(bf16) for lower in lowers]
            else:
                off = pick(off, size, 1)
                odd = [pick(lower, size, 1) for lower in lowers]
            inner = [dot(lower * off, blocks(inv)) for lower, inv in zip(odd, result)]
            fill(level)
            outer = [
                dot(pick(inv, size, 1), blocks(woven(part, size))) for inv, part in zip(result, inner)
            ]
            result = [
                weave(pick(inv, size, 0), pick(inv, size, 1) - part, size)
                for inv, part in zip(result, outer)
            ]
        size, level = size * 2, level + 1
    return result


def fetch(sources, buf, first_row, sems, base):
    copies, at = [], 0
    for i, src in enumerate(sources):
        width = src.shape[1]
        copies.append(
            pltpu.make_async_copy(
                src.at[pl.ds(pl.multiple_of(first_row, 1024), 1024), :],
                buf.at[:, at : at + width],
                sems.at[base + i],
            )
        )
        at += width
    return copies


def begin(copies):
    for copy in copies:
        copy.start()


def finish(copies):
    for copy in copies:
        copy.wait()


def own_kernel(*refs):
    token_ref, norm_ref = refs[:2]
    sources, normed_ref, squares_ref, partial_ref, rest_ref = refs[2:6], *refs[6:10]
    buf, sems, own_ref, gain_ref, first_sems = refs[10:15]
    tp = lax.axis_index("tp")
    early = [
        pltpu.make_async_copy(norm_ref, gain_ref, first_sems.at[0]),
        pltpu.make_async_copy(token_ref, own_ref, first_sems.at[1]),
    ]
    mine = fetch(sources, buf, tp * 1024, sems, 0)
    others = fetch(sources, rest_ref, (1 - tp) * 1024, sems, 4)
    mine = (mine[:2], mine[2:])
    others = (others[:2], others[2:])
    begin(early)
    begin(mine[0])
    pl.delay(400)
    begin(mine[1])
    pl.delay(400)
    begin(others[0])
    finish(early)
    own = own_ref[...].astype(f32)
    normed = (own * jnp.where(tp == 0, gain_ref[:, :1024], gain_ref[:, 1024:])).astype(bf16)
    normed_ref[...] = normed
    squares_ref[...] = jnp.broadcast_to(jnp.sum(own * own, axis=1, keepdims=True), (256, 128))
    begin(others[1])
    for i in range(2):
        finish(mine[i])
        cols = slice(768 * i, 768 * i + 768)
        partial_ref[:, cols] = dot(normed_ref[...], buf[:, cols])
    finish(others[0])
    finish(others[1])


def local_kernel(*refs):
    other_ref, own_ref, gain_ref, squares_ref, db_ref, rb_ref = refs[:6]
    partial_ref, rest_ref, pool_weight = refs[6:9]
    (
        normed_ref, scale_ref, pool_ref, home_ref, first_ref, second_ref, third_ref,
        right_ref, solved_ref, v_ref, grow_ref, lift_ref,
    ) = refs[9:21]
    k_s, d_s, a_s, maps, pool_buf, sems = refs[21:27]
    tp = lax.axis_index("tp")
    y = lax.axis_index("sp_1")
    pool_buf = pool_weight
    is_first = tp == 0
    other = other_ref[...].astype(f32)
    normed = (other * jnp.where(is_first, gain_ref[:, 1024:], gain_ref[:, :1024])).astype(bf16)
    normed_ref[...] = normed
    squares = squares_ref[:, :1] + jnp.sum(other * other, axis=1, keepdims=True)
    scale = lax.rsqrt(squares * (1.0 / D) + 0.25)
    scale_ref[...] = jnp.broadcast_to(scale, (256, 128))

    def project(rows, cols):
        total = partial_ref[rows, cols] + dot(normed_ref[rows], rest_ref[:, cols])
        return (total * scale_ref[rows, :1]).astype(bf16)

    rounded = project(slice(0, 256), slice(0, 1152))
    for u in range(UNITS):
        s, h = u // 3, u % 3
        for i, dest in enumerate((k_s, d_s, a_s)):
            at = 384 * i + h * 128
            dest[u] = rounded[s * 128 : s * 128 + 128, at : at + 128].astype(f32)

    def fill(level):
        if level > 4:
            return
        s = (level - 1) & 1
        rows = slice(s * 128, s * 128 + 128)
        if level <= 2:
            value = project(rows, slice(1152, 1536))
            for h in range(3):
                v_ref[3 * s + h] = value[:, h * 128 : h * 128 + 128]
            return
        total = dot(own_ref[rows], pool_buf[pl.ds(pl.multiple_of(tp * 1024, 1024), 1024), :])
        total = total + dot(normed_ref[rows], pool_buf[pl.ds(pl.multiple_of((1 - tp) * 1024, 1024), 1024), :])
        pool = (total * scale_ref[rows, :1]).astype(bf16)
        pool_ref[rows] = pool
        for half in (0, 1):
            at = 256 + (2 * s + half) * 16
            first_ref[at : at + 16] = pool[112:128, half * 128 : half * 128 + 128]

    masks = head_masks()
    n = SPAN
    row, col = iota(n, n, 0), iota(n, n, 1)
    strict, inclusive = row > col, row >= col
    triangle = inclusive.astype(f32)
    ones = ((row >> 6) == (col >> 6)).astype(f32)
    wide = (
        jnp.concatenate([masks[0], masks[0]], axis=1),
        jnp.concatenate([masks[1], masks[1]], axis=1),
    )
    slab = iota(HEAD, 128, 0)
    eye = (slab == (iota(HEAD, 128, 1) & 63)).astype(f32)
    units = range(UNITS)
    first_stage = []
    for u in units:
        h = u % 3
        lanes = slice(h * 128, h * 128 + 128)
        shifted = slice(384 + h * 128, 384 + h * 128 + 128)
        db = jnp.where(is_first, line_of(db_ref, lanes), line_of(db_ref, shifted))
        k = k_s[u]
        log_decay = -0.6065306597126334 * jax.nn.sigmoid(db + d_s[u])
        first_stage.append((log_decay, dot(k * k, ones), dot_fine_right(triangle, log_decay)))
    second_stage = []
    for u in units:
        h = u % 3
        lanes = slice(h * 128, h * 128 + 128)
        shifted = slice(384 + h * 128, 384 + h * 128 + 128)
        rb = jnp.where(is_first, line_of(rb_ref, lanes), line_of(rb_ref, shifted))
        rate = jax.nn.sigmoid(rb + a_s[u])
        log_decay, squared, total = first_stage[u]
        k = k_s[u]
        middle = total[63:64]
        unit_key = k * lax.rsqrt(squared + 1.0)
        centred = total - middle
        alpha = jnp.exp(centred - log_decay) * unit_key
        fading = jnp.exp(-centred)
        grow_ref[u] = jnp.exp(centred)
        lift = jnp.exp(middle)
        lift_ref[u : u + 1] = lift
        right = jnp.concatenate(
            [(unit_key * rate * fading).astype(bf16), (k * fading).astype(bf16)], axis=0
        )
        right_ref[u] = right
        ends = (jnp.exp(total[127:128]), jnp.exp(centred[127:128]))
        second_stage.append((right, alpha * lift, ends, dot(both(alpha, masks), right, NT)))
    lowers, carries = [], []
    for u in units:
        pairs = second_stage[u][3]
        block = lambda j, c: jnp.where(
            strict, pairs[j * n : j * n + n, c * n : c * n + n], 0.0
        ).astype(bf16)
        lowers.append(jnp.concatenate([block(0, 0), block(1, 0)], axis=1))
        carries.append(jnp.concatenate([block(0, 1), block(1, 1)], axis=1))
    inverse = inverses(lowers, fill)
    carries = [dot(carries[u], both(v_ref[u], masks)) for u in units]
    solutions = []
    for u in units:
        wanted = jnp.concatenate([second_stage[u][1], carries[u]], axis=1)
        solutions.append((wanted, dot(inverse[u], both(wanted, wide))))
    missing = []
    for u in units:
        wanted, solved = solutions[u]
        high, low = halves(solved)
        left = jnp.concatenate([lowers[u], lowers[u]], axis=1)
        applied = dot(left, jnp.concatenate([both(high, wide), both(low, wide)], axis=0))
        missing.append(wanted - solved - applied)
    for u in units:
        solved = (solutions[u][1] + dot(inverse[u], both(missing[u], wide))).astype(bf16)
        solved_ref[u] = solved
        solutions[u] = solved
    for u in units:
        right, _, ends, _ = second_stage[u]
        solved = solutions[u]
        transit = eye * ends[0] - joined(dot(solved[:, :n], right[:n], TN)) * ends[1]
        written = joined(
            dot(
                jnp.concatenate([-solved[:, n:], v_ref[u]], axis=0),
                right,
                TN,
            )
        ) * ends[1]
        at = (u // 3) * 128
        maps[u % 3, at : at + HEAD] = transit.astype(bf16)
        maps[u % 3, at + HEAD : at + 128] = written.astype(bf16)
    maps[3] = jnp.zeros((256, 128), bf16)
    for step, dest in enumerate((home_ref, first_ref, second_ref, third_ref)):
        dest[:256] = maps[(y + step) & 3]


def side_kernel(
    own_ref, other_ref, scale_ref, right_ref, solved_ref, v_ref, grow_ref, lift_ref, wr_ref, wg_ref, wq_ref,
    reads_ref, local_ref, gate_ref, pgate_ref,
):
    tp = lax.axis_index("tp")
    scale = scale_ref[:, :1]
    mine, theirs = pl.multiple_of(tp * 1024, 1024), pl.multiple_of((1 - tp) * 1024, 1024)

    def project(weight):
        total = dot(own_ref[...], weight[pl.ds(mine, 1024), :])
        total = total + dot(other_ref[...], weight[pl.ds(theirs, 1024), :])
        return (total * scale).astype(bf16)

    receptance = project(wr_ref)
    masks = head_masks()
    wide = (
        jnp.concatenate([masks[0], masks[0]], axis=1),
        jnp.concatenate([masks[1], masks[1]], axis=1),
    )
    inclusive = iota(128, 128, 0) >= iota(128, 128, 1)
    inside, rhos = [], []
    for u in range(UNITS):
        s, h = u // 3, u % 3
        rho = receptance[s * 128 : s * 128 + 128, h * 128 : h * 128 + 128].astype(f32) * grow_ref[u]
        rhos.append(rho * lift_ref[u : u + 1])
        pairs = dot(both(rho, masks), right_ref[u], NT)
        block = lambda j, c: jnp.where(
            inclusive, pairs[j * 128 : j * 128 + 128, c * 128 : c * 128 + 128], 0.0
        ).astype(bf16)
        inside.append([jnp.concatenate([block(0, c), block(1, c)], axis=1) for c in (0, 1)])
    for u in range(UNITS):
        removed = dot(inside[u][0], both(solved_ref[u], wide))
        reads_ref[u] = (rhos[u] - removed[:, :128]).astype(bf16)
        local_ref[u] = dot(inside[u][1], both(v_ref[u], masks)) - removed[:, 128:]
    gate_ref[...] = project(wg_ref)
    pgate_ref[...] = project(wq_ref)


def row_kernel(home_ref, first_ref, second_ref, third_ref, after_ref, prefix_ref, next_ref, total_ref, maps):
    y = lax.axis_index("sp_1")
    for step, src in enumerate((home_ref, first_ref, second_ref, third_ref)):
        maps[(y + 4 - step) & 3] = src[:256]
    next_ref[256:] = first_ref[256:]
    masks = head_masks()
    for s in (0, 1):
        rows = slice(s * 128, s * 128 + 128)
        own = [maps[j, rows] for j in range(4)]
        front = compose(own[0], own[1], masks)
        back = compose(own[2], own[3], masks)
        whole = compose(front, back, masks).astype(bf16)
        next_ref[rows] = whole
        total_ref[rows] = whole
        prefix_ref[0, s] = own[0].astype(f32)
        prefix_ref[1, s] = front
        prefix_ref[2, s] = compose(front, own[2], masks)


def column_kernel(
    prefix_ref, first_ref, second_ref, third_ref, init_ref,
    home_ref, one_ref, two_ref, three_ref,
    starts, rows,
):
    y = lax.axis_index("sp_1")
    z = lax.axis_index("sp_0")
    for step, src in enumerate((first_ref, second_ref, third_ref)):
        rows[(z + 3 - step) & 3] = src[:256]
    masks = head_masks()
    pair = jnp.minimum(y, 2) * 2
    for s in (0, 1):
        state = jnp.concatenate([init_ref[s, pair], init_ref[s, pair + 1]], axis=1)
        later = [rows[j, s * 128 : s * 128 + 128] for j in range(3)]
        first = compose(state, later[0], masks)
        second = compose(first, later[1], masks)
        third = compose(first, compose(later[1], later[2], masks), masks)
        state = jnp.where(z == 0, state, jnp.where(z == 1, first, jnp.where(z == 2, second, third)))
        starts[0, s] = state.astype(bf16)
        for j in range(3):
            starts[j + 1, s] = compose(state, prefix_ref[j, s], masks).astype(bf16)
    for step, dest in enumerate((home_ref, one_ref, two_ref, three_ref)):
        dest[...] = starts[(y + step) & 3]


def pool_kernel(pool_ref, beside_ref, above_ref, pgate_ref, mix_ref, pscale_ref, wp_ref, part_ref, out_ref):
    tp = lax.axis_index("tp")
    y = lax.axis_index("sp_1")
    place = lax.axis_index("sp_0") * 4 + y
    is_first = tp == 0
    factor = jnp.where(is_first, pscale_ref[:, :256], pscale_ref[:, 256:])
    for s in (0, 1):
        current = pool_ref[s * 128 : s * 128 + 128].astype(f32)
        tails = []
        for half in (0, 1):
            rows = slice(256 + (2 * s + half) * 16, 272 + (2 * s + half) * 16)
            tails.append(
                jnp.where(
                    place == 0,
                    0.0,
                    jnp.where(y > 0, beside_ref[rows].astype(f32), above_ref[rows].astype(f32)),
                )
            )
        padded = jnp.concatenate([jnp.concatenate(tails, axis=1), current], axis=0)
        sums = {1: padded}
        for by in (1, 2, 4, 8):
            before = sums[by]
            moved = jnp.concatenate([jnp.zeros((by, 256), f32), before[: 144 - by]], axis=0)
            sums[2 * by] = before + moved
        position = (place * 128 + iota(128, 128, 0) + 1).astype(f32)
        for g in (0, 1):
            lanes = slice(g * 128, g * 128 + 128)
            small, large = 2 << g, 8 << g
            trailing = jnp.where(is_first, sums[small][16:, lanes], sums[large][16:, lanes])
            window = jnp.where(is_first, float(small), float(large))
            diffs = trailing / jnp.minimum(position, window) - current[:, lanes]
            mixed = dot(diffs.astype(bf16), mix_ref[tp * 2 + g])
            gate = pgate_ref[s * 128 : s * 128 + 128, lanes].astype(f32)
            out_ref[s * 128 : s * 128 + 128, lanes] = (
                mixed * factor[:, lanes] * (gate * jax.nn.sigmoid(gate))
            ).astype(bf16)
    part_ref[...] = dot(out_ref[...], wp_ref[...])


def final_kernel(
    home_ref, one_ref, two_ref, three_ref, reads_ref, local_ref, gate_ref, hgain_ref, part_ref,
    wr_ref,
    send_ref, rec,
    starts,
):
    tp = lax.axis_index("tp")
    y = lax.axis_index("sp_1")
    for step, src in enumerate((home_ref, one_ref, two_ref, three_ref)):
        starts[(y + 4 - step) & 3] = src[...]
    masks = head_masks()
    row, col = iota(128, 128, 0), iota(128, 128, 1)
    mean_of = jnp.where((row >> 6) == (col >> 6), 1.0 / HEAD, 0.0).astype(bf16)
    is_first = tp == 0
    for u in range(UNITS):
        s, h = u // 3, u % 3
        lanes = slice(h * 128, h * 128 + 128)
        shifted = slice(384 + h * 128, 384 + h * 128 + 128)
        rows = slice(s * 128, s * 128 + 128)
        out = dot(reads_ref[u], both(starts[h, s], masks), NT) + local_ref[u]
        out = out - dot_fine_left(out, mean_of)
        spread = dot(out * out, mean_of)
        gain = jnp.where(is_first, line_of(hgain_ref, lanes), line_of(hgain_ref, shifted))
        gate = gate_ref[rows, lanes].astype(f32)
        rec[rows, lanes] = (
            out * lax.rsqrt(spread + 1.0) * gain * (gate * jax.nn.sigmoid(gate))
        ).astype(bf16)
    cols = pl.ds(pl.multiple_of((1 - tp) * 1024, 1024), 1024)
    send_ref[...] = (dot(rec[...], wr_ref[:, cols]) + part_ref[:, cols]).astype(bf16)


def keep_kernel(rec_ref, part_ref, wr_ref, keep_ref):
    cols = pl.ds(pl.multiple_of(lax.axis_index("tp") * 1024, 1024), 1024)
    keep_ref[...] = (dot(rec_ref[...], wr_ref[:, cols]) + part_ref[:, cols]).astype(bf16)


def sum_kernel(keep_ref, arrived_ref, out_ref, buf, sems):
    copies = []
    for i in range(4):
        rows = slice(i * 64, i * 64 + 64)
        buf[rows] = (keep_ref[rows].astype(f32) + arrived_ref[rows].astype(f32)).astype(bf16)
        copies.append(pltpu.make_async_copy(buf.at[rows], out_ref.at[rows], sems.at[i]))
        copies[-1].start()
    finish(copies)


def vmem(count):
    return [pl.BlockSpec(memory_space=pltpu.VMEM)] * count


def hbm(count):
    return [pl.BlockSpec(memory_space=pltpu.HBM)] * count


def shape(dims, kind=bf16):
    return jax.ShapeDtypeStruct(dims, kind)


def call(body, name, ins, outs, scratch, limit, flops=0):
    return pl.pallas_call(
        body,
        name=name,
        out_shape=outs,
        in_specs=ins,
        out_specs=vmem(len(outs)) if isinstance(outs, (list, tuple)) else vmem(1)[0],
        scratch_shapes=scratch,
        compiler_params=pltpu.CompilerParams(vmem_limit_bytes=limit * MIB),
        cost_estimate=pl.CostEstimate(flops=flops, transcendentals=0, bytes_accessed=0) if flops else None,
    )


def around(parts, axis):
    return [
        lax.ppermute(part, axis, [(i, (i + step) & 3) for i in range(4)]) for step, part in enumerate(parts, 1)
    ]


def shards(
    tokens, norm_gain, w_recept, w_key, w_value, w_decay, w_rate, w_gate_rec, w_pool, w_gate_pool,
    decay_base, rate_base, head_gain, pool_mix, pool_scale, w_out_rec, w_out_pool, init_state,
):
    other = lax.ppermute(tokens, "tp", [(0, 1), (1, 0)])
    line = lambda x: x.reshape(1, -1)
    pinned = lambda x: pltpu.with_memory_space_constraint(x, pltpu.HBM)
    weights = [pinned(w) for w in (w_key, w_decay, w_rate, w_value)]
    own_normed, squares, *prepared = call(
        own_kernel,
        "own",
        hbm(6),
        [shape((256, 1024)), shape((256, 128), f32)]
        + [shape((256, 1536), f32), shape((1024, 1536))],
        [pltpu.VMEM((1024, 1536), bf16)]
        + [
            pltpu.SemaphoreType.DMA((8,)), pltpu.VMEM((256, 1024), bf16), pltpu.VMEM((1, D), f32),
            pltpu.SemaphoreType.DMA((2,)),
        ],
        20,
        1_000_000_000,
    )(pinned(tokens.reshape(256, 1024)), pinned(line(norm_gain)), *weights)
    normed, scale, pool, home, m1, m2, m3, right, solved, v, grow, lift = call(
        local_kernel,
        "local",
        vmem(9),
        [
            shape((256, 1024)), shape((256, 128), f32), shape((256, 256)),
            shape((256, 128)), shape((320, 128)), shape((256, 128)), shape((256, 128)),
            shape((6, 256, 128)), shape((6, 128, 256)), shape((6, 128, 128)),
            shape((6, 128, 128), f32), shape((6, 128), f32),
        ],
        [pltpu.VMEM((6, 128, 128), f32)] * 3
        + [pltpu.VMEM((4, 256, 128), bf16)]
        + [pltpu.VMEM((D, 256), bf16), pltpu.SemaphoreType.DMA((1,))],
        24,
        3_000_000_000,
    )(
        other.reshape(256, 1024), own_normed, line(norm_gain), squares, decay_base, rate_base, *prepared,
        w_pool,
    )
    r1, r2, r3 = around((m1, m2, m3), "sp_1")
    reads, local, gate, pgate = call(
        side_kernel,
        "side",
        vmem(11),
        [shape((6, 128, 128)), shape((6, 128, 128), f32), shape((256, 384)), shape((256, 256))],
        [],
        16,
        1_000_000_000,
    )(own_normed, normed, scale, right, solved, v, grow, lift, w_recept, w_gate_rec, w_gate_pool)
    prefix, onward, total = call(
        row_kernel,
        "row",
        vmem(4) + [pl.BlockSpec(memory_space=pl.ANY)],
        [shape((3, 2, 128, 128), f32), shape((320, 128)), shape((256, 128))],
        [pltpu.VMEM((4, 256, 128), bf16)],
        8,
        100_000_000,
    )(home, r1, r2, r3, pgate)
    columns = around((onward, total, total), "sp_0")
    s0, s1, s2, s3 = call(
        column_kernel,
        "column",
        vmem(5),
        [shape((2, 64, 128))] * 4,
        [pltpu.VMEM((4, 2, 64, 128), bf16), pltpu.VMEM((4, 256, 128), bf16)],
        8,
        100_000_000,
    )(prefix, *columns, init_state)
    t1, t2, t3 = around((s1, s2, s3), "sp_1")
    pool_part = call(
        pool_kernel, "pool", vmem(7), shape((256, D), f32), [pltpu.VMEM((256, 256), bf16)], 12, 300_000_000
    )(pool, r1, columns[0], pgate, pool_mix, line(pool_scale), w_out_pool)
    send, rec = call(
        final_kernel,
        "final",
        vmem(10),
        [shape((256, 1024)), shape((256, 384))],
        [pltpu.VMEM((4, 2, 64, 128), bf16)],
        20,
        1_000_000_000,
    )(s0, t1, t2, t3, reads, local, gate, head_gain, pool_part, w_out_rec)
    arrived = lax.ppermute(send, "tp", [(0, 1), (1, 0)])
    keep = call(keep_kernel, "keep", vmem(3), shape((256, 1024)), [], 8, 300_000_000)(rec, pool_part, w_out_rec)
    mixed = pl.pallas_call(
        sum_kernel,
        name="sum",
        out_shape=shape((256, 1024)),
        in_specs=vmem(2),
        out_specs=hbm(1)[0],
        scratch_shapes=[pltpu.VMEM((256, 1024), bf16), pltpu.SemaphoreType.DMA((4,))],
        compiler_params=pltpu.CompilerParams(vmem_limit_bytes=4 * MIB),
    )(keep, arrived)
    return mixed.reshape(2, 128, 1024)


def solution(mesh):
    split = Mesh(
        mesh.devices.reshape(4, 4, mesh.shape["fs"], mesh.shape["tp"]), ("sp_0", "sp_1", "fs", "tp")
    )
    column = P(None, "tp")
    placed = (
        (P("fs", SP, "tp"), P()) + (column,) * 8 + (P(),) * 5
        + (P("tp", None), P("tp", None), P("fs", "tp", None, None))
    )
    return jax.shard_map(
        shards, mesh=split, in_specs=placed, out_specs=P("fs", SP, "tp"), check_vma=False
    )
```

```python
import functools

import jax
import jax.numpy as jnp
from jax import lax
from jax.experimental import pallas as pl
from jax.experimental.pallas import tpu as pltpu
from jax.sharding import Mesh
from jax.sharding import PartitionSpec as P

D = 2048
HEAD = 64
SPAN = 128
UNITS = 6
SP = ("sp_0", "sp_1")
f32 = jnp.float32
bf16 = jnp.bfloat16
NN = ((1,), (0,))
NT = ((1,), (1,))
TN = ((0,), (0,))
MIB = 2**20


def dot(a, b, dims=NN):
    return lax.dot_general(
        a.astype(bf16), b.astype(bf16), (dims, ((), ())), preferred_element_type=f32
    )


def halves(x):
    high = x.astype(bf16)
    return high, (x - high.astype(f32)).astype(bf16)


def dot_fine_left(a, b, dims=NN):
    b = b.astype(bf16)
    return dot(jnp.concatenate(halves(a), axis=1), jnp.concatenate([b, b], axis=0), dims)


def dot_fine_right(a, b, dims=NN):
    a = a.astype(bf16)
    return dot(jnp.concatenate([a, a], axis=1), jnp.concatenate(halves(b), axis=0), dims)


def iota(rows, cols, dim):
    return lax.broadcasted_iota(jnp.int32, (rows, cols), dim)


def line_of(ref, lanes):
    if len(ref.shape) == 1:
        return ref[lanes].reshape(1, 128)
    return ref[:, lanes]


def head_masks():
    first = (iota(1, 128, 1) < HEAD).astype(f32)
    return first.astype(bf16), (1.0 - first).astype(bf16)


def both(x, masks):
    x = x.astype(bf16)
    return jnp.concatenate([x * masks[0], x * masks[1]], axis=0)


def joined(x):
    return jnp.where(iota(HEAD, 128, 1) < HEAD, x[:HEAD], x[HEAD:])


def compose(earlier, later, masks):
    high, low = halves(earlier) if earlier.dtype == f32 else (earlier, None)
    upper, lower = halves(later[:HEAD]) if later.dtype == f32 else (later[:HEAD], None)
    left, right = [high], [both(upper, masks)]
    if low is not None:
        left.append(low)
        right.append(right[0])
    if lower is not None:
        left.append(high)
        right.append(both(lower, masks))
    moved = dot(jnp.concatenate(left, axis=1), jnp.concatenate(right, axis=0))
    written = later[HEAD:].astype(f32)
    if earlier.shape[0] == HEAD:
        return moved + written
    return jnp.concatenate([moved[:HEAD], moved[HEAD:] + written], axis=0)


def pick(x, size, odd):
    parts = [x[s : s + size] for s in range(size * odd, SPAN, 2 * size)]
    return parts[0] if len(parts) == 1 else jnp.concatenate(parts, axis=0)


def weave(even, odd, size):
    parts = []
    for s in range(0, SPAN // 2, size):
        parts += [even[s : s + size], odd[s : s + size]]
    return jnp.concatenate(parts, axis=0)


def woven(part, size):
    if size >= 16:
        part = part.astype(bf16)
    return weave(jnp.zeros_like(part), part, size)


def blocks(x):
    x = x.astype(bf16)
    zero = jnp.zeros((SPAN, 128), bf16)
    return jnp.concatenate(
        [jnp.concatenate([x[:, :128], zero], axis=1), jnp.concatenate([zero, x[:, 128:]], axis=1)], axis=0
    )


def inverses(lowers, fill):
    row, col = iota(SPAN, 256, 0), iota(SPAN, 256, 1) & 127
    eye = (row == col).astype(f32)
    near = ((row >> 1) == (col >> 1)).astype(bf16)
    result = [eye - (lower * near).astype(f32) for lower in lowers]
    size, level = 2, 1
    while size < 8:
        off = (((row >> (level + 1)) == (col >> (level + 1))) & ((row >> level) != (col >> level))).astype(bf16)
        inner = [dot(lower * off, blocks(inv)) for lower, inv in zip(lowers, result)]
        fill(level)
        result = [inv - dot(inv, blocks(part)) for inv, part in zip(result, inner)]
        size, level = size * 2, level + 1
    for turn in (3, 4):
        off = (((row >> (level + 2)) == (col >> (level + 2))) & ((row >> level) != (col >> level))).astype(bf16)
        mixes = [dot(inv, blocks(lower * off)).astype(bf16) for lower, inv in zip(lowers, result)]
        fill(turn)
        squares = [dot(mix, blocks(mix)) for mix in mixes]
        halfway = [inv - dot(mix, blocks(inv)) for mix, inv in zip(mixes, result)]
        result = [part + dot(square, blocks(part)) for part, square in zip(halfway, squares)]
        level += 2
    return result


def fetch(sources, buf, first_row, sems, base):
    copies, at = [], 0
    for i, src in enumerate(sources):
        width = src.shape[1]
        copies.append(
            pltpu.make_async_copy(
                src.at[pl.ds(pl.multiple_of(first_row, 1024), 1024), :],
                buf.at[:, at : at + width],
                sems.at[base + i],
            )
        )
        at += width
    return copies


def begin(copies):
    for copy in copies:
        copy.start()


def finish(copies):
    for copy in copies:
        copy.wait()


def own_kernel(*refs):
    token_ref, norm_ref = refs[:2]
    sources, normed_ref, squares_ref, partial_ref, rest_ref = refs[2:6], *refs[6:10]
    buf, sems, own_ref, gain_ref, first_sems = refs[10:15]
    tp = lax.axis_index("tp")
    early = [
        pltpu.make_async_copy(norm_ref, gain_ref, first_sems.at[0]),
        pltpu.make_async_copy(token_ref, own_ref, first_sems.at[1]),
    ]
    mine = fetch(sources, buf, tp * 1024, sems, 0)
    others = fetch(sources, rest_ref, (1 - tp) * 1024, sems, 4)
    mine = (mine[:2], mine[2:])
    others = (others[:2], others[2:])
    begin(early)
    begin(mine[0])
    pl.delay(400)
    begin(mine[1])
    pl.delay(400)
    begin(others[0])
    finish(early)
    own = own_ref[...].astype(f32)
    normed = (own * jnp.where(tp == 0, gain_ref[:, :1024], gain_ref[:, 1024:])).astype(bf16)
    normed_ref[...] = normed
    squares_ref[...] = jnp.broadcast_to(jnp.sum(own * own, axis=1, keepdims=True), (256, 128))
    begin(others[1])
    for i in range(2):
        finish(mine[i])
        cols = slice(768 * i, 768 * i + 768)
        partial_ref[:, cols] = dot(normed_ref[...], buf[:, cols])
    finish(others[0])
    finish(others[1])


def local_kernel(*refs):
    other_ref, own_ref, gain_ref, squares_ref, db_ref, rb_ref = refs[:6]
    partial_ref, rest_ref, pool_weight = refs[6:9]
    (
        normed_ref, scale_ref, pool_ref, home_ref, first_ref, second_ref, third_ref,
        right_ref, solved_ref, v_ref, grow_ref, lift_ref,
    ) = refs[9:21]
    k_s, d_s, a_s, maps, pool_buf, sems = refs[21:27]
    tp = lax.axis_index("tp")
    y = lax.axis_index("sp_1")
    pool_buf = pool_weight
    is_first = tp == 0
    other = other_ref[...].astype(f32)
    normed = (other * jnp.where(is_first, gain_ref[:, 1024:], gain_ref[:, :1024])).astype(bf16)
    normed_ref[...] = normed
    squares = squares_ref[:, :1] + jnp.sum(other * other, axis=1, keepdims=True)
    scale = lax.rsqrt(squares * (1.0 / D) + 0.25)
    scale_ref[...] = jnp.broadcast_to(scale, (256, 128))

    def project(rows, cols):
        total = partial_ref[rows, cols] + dot(normed_ref[rows], rest_ref[:, cols])
        return (total * scale_ref[rows, :1]).astype(bf16)

    rounded = project(slice(0, 256), slice(0, 1152))
    for u in range(UNITS):
        s, h = u // 3, u % 3
        for i, dest in enumerate((k_s, d_s, a_s)):
            at = 384 * i + h * 128
            dest[u] = rounded[s * 128 : s * 128 + 128, at : at + 128].astype(f32)

    def fill(level):
        if level > 4:
            return
        s = (level - 1) & 1
        rows = slice(s * 128, s * 128 + 128)
        if level <= 2:
            value = project(rows, slice(1152, 1536))
            for h in range(3):
                v_ref[3 * s + h] = value[:, h * 128 : h * 128 + 128]
            return
        total = dot(own_ref[rows], pool_buf[pl.ds(pl.multiple_of(tp * 1024, 1024), 1024), :])
        total = total + dot(normed_ref[rows], pool_buf[pl.ds(pl.multiple_of((1 - tp) * 1024, 1024), 1024), :])
        pool = (total * scale_ref[rows, :1]).astype(bf16)
        pool_ref[rows] = pool
        for half in (0, 1):
            at = 256 + (2 * s + half) * 16
            first_ref[at : at + 16] = pool[112:128, half * 128 : half * 128 + 128]

    masks = head_masks()
    n = SPAN
    row, col = iota(n, n, 0), iota(n, n, 1)
    strict, inclusive = row > col, row >= col
    triangle = inclusive.astype(f32)
    ones = ((row >> 6) == (col >> 6)).astype(f32)
    wide = (
        jnp.concatenate([masks[0], masks[0]], axis=1),
        jnp.concatenate([masks[1], masks[1]], axis=1),
    )
    slab = iota(HEAD, 128, 0)
    eye = (slab == (iota(HEAD, 128, 1) & 63)).astype(f32)
    units = range(UNITS)
    first_stage = []
    for u in units:
        h = u % 3
        lanes = slice(h * 128, h * 128 + 128)
        shifted = slice(384 + h * 128, 384 + h * 128 + 128)
        db = jnp.where(is_first, line_of(db_ref, lanes), line_of(db_ref, shifted))
        k = k_s[u]
        log_decay = -0.6065306597126334 * jax.nn.sigmoid(db + d_s[u])
        first_stage.append((log_decay, dot(k * k, ones), dot_fine_right(triangle, log_decay)))
    second_stage = []
    for u in units:
        h = u % 3
        lanes = slice(h * 128, h * 128 + 128)
        shifted = slice(384 + h * 128, 384 + h * 128 + 128)
        rb = jnp.where(is_first, line_of(rb_ref, lanes), line_of(rb_ref, shifted))
        rate = jax.nn.sigmoid(rb + a_s[u])
        log_decay, squared, total = first_stage[u]
        k = k_s[u]
        middle = total[63:64]
        unit_key = k * lax.rsqrt(squared + 1.0)
        centred = total - middle
        alpha = jnp.exp(centred - log_decay) * unit_key
        fading = jnp.exp(-centred)
        grow_ref[u] = jnp.exp(centred)
        lift = jnp.exp(middle)
        lift_ref[u : u + 1] = lift
        right = jnp.concatenate(
            [(unit_key * rate * fading).astype(bf16), (k * fading).astype(bf16)], axis=0
        )
        right_ref[u] = right
        ends = (jnp.exp(total[127:128]), jnp.exp(centred[127:128]))
        second_stage.append((right, alpha * lift, ends, dot(both(alpha, masks), right, NT)))
    lowers, carries = [], []
    for u in units:
        pairs = second_stage[u][3]
        block = lambda j, c: jnp.where(
            strict, pairs[j * n : j * n + n, c * n : c * n + n], 0.0
        ).astype(bf16)
        lowers.append(jnp.concatenate([block(0, 0), block(1, 0)], axis=1))
        carries.append(jnp.concatenate([block(0, 1), block(1, 1)], axis=1))
    inverse = inverses(lowers, fill)
    carries = [dot(carries[u], both(v_ref[u], masks)) for u in units]
    solutions = []
    for u in units:
        wanted = jnp.concatenate([second_stage[u][1], carries[u]], axis=1)
        solutions.append((wanted, dot(inverse[u], both(wanted, wide))))
    missing = []
    for u in units:
        wanted, solved = solutions[u]
        high, low = halves(solved)
        left = jnp.concatenate([lowers[u], lowers[u]], axis=1)
        applied = dot(left, jnp.concatenate([both(high, wide), both(low, wide)], axis=0))
        missing.append(wanted - solved - applied)
    for u in units:
        solved = (solutions[u][1] + dot(inverse[u], both(missing[u], wide))).astype(bf16)
        solved_ref[u] = solved
        solutions[u] = solved
    for u in units:
        right, _, ends, _ = second_stage[u]
        solved = solutions[u]
        transit = eye * ends[0] - joined(dot(solved[:, :n], right[:n], TN)) * ends[1]
        written = joined(
            dot(
                jnp.concatenate([-solved[:, n:], v_ref[u]], axis=0),
                right,
                TN,
            )
        ) * ends[1]
        at = (u // 3) * 128
        maps[u % 3, at : at + HEAD] = transit.astype(bf16)
        maps[u % 3, at + HEAD : at + 128] = written.astype(bf16)
    maps[3] = jnp.zeros((256, 128), bf16)
    for step, dest in enumerate((home_ref, first_ref, second_ref, third_ref)):
        dest[:256] = maps[(y + step) & 3]


def side_kernel(
    own_ref, other_ref, scale_ref, right_ref, solved_ref, v_ref, grow_ref, lift_ref, wr_ref, wg_ref, wq_ref,
    reads_ref, local_ref, gate_ref, pgate_ref,
):
    tp = lax.axis_index("tp")
    scale = scale_ref[:, :1]
    mine, theirs = pl.multiple_of(tp * 1024, 1024), pl.multiple_of((1 - tp) * 1024, 1024)

    def project(weight):
        total = dot(own_ref[...], weight[pl.ds(mine, 1024), :])
        total = total + dot(other_ref[...], weight[pl.ds(theirs, 1024), :])
        return (total * scale).astype(bf16)

    receptance = project(wr_ref)
    masks = head_masks()
    wide = (
        jnp.concatenate([masks[0], masks[0]], axis=1),
        jnp.concatenate([masks[1], masks[1]], axis=1),
    )
    inclusive = iota(128, 128, 0) >= iota(128, 128, 1)
    inside, rhos = [], []
    for u in range(UNITS):
        s, h = u // 3, u % 3
        rho = receptance[s * 128 : s * 128 + 128, h * 128 : h * 128 + 128].astype(f32) * grow_ref[u]
        rhos.append(rho * lift_ref[u : u + 1])
        pairs = dot(both(rho, masks), right_ref[u], NT)
        block = lambda j, c: jnp.where(
            inclusive, pairs[j * 128 : j * 128 + 128, c * 128 : c * 128 + 128], 0.0
        ).astype(bf16)
        inside.append([jnp.concatenate([block(0, c), block(1, c)], axis=1) for c in (0, 1)])
    for u in range(UNITS):
        removed = dot(inside[u][0], both(solved_ref[u], wide))
        reads_ref[u] = (rhos[u] - removed[:, :128]).astype(bf16)
        local_ref[u] = dot(inside[u][1], both(v_ref[u], masks)) - removed[:, 128:]
    gate_ref[...] = project(wg_ref)
    pgate_ref[...] = project(wq_ref)


def row_kernel(home_ref, first_ref, second_ref, third_ref, after_ref, prefix_ref, next_ref, total_ref, maps):
    y = lax.axis_index("sp_1")
    for step, src in enumerate((home_ref, first_ref, second_ref, third_ref)):
        maps[(y + 4 - step) & 3] = src[:256]
    next_ref[256:] = first_ref[256:]
    masks = head_masks()
    for s in (0, 1):
        rows = slice(s * 128, s * 128 + 128)
        own = [maps[j, rows] for j in range(4)]
        front = compose(own[0], own[1], masks)
        back = compose(own[2], own[3], masks)
        whole = compose(front, back, masks).astype(bf16)
        next_ref[rows] = whole
        total_ref[rows] = whole
        prefix_ref[0, s] = own[0].astype(f32)
        prefix_ref[1, s] = front
        prefix_ref[2, s] = compose(front, own[2], masks)


def column_kernel(
    prefix_ref, first_ref, second_ref, third_ref, init_ref,
    home_ref, one_ref, two_ref, three_ref,
    starts, rows,
):
    y = lax.axis_index("sp_1")
    z = lax.axis_index("sp_0")
    for step, src in enumerate((first_ref, second_ref, third_ref)):
        rows[(z + 3 - step) & 3] = src[:256]
    masks = head_masks()
    pair = jnp.minimum(y, 2) * 2
    for s in (0, 1):
        state = jnp.concatenate([init_ref[s, pair], init_ref[s, pair + 1]], axis=1)
        later = [rows[j, s * 128 : s * 128 + 128] for j in range(3)]
        first = compose(state, later[0], masks)
        second = compose(first, later[1], masks)
        third = compose(first, compose(later[1], later[2], masks), masks)
        state = jnp.where(z == 0, state, jnp.where(z == 1, first, jnp.where(z == 2, second, third)))
        starts[0, s] = state.astype(bf16)
        for j in range(3):
            starts[j + 1, s] = compose(state, prefix_ref[j, s], masks).astype(bf16)
    for step, dest in enumerate((home_ref, one_ref, two_ref, three_ref)):
        dest[...] = starts[(y + step) & 3]


def pool_kernel(pool_ref, beside_ref, above_ref, pgate_ref, mix_ref, pscale_ref, wp_ref, part_ref, out_ref):
    tp = lax.axis_index("tp")
    y = lax.axis_index("sp_1")
    place = lax.axis_index("sp_0") * 4 + y
    is_first = tp == 0
    factor = jnp.where(is_first, pscale_ref[:, :256], pscale_ref[:, 256:])
    for s in (0, 1):
        current = pool_ref[s * 128 : s * 128 + 128].astype(f32)
        tails = []
        for half in (0, 1):
            rows = slice(256 + (2 * s + half) * 16, 272 + (2 * s + half) * 16)
            tails.append(
                jnp.where(
                    place == 0,
                    0.0,
                    jnp.where(y > 0, beside_ref[rows].astype(f32), above_ref[rows].astype(f32)),
                )
            )
        padded = jnp.concatenate([jnp.concatenate(tails, axis=1), current], axis=0)
        sums = {1: padded}
        for by in (1, 2, 4, 8):
            before = sums[by]
            moved = jnp.concatenate([jnp.zeros((by, 256), f32), before[: 144 - by]], axis=0)
            sums[2 * by] = before + moved
        position = (place * 128 + iota(128, 128, 0) + 1).astype(f32)
        for g in (0, 1):
            lanes = slice(g * 128, g * 128 + 128)
            small, large = 2 << g, 8 << g
            trailing = jnp.where(is_first, sums[small][16:, lanes], sums[large][16:, lanes])
            window = jnp.where(is_first, float(small), float(large))
            diffs = trailing / jnp.minimum(position, window) - current[:, lanes]
            mixed = dot(diffs.astype(bf16), mix_ref[tp * 2 + g])
            gate = pgate_ref[s * 128 : s * 128 + 128, lanes].astype(f32)
            out_ref[s * 128 : s * 128 + 128, lanes] = (
                mixed * factor[:, lanes] * (gate * jax.nn.sigmoid(gate))
            ).astype(bf16)
    part_ref[...] = dot(out_ref[...], wp_ref[...])


def final_kernel(
    home_ref, one_ref, two_ref, three_ref, reads_ref, local_ref, gate_ref, hgain_ref, part_ref,
    wr_ref,
    send_ref, rec,
    starts,
):
    tp = lax.axis_index("tp")
    y = lax.axis_index("sp_1")
    for step, src in enumerate((home_ref, one_ref, two_ref, three_ref)):
        starts[(y + 4 - step) & 3] = src[...]
    masks = head_masks()
    row, col = iota(128, 128, 0), iota(128, 128, 1)
    mean_of = jnp.where((row >> 6) == (col >> 6), 1.0 / HEAD, 0.0).astype(bf16)
    is_first = tp == 0
    for u in range(UNITS):
        s, h = u // 3, u % 3
        lanes = slice(h * 128, h * 128 + 128)
        shifted = slice(384 + h * 128, 384 + h * 128 + 128)
        rows = slice(s * 128, s * 128 + 128)
        out = dot(reads_ref[u], both(starts[h, s], masks), NT) + local_ref[u]
        out = out - dot_fine_left(out, mean_of)
        spread = dot(out * out, mean_of)
        gain = jnp.where(is_first, line_of(hgain_ref, lanes), line_of(hgain_ref, shifted))
        gate = gate_ref[rows, lanes].astype(f32)
        rec[rows, lanes] = (
            out * lax.rsqrt(spread + 1.0) * gain * (gate * jax.nn.sigmoid(gate))
        ).astype(bf16)
    cols = pl.ds(pl.multiple_of((1 - tp) * 1024, 1024), 1024)
    send_ref[...] = (dot(rec[...], wr_ref[:, cols]) + part_ref[:, cols]).astype(bf16)


def keep_kernel(rec_ref, part_ref, wr_ref, keep_ref):
    cols = pl.ds(pl.multiple_of(lax.axis_index("tp") * 1024, 1024), 1024)
    keep_ref[...] = (dot(rec_ref[...], wr_ref[:, cols]) + part_ref[:, cols]).astype(bf16)


def sum_kernel(keep_ref, arrived_ref, out_ref, buf, sems):
    copies = []
    for i in range(4):
        rows = slice(i * 64, i * 64 + 64)
        buf[rows] = (keep_ref[rows].astype(f32) + arrived_ref[rows].astype(f32)).astype(bf16)
        copies.append(pltpu.make_async_copy(buf.at[rows], out_ref.at[rows], sems.at[i]))
        copies[-1].start()
    finish(copies)


def vmem(count):
    return [pl.BlockSpec(memory_space=pltpu.VMEM)] * count


def hbm(count):
    return [pl.BlockSpec(memory_space=pltpu.HBM)] * count


def shape(dims, kind=bf16):
    return jax.ShapeDtypeStruct(dims, kind)


def call(body, name, ins, outs, scratch, limit, flops=0):
    return pl.pallas_call(
        body,
        name=name,
        out_shape=outs,
        in_specs=ins,
        out_specs=vmem(len(outs)) if isinstance(outs, (list, tuple)) else vmem(1)[0],
        scratch_shapes=scratch,
        compiler_params=pltpu.CompilerParams(vmem_limit_bytes=limit * MIB),
        cost_estimate=pl.CostEstimate(flops=flops, transcendentals=0, bytes_accessed=0) if flops else None,
    )


def around(parts, axis):
    return [
        lax.ppermute(part, axis, [(i, (i + step) & 3) for i in range(4)]) for step, part in enumerate(parts, 1)
    ]


def shards(
    tokens, norm_gain, w_recept, w_key, w_value, w_decay, w_rate, w_gate_rec, w_pool, w_gate_pool,
    decay_base, rate_base, head_gain, pool_mix, pool_scale, w_out_rec, w_out_pool, init_state,
):
    other = lax.ppermute(tokens, "tp", [(0, 1), (1, 0)])
    line = lambda x: x.reshape(1, -1)
    pinned = lambda x: pltpu.with_memory_space_constraint(x, pltpu.HBM)
    weights = [pinned(w) for w in (w_key, w_decay, w_rate, w_value)]
    own_normed, squares, *prepared = call(
        own_kernel,
        "own",
        hbm(6),
        [shape((256, 1024)), shape((256, 128), f32)]
        + [shape((256, 1536), f32), shape((1024, 1536))],
        [pltpu.VMEM((1024, 1536), bf16)]
        + [
            pltpu.SemaphoreType.DMA((8,)), pltpu.VMEM((256, 1024), bf16), pltpu.VMEM((1, D), f32),
            pltpu.SemaphoreType.DMA((2,)),
        ],
        20,
        1_000_000_000,
    )(pinned(tokens.reshape(256, 1024)), pinned(line(norm_gain)), *weights)
    normed, scale, pool, home, m1, m2, m3, right, solved, v, grow, lift = call(
        local_kernel,
        "local",
        vmem(9),
        [
            shape((256, 1024)), shape((256, 128), f32), shape((256, 256)),
            shape((256, 128)), shape((320, 128)), shape((256, 128)), shape((256, 128)),
            shape((6, 256, 128)), shape((6, 128, 256)), shape((6, 128, 128)),
            shape((6, 128, 128), f32), shape((6, 128), f32),
        ],
        [pltpu.VMEM((6, 128, 128), f32)] * 3
        + [pltpu.VMEM((4, 256, 128), bf16)]
        + [pltpu.VMEM((D, 256), bf16), pltpu.SemaphoreType.DMA((1,))],
        24,
        3_000_000_000,
    )(
        other.reshape(256, 1024), own_normed, line(norm_gain), squares, decay_base, rate_base, *prepared,
        w_pool,
    )
    r1, r2, r3 = around((m1, m2, m3), "sp_1")
    reads, local, gate, pgate = call(
        side_kernel,
        "side",
        vmem(11),
        [shape((6, 128, 128)), shape((6, 128, 128), f32), shape((256, 384)), shape((256, 256))],
        [],
        16,
        1_000_000_000,
    )(own_normed, normed, scale, right, solved, v, grow, lift, w_recept, w_gate_rec, w_gate_pool)
    prefix, onward, total = call(
        row_kernel,
        "row",
        vmem(4) + [pl.BlockSpec(memory_space=pl.ANY)],
        [shape((3, 2, 128, 128), f32), shape((320, 128)), shape((256, 128))],
        [pltpu.VMEM((4, 256, 128), bf16)],
        8,
        100_000_000,
    )(home, r1, r2, r3, pgate)
    columns = around((onward, total, total), "sp_0")
    s0, s1, s2, s3 = call(
        column_kernel,
        "column",
        vmem(5),
        [shape((2, 64, 128))] * 4,
        [pltpu.VMEM((4, 2, 64, 128), bf16), pltpu.VMEM((4, 256, 128), bf16)],
        8,
        100_000_000,
    )(prefix, *columns, init_state)
    t1, t2, t3 = around((s1, s2, s3), "sp_1")
    pool_part = call(
        pool_kernel, "pool", vmem(7), shape((256, D), f32), [pltpu.VMEM((256, 256), bf16)], 12, 300_000_000
    )(pool, r1, columns[0], pgate, pool_mix, line(pool_scale), w_out_pool)
    send, rec = call(
        final_kernel,
        "final",
        vmem(10),
        [shape((256, 1024)), shape((256, 384))],
        [pltpu.VMEM((4, 2, 64, 128), bf16)],
        20,
        1_000_000_000,
    )(s0, t1, t2, t3, reads, local, gate, head_gain, pool_part, w_out_rec)
    arrived = lax.ppermute(send, "tp", [(0, 1), (1, 0)])
    keep = call(keep_kernel, "keep", vmem(3), shape((256, 1024)), [], 8, 300_000_000)(rec, pool_part, w_out_rec)
    mixed = pl.pallas_call(
        sum_kernel,
        name="sum",
        out_shape=shape((256, 1024)),
        in_specs=vmem(2),
        out_specs=hbm(1)[0],
        scratch_shapes=[pltpu.VMEM((256, 1024), bf16), pltpu.SemaphoreType.DMA((4,))],
        compiler_params=pltpu.CompilerParams(vmem_limit_bytes=4 * MIB),
    )(keep, arrived)
    return mixed.reshape(2, 128, 1024)


def solution(mesh):
    split = Mesh(
        mesh.devices.reshape(4, 4, mesh.shape["fs"], mesh.shape["tp"]), ("sp_0", "sp_1", "fs", "tp")
    )
    column = P(None, "tp")
    placed = (
        (P("fs", SP, "tp"), P()) + (column,) * 8 + (P(),) * 5
        + (P("tp", None), P("tp", None), P("fs", "tp", None, None))
    )
    return jax.shard_map(
        shards, mesh=split, in_specs=placed, out_specs=P("fs", SP, "tp"), check_vma=False
    )
```
